32 devices in a mesh: ep: 4 (over y, x), tp: 8 (over z, core).
Axes of the slice: x: 2, y: 2, z: 4, core: 2. Of those that a mesh axis runs over, the one named last changes fastest.
Arguments:
- tokens: bfloat16 [2048, 2048], P('ep', 'tp'), may hold values from -6 to 6
- norm_gain: float32 [2048], replicated, may hold values from 0.1 to 1.9
- norm_shift: float32 [2048], replicated, may hold values from -3 to 3
- expert_ids: int32 [2048, 6], P('ep'), may hold values from 0 to 31, all different within a row; in each aligned block of 64 rows (0 to 63, 64 to 127, ...) at most 24 rows name the same one
- affinity: float32 [2048, 6], P('ep'), may hold values from 0.05 to 1
- expert_gate: bfloat16 [32, 2048, 512], P(('ep', 'tp')), may hold values from -0.125 to 0.125
- expert_up: bfloat16 [32, 2048, 512], P(('ep', 'tp')), may hold values from -0.125 to 0.125
- expert_down: bfloat16 [32, 512, 2048], P(('ep', 'tp')), may hold values from -0.25 to 0.25
- shared_gate: bfloat16 [512, 2048], P('tp'), may hold values from -0.125 to 0.125
- shared_up: bfloat16 [512, 2048], P('tp'), may hold values from -0.125 to 0.125
- shared_down: bfloat16 [512, 2048], replicated, may hold values from -0.25 to 0.25
Outputs:
- mixed: bfloat16 [2048, 2048], P(('ep', 'tp'))
The draws below stay inside these ranges and needn't reach their ends.
Inputs may be any that keep to these rules, and one draw needn't show every extreme that they name: `expert_ids`: each row names 6 different experts; in each aligned block of 64 rows (the rows of one device of tp) no expert is named more than 24 times, and in some blocks an expert is named exactly 24 times.
All inputs are finite; a program needn't handle non-finite values.
Results may differ from the reference program's by a relative error of at most 0.0069.
Values may be sent and summed in bfloat16 or wider, within the bound.
A program may use at most 64 MiB of HBM per device.

```python
import math
import jax
import jax.numpy as jnp
import numpy as np
from jax import lax

D = 2048
HID = 512
SHARED_HID = 512
TOP_K = 6
EXPERTS = 32
ROWS_BLK = 64
SLOTS = 24
TOKENS = 2048


def block_scale(stream_key, extent, cuts, least, top_value):
    level = 1.0
    for dim, parts in cuts:
        heights = jax.random.uniform(jax.random.fold_in(jax.random.fold_in(stream_key, 6), dim), (parts,), jnp.float32, least / len(cuts), top_value / len(cuts))
        level = level * jnp.repeat(jnp.exp(heights), extent[dim] // parts).reshape((-1,) + (1,) * (len(extent) - 1 - dim))
    return level


def routed_block(key, own, number, rows, number_of, top, bound, slope):
    ranking = jax.random.permutation(key, number_of)
    crowded, ordinary = portions_of(number_of, rows * top, bound, slope, True), portions_of(number_of, rows * top, bound, slope, False)
    places = jnp.arange(number_of)

    def named(lengths, rotation):
        used = int((lengths > 0).sum())
        fixed = max(1, used // 4)
        shifted = fixed + (places - fixed + rotation * (used - fixed)) % max(1, number_of - fixed)
        return jnp.zeros((number_of,), jnp.int32).at[ranking[jnp.where(places < fixed, places, shifted)]].set(jnp.asarray(lengths, jnp.int32))

    lengths = jnp.where(number % 4 == 0, named(crowded, number // 4), named(ordinary, number - number // 4 - 1))
    mixed = jax.random.permutation(jax.random.fold_in(own, 3), number_of)
    giver, sink = mixed[0:number_of // 2 * 2:2], mixed[1:number_of // 2 * 2:2]
    room = jnp.minimum(lengths[giver] - 1, bound - lengths[sink]) // 2
    room = jnp.where((giver == ranking[0]) | (sink == ranking[0]) | (lengths[sink] == 0), 0, jnp.maximum(room, 0))
    shifted = jax.random.randint(jax.random.fold_in(own, 4), (number_of // 2,), 0, 1 << 20) % (room + 1)
    lengths = lengths.at[giver].add(-shifted).at[sink].add(shifted)
    members = jnp.searchsorted(jnp.cumsum(lengths), jnp.arange(rows * top), side="right").astype(jnp.int32)
    listing = members.reshape(top, rows).T
    listing = listing[jax.random.permutation(jax.random.fold_in(own, 1), rows)]
    rotation = jax.random.randint(jax.random.fold_in(own, 2), (rows, 1), 0, top)
    return jnp.take_along_axis(listing, (jnp.arange(top)[None, :] + rotation) % top, axis=1)


def portions_of(count, total, reach, skew, full):
    portions = [(1 << 20) // math.isqrt(standing ** skew) + 1 for standing in range(1, count + 1)]
    largest = reach if full else min(reach, max(-(-total // count), total * portions[0] // sum(portions)))
    least = 1 if total - largest >= count - 1 else 0
    given, surplus = [largest] + [least] * (count - 1), total - largest - least * (count - 1)
    while surplus > 0:
        free = [i for i in range(1, count) if given[i] < largest] or [i for i in range(1, count) if given[i] < reach]
        pool, remaining = sum([portions[i] for i in free]), surplus
        for i in free:
            more = min(reach - given[i], max(1, remaining * portions[i] // pool), surplus)
            given[i] = given[i] + more
            surplus = surplus - more
    return np.array(given)


def normal_values(rng, extent, width, most, cuts=(), kind=jnp.bfloat16):
    entries = width * jax.random.normal(rng, extent, jnp.float32)
    if cuts:
        entries = entries * block_scale(rng, extent, cuts, -0.22, 0.18)
    return jnp.clip(entries, -most, most).astype(kind)


def setup_inputs(seed: int = 0) -> dict:
    key_of = jax.random.split(jax.random.key(seed), 12)
    tokens = normal_values(key_of[0], (TOKENS, D), 1.0, 6.0, ((0, 4), (1, 8)))
    norm_gain = jnp.clip(1.0 + 0.18 * jax.random.normal(key_of[1], (D,), jnp.float32), 0.1, 1.9)
    norm_shift = normal_values(key_of[2], (D,), 0.5, 3.0, (), jnp.float32)
    expert_ids_keys = jax.random.split(jax.random.fold_in(key_of[3], 1), TOKENS // ROWS_BLK)
    expert_ids_turns = jax.random.permutation(jax.random.fold_in(key_of[3], 3), TOKENS // ROWS_BLK)
    expert_ids = jax.vmap(lambda own, number: routed_block(jax.random.fold_in(key_of[3], 2), own, number, ROWS_BLK, EXPERTS, TOP_K, SLOTS, 2))(expert_ids_keys, expert_ids_turns).reshape((TOKENS, TOP_K))
    affinity = jnp.clip(0.05 + 0.95 * jax.random.uniform(key_of[4], (TOKENS, TOP_K), jnp.float32) ** block_scale(key_of[4], (TOKENS, TOP_K), ((0, 4),), -0.2, 0.2), 0.05, 1.0)
    expert_gate = normal_values(key_of[5], (EXPERTS, D, HID), D ** -0.5, 0.125, ((0, 32),))
    expert_up = normal_values(key_of[6], (EXPERTS, D, HID), D ** -0.5, 0.125, ((0, 32),))
    expert_down = normal_values(key_of[7], (EXPERTS, HID, D), HID ** -0.5, 0.25, ((0, 32),))
    shared_gate = normal_values(key_of[8], (SHARED_HID, D), D ** -0.5, 0.125, ((0, 8),))
    shared_up = normal_values(key_of[9], (SHARED_HID, D), D ** -0.5, 0.125, ((0, 8),))
    shared_down = normal_values(key_of[10], (SHARED_HID, D), SHARED_HID ** -0.5, 0.25)
    return dict(tokens=tokens, norm_gain=norm_gain, norm_shift=norm_shift, expert_ids=expert_ids, affinity=affinity, expert_gate=expert_gate, expert_up=expert_up, expert_down=expert_down, shared_gate=shared_gate, shared_up=shared_up, shared_down=shared_down)


ROUTED_SCALE = 2.5
EPSILON = 1e-05

def pair_ranks(flat_ids, expert_count):
    onehot = flat_ids[..., None] == jnp.arange(expert_count, dtype=jnp.int32)
    running = jnp.cumsum(onehot.astype(jnp.int32), axis=-2)
    return (lax.optimization_barrier(jnp.sum(jnp.where(onehot, running, 0), axis=-1)) - 1).astype(jnp.int32)

def expert_rows(tok_rows, w_gate, w_up, w_down):
    gate_act = jnp.dot(tok_rows, w_gate, preferred_element_type=jnp.float32)
    up_act = jnp.dot(tok_rows, w_up, preferred_element_type=jnp.float32)
    hidden = (jax.nn.silu(gate_act) * up_act).astype(jnp.bfloat16)
    return jnp.dot(hidden, w_down, preferred_element_type=jnp.float32).astype(jnp.bfloat16)

def rank_block(block_ids):
    return pair_ranks(block_ids, EXPERTS)

def reference(tokens, norm_gain, norm_shift, expert_ids, affinity, expert_gate, expert_up, expert_down, shared_gate, shared_up, shared_down):
    values = tokens.astype(jnp.float32)
    center = values - lax.optimization_barrier(jnp.mean(values, axis=1, keepdims=True))
    spread = lax.optimization_barrier(jnp.mean(center * center, axis=1, keepdims=True))
    normed = (center * lax.rsqrt(spread + EPSILON) * norm_gain + norm_shift).astype(jnp.bfloat16)
    weights = affinity / lax.optimization_barrier(jnp.sum(affinity, axis=1, keepdims=True)) * ROUTED_SCALE
    contract = (((1,), (1,)), ((), ()))
    shared_g = lax.dot_general(normed, shared_gate, contract, preferred_element_type=jnp.float32)
    shared_u = lax.dot_general(normed, shared_up, contract, preferred_element_type=jnp.float32)
    shared_hidden = (jax.nn.silu(shared_g) * shared_u).astype(jnp.bfloat16)
    shared_out = jnp.dot(shared_hidden, shared_down, preferred_element_type=jnp.float32)
    blocks = TOKENS // ROWS_BLK
    block_ids = expert_ids.reshape(blocks, ROWS_BLK * TOP_K).astype(jnp.int32)
    ranks = lax.map(rank_block, block_ids)
    block_index = jnp.arange(blocks, dtype=jnp.int32)[:, None]
    dest = (block_ids * blocks + block_index) * SLOTS + ranks
    token_index = block_index * ROWS_BLK + jnp.arange(ROWS_BLK * TOP_K, dtype=jnp.int32)[None, :] // TOP_K
    token_index = jnp.broadcast_to(token_index, dest.shape)
    per_expert = blocks * SLOTS
    source_row = jnp.full((EXPERTS * per_expert,), TOKENS, jnp.int32).at[dest.reshape(-1)].set(token_index.reshape(-1))
    source_row = source_row.reshape(EXPERTS, per_expert)
    slot_weight = jnp.zeros((EXPERTS * per_expert,), jnp.float32).at[dest.reshape(-1)].set(weights.reshape(-1))
    slot_weight = slot_weight.reshape(EXPERTS, per_expert)

    def one_expert(total, inputs):
        w_gate, w_up, w_down, row_index, row_weight = inputs
        tok_rows = jnp.take(normed, row_index, axis=0, mode='fill', fill_value=0)
        result = expert_rows(tok_rows, w_gate, w_up, w_down)
        total = total.at[row_index].add(result.astype(jnp.float32) * row_weight[:, None], mode='drop')
        return (total, None)
    routed, unused = lax.scan(one_expert, jnp.zeros((TOKENS, D), jnp.float32), (expert_gate, expert_up, expert_down, source_row, slot_weight))
    return (routed + shared_out).astype(jnp.bfloat16)
```

```python
import functools
import math

import jax
import jax.numpy as jnp
from jax import lax
from jax.experimental import pallas as pl
from jax.experimental.pallas import tpu as pltpu
from jax.sharding import PartitionSpec as P

ROUTED_SCALE = 2.5
EPSILON = 1e-05
MESH = pl.DeviceIdType.MESH
F32 = jnp.float32
BF16 = jnp.bfloat16


def partner(index, step, count):
    if count & (count - 1):
        return lax.rem(index + step, count)
    result, bit = 0, 1
    while bit < count:
        result = result + ((index // bit) % 2 + (step // bit) % 2) % 2 * bit
        bit *= 2
    return result


def layer_kernel(
    sizes,
    tokens_hbm,
    ids_hbm,
    affinity_hbm,
    gain_hbm,
    shift_hbm,
    sgate_hbm,
    sup_hbm,
    gate_hbm,
    up_hbm,
    down_hbm,
    sdown_hbm,
    out_ref,
    ids_ref,
    affinity_ref,
    gain_ref,
    shift_ref,
    sgate_ref,
    sup_ref,
    gate_ref,
    up_ref,
    down_ref,
    sdown_ref,
    whole,
    pick,
    spread_t,
    spread,
    sent,
    inc,
    norm,
    hidden,
    shidden,
    res,
    ret,
    part,
    own,
    pair_out,
    pair_in,
    far_out,
    far_in,
    load_sem,
    first_sem,
    u_send,
    d_send,
    f_send,
    a_recv,
    b_send,
    b_recv,
    r_send,
    r_recv,
    p_send,
    p_recv,
    q_send,
    q_recv,
):
    ep, tp, rows, slots, slot_cap, feat, chunks, cols = sizes
    chips = tp // 2
    g = lax.axis_index("ep")
    t = lax.axis_index("tp")
    z = t // 2
    c = t % 2
    mate = z * 2 + 1 - c
    width = tp * feat
    shared_rows = sdown_ref.shape[0]

    firsts = [
        pltpu.make_async_copy(ids_hbm, ids_ref, first_sem.at[0]),
        pltpu.make_async_copy(affinity_hbm, affinity_ref, first_sem.at[1]),
        pltpu.make_async_copy(tokens_hbm, whole.at[t], first_sem.at[2]),
    ]
    loads = [
        pltpu.make_async_copy(gain_hbm, gain_ref, load_sem.at[0]),
        pltpu.make_async_copy(shift_hbm, shift_ref, load_sem.at[1]),
        pltpu.make_async_copy(sgate_hbm, sgate_ref, load_sem.at[2]),
        pltpu.make_async_copy(sup_hbm, sup_ref, load_sem.at[3]),
        pltpu.make_async_copy(
            sdown_hbm.at[pl.ds(pl.multiple_of(t * shared_rows, 8), shared_rows)],
            sdown_ref,
            load_sem.at[4],
        ),
        pltpu.make_async_copy(gate_hbm, gate_ref, load_sem.at[5]),
        pltpu.make_async_copy(up_hbm, up_ref, load_sem.at[6]),
        pltpu.make_async_copy(down_hbm, down_ref, load_sem.at[7]),
    ]
    for load in firsts:
        load.start()

    def remote(src, dst, send, recv, e, k):
        return pltpu.make_async_remote_copy(
            src_ref=src,
            dst_ref=dst,
            send_sem=send,
            recv_sem=recv,
            device_id=(e, k),
            device_id_type=MESH,
        )

    barrier = pltpu.get_barrier_semaphore()
    partners = [(partner(g, p, ep), t) for p in range(1, ep)]
    partners += [(g, partner(z, d, chips) * 2 + c) for d in range(1, chips)]
    partners += [(g, mate)]
    for e, k in partners:
        pl.semaphore_signal(barrier, inc=1, device_id=(e, k), device_id_type=MESH)
    for load in loads:
        load.start()
    for load in firsts[:2]:
        load.wait()
    ids = ids_ref[...]
    affinity = affinity_ref[...]
    weights = affinity / jnp.sum(affinity, axis=0, keepdims=True) * ROUTED_SCALE
    block = rows // tp
    early = lax.broadcasted_iota(jnp.int32, (rows, rows), 0)
    late = lax.broadcasted_iota(jnp.int32, (rows, rows), 1)
    before = jnp.where((early < late) & (early // block == late // block), 1.0, 0.0).astype(BF16)
    hits = [ids == e * tp + t for e in range(ep)]
    chosen = [jnp.sum(jnp.where(hit, 1.0, 0.0), axis=0, keepdims=True) for hit in hits]
    pad = [jnp.zeros((-ep % 16, rows), F32)] if ep % 16 else []
    ranks = jnp.dot(
        jnp.concatenate(chosen + pad, axis=0).astype(BF16), before, preferred_element_type=F32
    ).astype(jnp.int32)
    base = lax.broadcasted_iota(jnp.int32, (1, rows), 1) // block * slot_cap
    line = lax.broadcasted_iota(jnp.int32, (slots, rows), 0)
    for e in range(ep):
        place = jnp.where(chosen[e] > 0.5, base + ranks[e : e + 1, :], -1)
        weight = jnp.sum(jnp.where(hits[e], weights, 0.0), axis=0, keepdims=True)
        pick[e] = jnp.where(line == place, 1.0, 0.0).astype(BF16)
        spread_t[pl.ds(e * slots, slots), :] = jnp.where(line == place, weight, 0.0)
    pl.semaphore_wait(barrier, len(partners))

    def forward(k):
        return remote(whole.at[k], whole.at[k], f_send.at[k // 2], a_recv.at[k], g, mate)

    def upward(k):
        there = lax.rem(z + 1, chips) * 2 + c
        return remote(whole.at[k], whole.at[k], u_send.at[k // 2], a_recv.at[k], g, there)

    def downward(k):
        there = lax.rem(z + chips - 1, chips) * 2 + c
        return remote(whole.at[k], whole.at[k], d_send.at[k // 2], a_recv.at[k], g, there)

    firsts[2].wait()

    @pl.when(z < chips - 1)
    def _():
        upward(t).start()

    @pl.when(z > 0)
    def _():
        downward(t).start()

    forward(t).start()

    both = jnp.minimum(z, chips - 1 - z)
    longer = jnp.where(z > chips - 1 - z, -1, 1)

    def chunk_at(i):
        j = i // 2
        side = i % 2
        alternate = (j + 1) // 2 * (j % 2 * 2 - 1)
        step = jnp.where(j <= 2 * both, alternate, longer * (j - both))
        return side, z + step, (z + step) * 2 + lax.rem(c + side, 2)

    near = [p for p in range(1, ep) if not p & (p - 1)]
    far = [p for p in range(1, ep) if p & (p - 1)]
    lag = 3 * tp // 8
    half = chunks // 8

    def send_rows(k, p):
        e = partner(g, p, ep)
        remote(sent.at[k, e], inc.at[k, g], b_send, b_recv.at[g], e, t).start()

    def chunk_step(i, carry):
        side, chip, k = chunk_at(i)

        @pl.when(i > 0)
        def _():
            forward(k).wait_recv()

        fresh = (i > 0) & (side == 0)

        @pl.when(fresh & (chip < z) & (z < chips - 1))
        def _():
            upward(k).start()

        @pl.when(fresh & (chip > z) & (z > 0))
        def _():
            downward(k).start()

        @pl.when(fresh)
        def _():
            forward(k).start()

        picked = jnp.dot(
            pick[...].reshape(ep * slots, rows), whole[k], preferred_element_type=F32
        ).astype(BF16)
        sent[k] = picked.reshape(ep, slots, feat)
        inc[k, g] = sent[k, g]
        for p in near:
            send_rows(k, p)
        if far:

            @pl.when(i >= lag)
            def _():
                for p in far:
                    send_rows(chunk_at(i - lag)[2], p)

        return carry

    lax.fori_loop(0, tp, chunk_step, 0)

    def late_step(i, carry):
        for p in far:
            send_rows(chunk_at(i)[2], p)
        return carry

    if far:
        lax.fori_loop(tp - lag, tp, late_step, 0)
    spread[...] = spread_t[...].T.astype(BF16)

    def normalise(read, count):
        tile = math.gcd(64, count)

        def body(i, carry):
            at = pl.ds(pl.multiple_of(i * tile, tile), tile)
            total = jnp.zeros((tile, feat), F32)
            for k in range(tp):
                total = total + read(k, at).astype(F32)
            mean = jnp.sum(total, axis=1, keepdims=True) / width
            total = jnp.zeros((tile, feat), F32)
            for k in range(tp):
                center = read(k, at).astype(F32) - mean
                total = total + center * center
            scale = lax.rsqrt(jnp.sum(total, axis=1, keepdims=True) / width + EPSILON)
            for k in range(tp):
                lanes = slice(k * feat, (k + 1) * feat)
                value = (read(k, at).astype(F32) - mean) * scale
                value = value * gain_ref[:, lanes] + shift_ref[:, lanes]
                norm[at, lanes] = value.astype(BF16)
            return carry

        lax.fori_loop(0, count // tile, body, 0)

    for load in loads[:5]:
        load.wait()
    normalise(lambda k, at: whole[k, at, :], rows)
    contract = (((1,), (1,)), ((), ()))
    sg = lax.dot_general(norm[...], sgate_ref[...], contract, preferred_element_type=F32)
    su = lax.dot_general(norm[...], sup_ref[...], contract, preferred_element_type=F32)
    shidden[...] = (jax.nn.silu(sg) * su).astype(BF16)

    for load in loads[5:]:
        load.wait()

    def expert_step(p, carry):
        s = partner(g, p, ep)

        @pl.when(p > 0)
        def _():
            remote(sent.at[:, s], inc.at[:, s], b_send, b_recv.at[s], s, t).wait_recv()

        normalise(lambda k, at: inc[k, s, at, :], slots)
        got = norm[0:slots, :]
        gate_act = jnp.dot(got, gate_ref[...], preferred_element_type=F32)
        up_act = jnp.dot(got, up_ref[...], preferred_element_type=F32)
        hidden[s] = (jax.nn.silu(gate_act) * up_act).astype(BF16)

        @pl.when(p == 0)
        def _():
            def own_step(i, carry):
                ret[i, g] = down_rows(i, g)
                return carry

            lax.fori_loop(0, chunks, own_step, 0)

        is_near = functools.reduce(jnp.logical_or, [p == n for n in near])

        @pl.when(is_near)
        def _():
            def near_step(i, carry):
                send_result(i, s)
                return carry

            lax.fori_loop(0, half, near_step, 0)

        return carry

    def lanes_of(i):
        return pl.ds(pl.multiple_of(i * cols, cols), cols)

    def down_rows(i, s):
        return jnp.dot(
            hidden[s], down_ref[:, lanes_of(i)], preferred_element_type=F32
        ).astype(BF16)

    def send_result(i, s):
        res[i, s] = down_rows(i, s)
        remote(res.at[i, s], ret.at[i, g], r_send, r_recv.at[i], s, t).start()

    lax.fori_loop(0, ep, expert_step, 0)

    def down_step(i, carry):
        for p in far:
            send_result(i, partner(g, p, ep))

        @pl.when(i < chunks - half)
        def _():
            for p in near:
                send_result(i + half, partner(g, p, ep))

        return carry

    lax.fori_loop(0, chunks, down_step, 0)

    def pair_copy(i):
        return remote(pair_out.at[i], pair_in.at[i], p_send, p_recv.at[i], g, mate)

    def produce(i):
        others = pl.ds(0, ep - 1)
        remote(res.at[i, others], ret.at[i, others], r_send, r_recv.at[i], g, mate).wait_recv()
        total = jnp.dot(
            spread[...], ret[i].reshape(ep * slots, cols), preferred_element_type=F32
        ) + jnp.dot(shidden[...], sdown_ref[:, lanes_of(i)], preferred_element_type=F32)
        part[i % 2] = total.reshape(part.shape[1:])
        for zz in range(chips):
            pair_out[i, zz] = part[i % 2, zz * 2 + 1 - c].astype(BF16)
        pair_copy(i).start()

    def finish(i):
        pair_copy(i).wait_recv()
        for d in range(1, chips):
            zz = partner(z, d, chips)
            far_out[i, zz] = (part[i % 2, zz * 2 + c] + pair_in[i, zz].astype(F32)).astype(BF16)
            remote(
                far_out.at[i, zz],
                far_in.at[i, z],
                q_send,
                q_recv,
                g,
                zz * 2 + c,
            ).start()
        own[i] = part[i % 2, t] + pair_in[i, z].astype(F32)

    def sum_step(i, carry):
        @pl.when(i < chunks)
        def _():
            produce(i)

        @pl.when(i > 0)
        def _():
            finish(i - 1)

        return carry

    lax.fori_loop(0, chunks + 1, sum_step, 0)

    rest = pl.ds(0, chips - 1)
    remote(far_out.at[:, rest], far_in.at[:, rest], q_send, q_recv, g, mate).wait()

    def out_step(i, carry):
        total = own[i]
        for d in range(1, chips):
            total = total + far_in[i, partner(z, d, chips)].astype(F32)
        out_ref[:, lanes_of(i)] = total.astype(BF16)
        return carry

    lax.fori_loop(0, chunks, out_step, 0)

    others = pl.ds(0, ep - 1)
    remote(sent.at[:, others], inc.at[:, others], b_send, b_recv.at[g], g, mate).wait_send()
    remote(res.at[:, others], ret.at[:, others], r_send, r_recv.at[0], g, mate).wait_send()
    remote(pair_out, pair_in, p_send, p_recv.at[0], g, mate).wait_send()

    def sent_step(chip, carry):
        k = chip * 2 + c
        forward(k).wait_send()

        @pl.when((chip <= z) & (z < chips - 1))
        def _():
            upward(k).wait_send()

        @pl.when((chip >= z) & (z > 0))
        def _():
            downward(k).wait_send()

        return carry

    lax.fori_loop(0, chips, sent_step, 0)


def on_device(
    tokens,
    norm_gain,
    norm_shift,
    expert_ids,
    affinity,
    expert_gate,
    expert_up,
    expert_down,
    shared_gate,
    shared_up,
    shared_down,
):
    ep = lax.axis_size("ep")
    tp = lax.axis_size("tp")
    rows, feat = tokens.shape
    width = feat * tp
    top_count = expert_ids.shape[1]
    block = rows // tp
    expert_count = ep * tp
    slot_cap = max(1, 2 * block * top_count // expert_count)
    slots = tp * slot_cap
    hid = expert_gate.shape[2]
    shared_rows = shared_gate.shape[0]
    cols = 256
    chunks = width // cols
    chips = tp // 2

    vmem = pl.BlockSpec(memory_space=pltpu.VMEM)
    anywhere = pl.BlockSpec(memory_space=pl.ANY)
    dma = pltpu.SemaphoreType.DMA
    return pl.pallas_call(
        functools.partial(layer_kernel, (ep, tp, rows, slots, slot_cap, feat, chunks, cols)),
        out_shape=jax.ShapeDtypeStruct((block, width), BF16),
        in_specs=[anywhere] * 11,
        out_specs=vmem,
        scratch_shapes=[
            pltpu.VMEM((top_count, rows), jnp.int32),
            pltpu.VMEM((top_count, rows), F32),
            pltpu.VMEM((1, width), F32),
            pltpu.VMEM((1, width), F32),
            pltpu.VMEM((shared_rows, width), BF16),
            pltpu.VMEM((shared_rows, width), BF16),
            pltpu.VMEM((width, hid), BF16),
            pltpu.VMEM((width, hid), BF16),
            pltpu.VMEM((hid, width), BF16),
            pltpu.VMEM((shared_rows, width), BF16),
            pltpu.VMEM((tp, rows, feat), BF16),
            pltpu.VMEM((ep, slots, rows), BF16),
            pltpu.VMEM((ep * slots, rows), F32),
            pltpu.VMEM((rows, ep * slots), BF16),
            pltpu.VMEM((tp, ep, slots, feat), BF16),
            pltpu.VMEM((tp, ep, slots, feat), BF16),
            pltpu.VMEM((max(rows, slots), width), BF16),
            pltpu.VMEM((ep, slots, hid), BF16),
            pltpu.VMEM((rows, shared_rows), BF16),
            pltpu.VMEM((chunks, ep, slots, cols), BF16),
            pltpu.VMEM((chunks, ep, slots, cols), BF16),
            pltpu.VMEM((2, tp, block, cols), F32),
            pltpu.VMEM((chunks, block, cols), F32),
            pltpu.VMEM((chunks, chips, block, cols), BF16),
            pltpu.VMEM((chunks, chips, block, cols), BF16),
            pltpu.VMEM((chunks, chips, block, cols), BF16),
            pltpu.VMEM((chunks, chips, block, cols), BF16),
            dma((8,)),
            dma((3,)),
            dma((chips,)),
            dma((chips,)),
            dma((chips,)),
            dma((tp,)),
            dma,
            dma((ep,)),
            dma,
            dma((chunks,)),
            dma,
            dma((chunks,)),
            dma,
            dma,
        ],
        compiler_params=pltpu.CompilerParams(
            collective_id=0, has_side_effects=True, vmem_limit_bytes=56 * 1024 * 1024
        ),
        name="moe_layer",
    )(
        tokens,
        expert_ids.T,
        affinity.T,
        norm_gain.reshape(1, width),
        norm_shift.reshape(1, width),
        shared_gate,
        shared_up,
        expert_gate[0],
        expert_up[0],
        expert_down[0],
        shared_down,
    )


def solution(mesh):
    placed = (
        P("ep", "tp"),
        P(),
        P(),
        P("ep", None),
        P("ep", None),
        P(("ep", "tp"), None, None),
        P(("ep", "tp"), None, None),
        P(("ep", "tp"), None, None),
        P("tp", None),
        P("tp", None),
        P(),
    )
    return jax.shard_map(
        on_device, mesh=mesh, in_specs=placed, out_specs=P(("ep", "tp"), None), check_vma=False
    )
```

```python
import functools
import math

import jax
import jax.numpy as jnp
from jax import lax
from jax.experimental import pallas as pl
from jax.experimental.pallas import tpu as pltpu
from jax.sharding import PartitionSpec as P

ROUTED_SCALE = 2.5
EPSILON = 1e-05
MESH = pl.DeviceIdType.MESH
F32 = jnp.float32
BF16 = jnp.bfloat16


def partner(index, step, count):
    if count & (count - 1):
        return lax.rem(index + step, count)
    result, bit = 0, 1
    while bit < count:
        result = result + ((index // bit) % 2 + (step // bit) % 2) % 2 * bit
        bit *= 2
    return result


def layer_kernel(
    sizes,
    tokens_hbm,
    ids_hbm,
    affinity_hbm,
    gain_hbm,
    shift_hbm,
    sgate_hbm,
    sup_hbm,
    gate_hbm,
    up_hbm,
    down_hbm,
    sdown_hbm,
    out_ref,
    ids_ref,
    affinity_ref,
    gain_ref,
    shift_ref,
    sgate_ref,
    sup_ref,
    gate_ref,
    up_ref,
    down_ref,
    sdown_ref,
    whole,
    pick,
    spread_t,
    spread,
    sent,
    inc,
    norm,
    hidden,
    shidden,
    res,
    ret,
    part,
    own,
    pair_out,
    pair_in,
    far_out,
    far_in,
    load_sem,
    first_sem,
    u_send,
    d_send,
    f_send,
    a_recv,
    b_send,
    b_recv,
    r_send,
    r_recv,
    p_send,
    p_recv,
    q_send,
    q_recv,
):
    ep, tp, rows, slots, slot_cap, feat, chunks, cols = sizes
    chips = tp // 2
    g = lax.axis_index("ep")
    t = lax.axis_index("tp")
    z = t // 2
    c = t % 2
    mate = z * 2 + 1 - c
    width = tp * feat
    shared_rows = sdown_ref.shape[0]

    firsts = [
        pltpu.make_async_copy(ids_hbm, ids_ref, first_sem.at[0]),
        pltpu.make_async_copy(affinity_hbm, affinity_ref, first_sem.at[1]),
        pltpu.make_async_copy(tokens_hbm, whole.at[t], first_sem.at[2]),
    ]
    loads = [
        pltpu.make_async_copy(gain_hbm, gain_ref, load_sem.at[0]),
        pltpu.make_async_copy(shift_hbm, shift_ref, load_sem.at[1]),
        pltpu.make_async_copy(sgate_hbm, sgate_ref, load_sem.at[2]),
        pltpu.make_async_copy(sup_hbm, sup_ref, load_sem.at[3]),
        pltpu.make_async_copy(
            sdown_hbm.at[pl.ds(pl.multiple_of(t * shared_rows, 8), shared_rows)],
            sdown_ref,
            load_sem.at[4],
        ),
        pltpu.make_async_copy(gate_hbm, gate_ref, load_sem.at[5]),
        pltpu.make_async_copy(up_hbm, up_ref, load_sem.at[6]),
        pltpu.make_async_copy(down_hbm, down_ref, load_sem.at[7]),
    ]
    for load in firsts:
        load.start()

    def remote(src, dst, send, recv, e, k):
        return pltpu.make_async_remote_copy(
            src_ref=src,
            dst_ref=dst,
            send_sem=send,
            recv_sem=recv,
            device_id=(e, k),
            device_id_type=MESH,
        )

    barrier = pltpu.get_barrier_semaphore()
    partners = [(partner(g, p, ep), t) for p in range(1, ep)]
    partners += [(g, partner(z, d, chips) * 2 + c) for d in range(1, chips)]
    partners += [(g, mate)]
    for e, k in partners:
        pl.semaphore_signal(barrier, inc=1, device_id=(e, k), device_id_type=MESH)
    for load in loads:
        load.start()
    for load in firsts[:2]:
        load.wait()
    ids = ids_ref[...]
    affinity = affinity_ref[...]
    weights = affinity / jnp.sum(affinity, axis=0, keepdims=True) * ROUTED_SCALE
    block = rows // tp
    early = lax.broadcasted_iota(jnp.int32, (rows, rows), 0)
    late = lax.broadcasted_iota(jnp.int32, (rows, rows), 1)
    before = jnp.where((early < late) & (early // block == late // block), 1.0, 0.0).astype(BF16)
    hits = [ids == e * tp + t for e in range(ep)]
    chosen = [jnp.sum(jnp.where(hit, 1.0, 0.0), axis=0, keepdims=True) for hit in hits]
    pad = [jnp.zeros((-ep % 16, rows), F32)] if ep % 16 else []
    ranks = jnp.dot(
        jnp.concatenate(chosen + pad, axis=0).astype(BF16), before, preferred_element_type=F32
    ).astype(jnp.int32)
    base = lax.broadcasted_iota(jnp.int32, (1, rows), 1) // block * slot_cap
    line = lax.broadcasted_iota(jnp.int32, (slots, rows), 0)
    for e in range(ep):
        place = jnp.where(chosen[e] > 0.5, base + ranks[e : e + 1, :], -1)
        weight = jnp.sum(jnp.where(hits[e], weights, 0.0), axis=0, keepdims=True)
        pick[e] = jnp.where(line == place, 1.0, 0.0).astype(BF16)
        spread_t[pl.ds(e * slots, slots), :] = jnp.where(line == place, weight, 0.0)
    pl.semaphore_wait(barrier, len(partners))

    def forward(k):
        return remote(whole.at[k], whole.at[k], f_send.at[k // 2], a_recv.at[k], g, mate)

    def upward(k):
        there = lax.rem(z + 1, chips) * 2 + c
        return remote(whole.at[k], whole.at[k], u_send.at[k // 2], a_recv.at[k], g, there)

    def downward(k):
        there = lax.rem(z + chips - 1, chips) * 2 + c
        return remote(whole.at[k], whole.at[k], d_send.at[k // 2], a_recv.at[k], g, there)

    firsts[2].wait()

    @pl.when(z < chips - 1)
    def _():
        upward(t).start()

    @pl.when(z > 0)
    def _():
        downward(t).start()

    forward(t).start()

    near = [p for p in range(1, ep) if not p & (p - 1)]
    far = [p for p in range(1, ep) if p & (p - 1)]
    half = chunks // 8

    def send_rows(k, p):
        e = partner(g, p, ep)
        remote(sent.at[k, e], inc.at[k, g], b_send, b_recv.at[g], e, t).start()

    def arrive(chip):
        k = chip * 2 + c
        forward(k).wait_recv()

        @pl.when((chip < z) & (z < chips - 1))
        def _():
            upward(k).start()

        @pl.when((chip > z) & (z > 0))
        def _():
            downward(k).start()

        forward(k).start()

    def distance_step(d, carry):
        def at_side(side):
            chip = z + d * (side * 2 - 1)
            return chip, (chip >= 0) & (chip < chips) & ((d > 0) | (side == 0))

        for side in range(2):
            chip, there = at_side(side)

            @pl.when(there & (d > 0))
            def _():
                arrive(chip)

        def chunk_step(q, carry):
            chip, there = at_side(q % 2)
            lane = q // 2
            k = chip * 2 + lax.rem(c + lane, 2)

            @pl.when(there)
            def _():
                @pl.when(lane > 0)
                def _():
                    forward(k).wait_recv()

                picked = jnp.dot(
                    pick[...].reshape(ep * slots, rows), whole[k], preferred_element_type=F32
                ).astype(BF16)
                sent[k] = picked.reshape(ep, slots, feat)
                inc[k, g] = sent[k, g]
                for p in near:
                    send_rows(k, p)

            return carry

        lax.fori_loop(0, 4, chunk_step, 0)

        def far_step(q, carry):
            chip, there = at_side(q % 2)

            @pl.when(there)
            def _():
                for p in far:
                    send_rows(chip * 2 + lax.rem(c + q // 2, 2), p)

            return carry

        lax.fori_loop(0, 4, far_step, 0)
        return carry

    lax.fori_loop(0, chips, distance_step, 0)
    spread[...] = spread_t[...].T.astype(BF16)

    def normalise(read, count):
        tile = math.gcd(64, count)

        def body(i, carry):
            at = pl.ds(pl.multiple_of(i * tile, tile), tile)
            total = jnp.zeros((tile, feat), F32)
            for k in range(tp):
                total = total + read(k, at).astype(F32)
            mean = jnp.sum(total, axis=1, keepdims=True) / width
            total = jnp.zeros((tile, feat), F32)
            for k in range(tp):
                center = read(k, at).astype(F32) - mean
                total = total + center * center
            scale = lax.rsqrt(jnp.sum(total, axis=1, keepdims=True) / width + EPSILON)
            for k in range(tp):
                lanes = slice(k * feat, (k + 1) * feat)
                value = (read(k, at).astype(F32) - mean) * scale
                value = value * gain_ref[:, lanes] + shift_ref[:, lanes]
                norm[at, lanes] = value.astype(BF16)
            return carry

        lax.fori_loop(0, count // tile, body, 0)

    for load in loads[:5]:
        load.wait()
    normalise(lambda k, at: whole[k, at, :], rows)
    contract = (((1,), (1,)), ((), ()))
    sg = lax.dot_general(norm[...], sgate_ref[...], contract, preferred_element_type=F32)
    su = lax.dot_general(norm[...], sup_ref[...], contract, preferred_element_type=F32)
    shidden[...] = (jax.nn.silu(sg) * su).astype(BF16)

    for load in loads[5:]:
        load.wait()

    def expert_step(p, carry):
        s = partner(g, p, ep)

        @pl.when(p > 0)
        def _():
            remote(sent.at[:, s], inc.at[:, s], b_send, b_recv.at[s], s, t).wait_recv()

        normalise(lambda k, at: inc[k, s, at, :], slots)
        got = norm[0:slots, :]
        gate_act = jnp.dot(got, gate_ref[...], preferred_element_type=F32)
        up_act = jnp.dot(got, up_ref[...], preferred_element_type=F32)
        hidden[s] = (jax.nn.silu(gate_act) * up_act).astype(BF16)

        @pl.when(p == 0)
        def _():
            def own_step(i, carry):
                ret[i, g] = down_rows(i, g)
                return carry

            lax.fori_loop(0, chunks, own_step, 0)

        is_near = functools.reduce(jnp.logical_or, [p == n for n in near])

        @pl.when(is_near)
        def _():
            def near_step(i, carry):
                send_result(i, s)
                return carry

            lax.fori_loop(0, half, near_step, 0)

        return carry

    def lanes_of(i):
        return pl.ds(pl.multiple_of(i * cols, cols), cols)

    def down_rows(i, s):
        return jnp.dot(
            hidden[s], down_ref[:, lanes_of(i)], preferred_element_type=F32
        ).astype(BF16)

    def send_result(i, s):
        res[i, s] = down_rows(i, s)
        remote(res.at[i, s], ret.at[i, g], r_send, r_recv.at[i], s, t).start()

    lax.fori_loop(0, ep, expert_step, 0)

    def down_step(i, carry):
        for p in far:
            send_result(i, partner(g, p, ep))

        @pl.when(i < chunks - half)
        def _():
            for p in near:
                send_result(i + half, partner(g, p, ep))

        return carry

    lax.fori_loop(0, chunks, down_step, 0)

    def pair_copy(i):
        return remote(pair_out.at[i], pair_in.at[i], p_send, p_recv.at[i], g, mate)

    def produce(i):
        others = pl.ds(0, ep - 1)
        remote(res.at[i, others], ret.at[i, others], r_send, r_recv.at[i], g, mate).wait_recv()
        total = jnp.dot(
            spread[...], ret[i].reshape(ep * slots, cols), preferred_element_type=F32
        ) + jnp.dot(shidden[...], sdown_ref[:, lanes_of(i)], preferred_element_type=F32)
        part[i % 2] = total.reshape(part.shape[1:])
        for zz in range(chips):
            pair_out[i, zz] = part[i % 2, zz * 2 + 1 - c].astype(BF16)
        pair_copy(i).start()

    def finish(i):
        pair_copy(i).wait_recv()
        for d in range(1, chips):
            zz = partner(z, d, chips)
            far_out[i, zz] = (part[i % 2, zz * 2 + c] + pair_in[i, zz].astype(F32)).astype(BF16)
            remote(
                far_out.at[i, zz],
                far_in.at[i, z],
                q_send,
                q_recv,
                g,
                zz * 2 + c,
            ).start()
        own[i] = part[i % 2, t] + pair_in[i, z].astype(F32)

    def sum_step(i, carry):
        @pl.when(i < chunks)
        def _():
            produce(i)

        @pl.when(i > 0)
        def _():
            finish(i - 1)

        return carry

    lax.fori_loop(0, chunks + 1, sum_step, 0)

    rest = pl.ds(0, chips - 1)
    remote(far_out.at[:, rest], far_in.at[:, rest], q_send, q_recv, g, mate).wait()

    def out_step(i, carry):
        total = own[i]
        for d in range(1, chips):
            total = total + far_in[i, partner(z, d, chips)].astype(F32)
        out_ref[:, lanes_of(i)] = total.astype(BF16)
        return carry

    lax.fori_loop(0, chunks, out_step, 0)

    others = pl.ds(0, ep - 1)
    remote(sent.at[:, others], inc.at[:, others], b_send, b_recv.at[g], g, mate).wait_send()
    remote(res.at[:, others], ret.at[:, others], r_send, r_recv.at[0], g, mate).wait_send()
    remote(pair_out, pair_in, p_send, p_recv.at[0], g, mate).wait_send()

    def sent_step(chip, carry):
        k = chip * 2 + c
        forward(k).wait_send()

        @pl.when((chip <= z) & (z < chips - 1))
        def _():
            upward(k).wait_send()

        @pl.when((chip >= z) & (z > 0))
        def _():
            downward(k).wait_send()

        return carry

    lax.fori_loop(0, chips, sent_step, 0)


def on_device(
    tokens,
    norm_gain,
    norm_shift,
    expert_ids,
    affinity,
    expert_gate,
    expert_up,
    expert_down,
    shared_gate,
    shared_up,
    shared_down,
):
    ep = lax.axis_size("ep")
    tp = lax.axis_size("tp")
    rows, feat = tokens.shape
    width = feat * tp
    top_count = expert_ids.shape[1]
    block = rows // tp
    expert_count = ep * tp
    slot_cap = max(1, 2 * block * top_count // expert_count)
    slots = tp * slot_cap
    hid = expert_gate.shape[2]
    shared_rows = shared_gate.shape[0]
    cols = 256
    chunks = width // cols
    chips = tp // 2

    vmem = pl.BlockSpec(memory_space=pltpu.VMEM)
    anywhere = pl.BlockSpec(memory_space=pl.ANY)
    dma = pltpu.SemaphoreType.DMA
    return pl.pallas_call(
        functools.partial(layer_kernel, (ep, tp, rows, slots, slot_cap, feat, chunks, cols)),
        out_shape=jax.ShapeDtypeStruct((block, width), BF16),
        in_specs=[anywhere] * 11,
        out_specs=vmem,
        scratch_shapes=[
            pltpu.VMEM((top_count, rows), jnp.int32),
            pltpu.VMEM((top_count, rows), F32),
            pltpu.VMEM((1, width), F32),
            pltpu.VMEM((1, width), F32),
            pltpu.VMEM((shared_rows, width), BF16),
            pltpu.VMEM((shared_rows, width), BF16),
            pltpu.VMEM((width, hid), BF16),
            pltpu.VMEM((width, hid), BF16),
            pltpu.VMEM((hid, width), BF16),
            pltpu.VMEM((shared_rows, width), BF16),
            pltpu.VMEM((tp, rows, feat), BF16),
            pltpu.VMEM((ep, slots, rows), BF16),
            pltpu.VMEM((ep * slots, rows), F32),
            pltpu.VMEM((rows, ep * slots), BF16),
            pltpu.VMEM((tp, ep, slots, feat), BF16),
            pltpu.VMEM((tp, ep, slots, feat), BF16),
            pltpu.VMEM((max(rows, slots), width), BF16),
            pltpu.VMEM((ep, slots, hid), BF16),
            pltpu.VMEM((rows, shared_rows), BF16),
            pltpu.VMEM((chunks, ep, slots, cols), BF16),
            pltpu.VMEM((chunks, ep, slots, cols), BF16),
            pltpu.VMEM((2, tp, block, cols), F32),
            pltpu.VMEM((chunks, block, cols), F32),
            pltpu.VMEM((chunks, chips, block, cols), BF16),
            pltpu.VMEM((chunks, chips, block, cols), BF16),
            pltpu.VMEM((chunks, chips, block, cols), BF16),
            pltpu.VMEM((chunks, chips, block, cols), BF16),
            dma((8,)),
            dma((3,)),
            dma((chips,)),
            dma((chips,)),
            dma((chips,)),
            dma((tp,)),
            dma,
            dma((ep,)),
            dma,
            dma((chunks,)),
            dma,
            dma((chunks,)),
            dma,
            dma,
        ],
        compiler_params=pltpu.CompilerParams(
            collective_id=0, has_side_effects=True, vmem_limit_bytes=56 * 1024 * 1024
        ),
        name="moe_layer",
    )(
        tokens,
        expert_ids.T,
        affinity.T,
        norm_gain.reshape(1, width),
        norm_shift.reshape(1, width),
        shared_gate,
        shared_up,
        expert_gate[0],
        expert_up[0],
        expert_down[0],
        shared_down,
    )


def solution(mesh):
    placed = (
        P("ep", "tp"),
        P(),
        P(),
        P("ep", None),
        P("ep", None),
        P(("ep", "tp"), None, None),
        P(("ep", "tp"), None, None),
        P(("ep", "tp"), None, None),
        P("tp", None),
        P("tp", None),
        P(),
    )
    return jax.shard_map(
        on_device, mesh=mesh, in_specs=placed, out_specs=P(("ep", "tp"), None), check_vma=False
    )
```

```python
import functools
import math

import jax
import jax.numpy as jnp
from jax import lax
from jax.experimental import pallas as pl
from jax.experimental.pallas import tpu as pltpu
from jax.sharding import PartitionSpec as P

ROUTED_SCALE = 2.5
EPSILON = 1e-05
MESH = pl.DeviceIdType.MESH
F32 = jnp.float32
BF16 = jnp.bfloat16


def partner(index, step, count):
    if count & (count - 1):
        return lax.rem(index + step, count)
    result, bit = 0, 1
    while bit < count:
        result = result + ((index // bit) % 2 + (step // bit) % 2) % 2 * bit
        bit *= 2
    return result


def layer_kernel(
    sizes,
    tokens_hbm,
    ids_hbm,
    affinity_hbm,
    gain_hbm,
    shift_hbm,
    sgate_hbm,
    sup_hbm,
    gate_hbm,
    up_hbm,
    down_hbm,
    sdown_hbm,
    out_ref,
    ids_ref,
    affinity_ref,
    gain_ref,
    shift_ref,
    sgate_ref,
    sup_ref,
    gate_ref,
    up_ref,
    down_ref,
    sdown_ref,
    whole,
    pick,
    spread_t,
    spread,
    sent,
    inc,
    norm,
    hidden,
    shidden,
    res,
    ret,
    ids_other,
    extra,
    pick_other,
    part,
    own,
    pair_out,
    pair_in,
    far_out,
    far_in,
    load_sem,
    first_sem,
    u_send,
    d_send,
    f_send,
    a_recv,
    b_send,
    b_recv,
    r_send,
    r_recv,
    p_send,
    p_recv,
    q_send,
    q_recv,
    i_send,
    i_recv,
    x_send,
    x_recv,
    eu_send,
    ed_send,
    ef_send,
    e_recv,
):
    ep, tp, rows, slots, slot_cap, feat, chunks, cols, shift = sizes
    chips = tp // 2
    g = lax.axis_index("ep")
    t = lax.axis_index("tp")
    z = t // 2
    c = t % 2
    mate = z * 2 + 1 - c
    width = tp * feat
    shared_rows = sdown_ref.shape[0]

    firsts = [
        pltpu.make_async_copy(ids_hbm, ids_ref, first_sem.at[0]),
        pltpu.make_async_copy(affinity_hbm, affinity_ref, first_sem.at[1]),
        pltpu.make_async_copy(tokens_hbm, whole.at[t], first_sem.at[2]),
    ]
    loads = [
        pltpu.make_async_copy(gain_hbm, gain_ref, load_sem.at[0]),
        pltpu.make_async_copy(shift_hbm, shift_ref, load_sem.at[1]),
        pltpu.make_async_copy(sgate_hbm, sgate_ref, load_sem.at[2]),
        pltpu.make_async_copy(sup_hbm, sup_ref, load_sem.at[3]),
        pltpu.make_async_copy(
            sdown_hbm.at[pl.ds(pl.multiple_of(t * shared_rows, 8), shared_rows)],
            sdown_ref,
            load_sem.at[4],
        ),
        pltpu.make_async_copy(gate_hbm, gate_ref, load_sem.at[5]),
        pltpu.make_async_copy(up_hbm, up_ref, load_sem.at[6]),
        pltpu.make_async_copy(down_hbm, down_ref, load_sem.at[7]),
    ]
    for load in firsts:
        load.start()

    def remote(src, dst, send, recv, e, k):
        return pltpu.make_async_remote_copy(
            src_ref=src,
            dst_ref=dst,
            send_sem=send,
            recv_sem=recv,
            device_id=(e, k),
            device_id_type=MESH,
        )

    barrier = pltpu.get_barrier_semaphore()
    partners = [(partner(g, p, ep), t) for p in range(1, ep)]
    partners += [(g, partner(z, d, chips) * 2 + c) for d in range(1, chips)]
    partners += [(g, mate)]
    for e, k in partners:
        pl.semaphore_signal(barrier, inc=1, device_id=(e, k), device_id_type=MESH)
    for load in loads:
        load.start()
    for load in firsts[:2]:
        load.wait()
    ids = ids_ref[...]
    affinity = affinity_ref[...]
    weights = affinity / jnp.sum(affinity, axis=0, keepdims=True) * ROUTED_SCALE
    block = rows // tp
    early = lax.broadcasted_iota(jnp.int32, (rows, rows), 0)
    late = lax.broadcasted_iota(jnp.int32, (rows, rows), 1)
    before = jnp.where((early < late) & (early // block == late // block), 1.0, 0.0).astype(BF16)
    hits = [ids == e * tp + t for e in range(ep)]
    chosen = [jnp.sum(jnp.where(hit, 1.0, 0.0), axis=0, keepdims=True) for hit in hits]
    pad = [jnp.zeros((-ep % 16, rows), F32)] if ep % 16 else []
    ranks = jnp.dot(
        jnp.concatenate(chosen + pad, axis=0).astype(BF16), before, preferred_element_type=F32
    ).astype(jnp.int32)
    base = (tp - 1 - lax.broadcasted_iota(jnp.int32, (1, rows), 1) // block) * slot_cap
    line = lax.broadcasted_iota(jnp.int32, (slots, rows), 0)
    for e in range(ep):
        place = jnp.where(chosen[e] > 0.5, base + ranks[e : e + 1, :], -1)
        weight = jnp.sum(jnp.where(hits[e], weights, 0.0), axis=0, keepdims=True)
        pick[e] = jnp.where(line == place, 1.0, 0.0).astype(BF16)
        spread_t[pl.ds(e * slots, slots), :] = jnp.where(line == place, weight, 0.0)
    pl.semaphore_wait(barrier, len(partners))

    def forward(k):
        return remote(whole.at[k], whole.at[k], f_send.at[k // 2], a_recv.at[k], g, mate)

    def upward(k):
        there = lax.rem(z + 1, chips) * 2 + c
        return remote(whole.at[k], whole.at[k], u_send.at[k // 2], a_recv.at[k], g, there)

    def downward(k):
        there = lax.rem(z + chips - 1, chips) * 2 + c
        return remote(whole.at[k], whole.at[k], d_send.at[k // 2], a_recv.at[k], g, there)

    firsts[2].wait()

    @pl.when(z < chips - 1)
    def _():
        upward(t).start()

    @pl.when(z > 0)
    def _():
        downward(t).start()

    forward(t).start()

    crossed = slots - shift * slot_cap
    extra_rows = shift * block

    def ids_copy(p):
        lanes = pl.ds(0, ids_other.shape[2])
        e = partner(g, p, ep)
        return remote(ids_ref.at[:, lanes], ids_other.at[p - 1], i_send, i_recv, e, t)

    def extra_copy(p):
        e = partner(g, p, ep)
        rows_out = whole.at[t, pl.ds(0, extra_rows)]
        return remote(rows_out, extra.at[t, p - 1], x_send, x_recv, e, t)

    def extra_forward(k):
        return remote(extra.at[k], extra.at[k], ef_send.at[k // 2], e_recv.at[k], g, mate)

    def extra_upward(k):
        there = lax.rem(z + 1, chips) * 2 + c
        return remote(extra.at[k], extra.at[k], eu_send.at[k // 2], e_recv.at[k], g, there)

    def extra_downward(k):
        there = lax.rem(z + chips - 1, chips) * 2 + c
        return remote(extra.at[k], extra.at[k], ed_send.at[k // 2], e_recv.at[k], g, there)

    if shift:
        for p in range(1, ep):
            ids_copy(p).start()
            extra_copy(p).start()

    def extra_onward(chip):
        k = chip * 2 + c

        @pl.when((chip <= z) & (z < chips - 1))
        def _():
            extra_upward(k).start()

        @pl.when((chip >= z) & (z > 0))
        def _():
            extra_downward(k).start()

        extra_forward(k).start()

    def pick_others():
        remote(ids_other, ids_other, i_send, i_recv, g, mate).wait_recv()
        lanes = ids_other.shape[2]
        early = lax.broadcasted_iota(jnp.int32, (lanes, lanes), 0)
        late = lax.broadcasted_iota(jnp.int32, (lanes, lanes), 1)
        before = jnp.where((early < late) & (early // block == late // block), 1.0, 0.0)
        chosen = [
            jnp.sum(jnp.where(ids_other[p] == g * tp + t, 1.0, 0.0), axis=0, keepdims=True)
            for p in range(ep - 1)
        ]
        pad = [jnp.zeros((-(ep - 1) % 16, lanes), F32)]
        ranks = jnp.dot(
            jnp.concatenate(chosen + pad, axis=0).astype(BF16),
            before.astype(BF16),
            preferred_element_type=F32,
        ).astype(jnp.int32)
        blocks = lax.broadcasted_iota(jnp.int32, (1, lanes), 1) // block
        base = (shift - 1 - blocks) * slot_cap
        line = lax.broadcasted_iota(jnp.int32, (shift * slot_cap, lanes), 0)
        for p in range(ep - 1):
            named = (chosen[p] > 0.5) & (blocks < shift)
            place = jnp.where(named, base + ranks[p : p + 1, :], -1)
            pick_other[p] = jnp.where(line == place, 1.0, 0.0).astype(BF16)

    near = [p for p in range(1, ep) if not p & (p - 1)]
    far = [p for p in range(1, ep) if p & (p - 1)]
    half = chunks // 8

    def send_rows(k, p):
        e = partner(g, p, ep)
        over = pl.ds(0, crossed)
        remote(sent.at[k, e, over], inc.at[k, g, over], b_send, b_recv.at[g], e, t).start()

    def arrive(chip):
        k = chip * 2 + c
        forward(k).wait_recv()

        @pl.when((chip < z) & (z < chips - 1))
        def _():
            upward(k).start()

        @pl.when((chip > z) & (z > 0))
        def _():
            downward(k).start()

        forward(k).start()

    def distance_step(d, carry):
        def at_side(side):
            chip = z + d * (side * 2 - 1)
            return chip, (chip >= 0) & (chip < chips) & ((d > 0) | (side == 0))

        for side in range(2):
            chip, there = at_side(side)

            @pl.when(there & (d > 0))
            def _():
                arrive(chip)

        def chunk_step(q, carry):
            chip, there = at_side(q % 2)
            lane = q // 2
            k = chip * 2 + lax.rem(c + lane, 2)

            @pl.when(there)
            def _():
                @pl.when(lane > 0)
                def _():
                    forward(k).wait_recv()

                picked = jnp.dot(
                    pick[...].reshape(ep * slots, rows), whole[k], preferred_element_type=F32
                ).astype(BF16)
                sent[k] = picked.reshape(ep, slots, feat)
                inc[k, g] = sent[k, g]
                for p in near:
                    send_rows(k, p)

            return carry

        lax.fori_loop(0, 4, chunk_step, 0)

        def far_step(q, carry):
            chip, there = at_side(q % 2)

            @pl.when(there)
            def _():
                for p in far:
                    send_rows(chip * 2 + lax.rem(c + q // 2, 2), p)

            return carry

        lax.fori_loop(0, 4, far_step, 0)
        if not shift:
            return carry

        @pl.when(d == 0)
        def _():
            remote(extra.at[t], extra.at[t], x_send, x_recv, g, mate).wait_recv()
            extra_onward(z)
            pick_others()

        for side in range(2):
            chip, there = at_side(side)

            @pl.when(there & (d > 0))
            def _():
                extra_forward(chip * 2 + c).wait_recv()
                extra_onward(chip)

        def extra_step(q, carry):
            chip, there = at_side(q % 2)
            lane = q // 2
            k = chip * 2 + lax.rem(c + lane, 2)

            @pl.when(there)
            def _():
                @pl.when(lane > 0)
                def _():
                    extra_forward(k).wait_recv()

                for p in range(1, ep):
                    inc[k, partner(g, p, ep), crossed:slots, :] = jnp.dot(
                        pick_other[p - 1][:, :extra_rows], extra[k, p - 1], preferred_element_type=F32
                    ).astype(BF16)

            return carry

        lax.fori_loop(0, 4, extra_step, 0)
        return carry

    lax.fori_loop(0, chips, distance_step, 0)
    def normalise(read, count):
        tile = math.gcd(64, count)

        def body(i, carry):
            at = pl.ds(pl.multiple_of(i * tile, tile), tile)
            total = jnp.zeros((tile, feat), F32)
            for k in range(tp):
                total = total + read(k, at).astype(F32)
            mean = jnp.sum(total, axis=1, keepdims=True) / width
            total = jnp.zeros((tile, feat), F32)
            for k in range(tp):
                center = read(k, at).astype(F32) - mean
                total = total + center * center
            scale = lax.rsqrt(jnp.sum(total, axis=1, keepdims=True) / width + EPSILON)
            for k in range(tp):
                lanes = slice(k * feat, (k + 1) * feat)
                value = (read(k, at).astype(F32) - mean) * scale
                value = value * gain_ref[:, lanes] + shift_ref[:, lanes]
                norm[at, lanes] = value.astype(BF16)
            return carry

        lax.fori_loop(0, count // tile, body, 0)

    for load in loads:
        load.wait()

    def activate(s):
        normalise(lambda k, at: inc[k, s, at, :], slots)
        got = norm[0:slots, :]
        gate_act = jnp.dot(got, gate_ref[...], preferred_element_type=F32)
        up_act = jnp.dot(got, up_ref[...], preferred_element_type=F32)
        hidden[s] = (jax.nn.silu(gate_act) * up_act).astype(BF16)

    def expert_step(j, carry):
        p = expert_order(j)
        s = partner(g, p, ep)
        over = pl.ds(0, crossed)
        remote(sent.at[:, s, over], inc.at[:, s, over], b_send, b_recv.at[s], s, t).wait_recv()

        activate(s)
        is_near = functools.reduce(jnp.logical_or, [p == n for n in near])

        @pl.when(is_near)
        def _():
            def near_step(i, carry):
                send_result(i, s)
                return carry

            lax.fori_loop(0, half, near_step, 0)

        return carry

    def lanes_of(i):
        return pl.ds(pl.multiple_of(i * cols, cols), cols)

    def down_rows(i, s):
        return jnp.dot(
            hidden[s], down_ref[:, lanes_of(i)], preferred_element_type=F32
        ).astype(BF16)

    def send_result(i, s):
        res[i, s] = down_rows(i, s)
        remote(res.at[i, s], ret.at[i, g], r_send, r_recv.at[i], s, t).start()

    order = near + far

    def expert_order(j):
        return sum(jnp.where(j == n, p, 0) for n, p in enumerate(order))

    lax.fori_loop(0, ep - 1, expert_step, 0)

    def down_step(i, carry):
        for p in far:
            send_result(i, partner(g, p, ep))

        @pl.when(i < chunks - half)
        def _():
            for p in near:
                send_result(i + half, partner(g, p, ep))

        return carry

    lax.fori_loop(0, chunks, down_step, 0)
    activate(g)

    def own_step(i, carry):
        ret[i, g] = down_rows(i, g)
        return carry

    lax.fori_loop(0, chunks, own_step, 0)
    spread[...] = spread_t[...].T.astype(BF16)
    normalise(lambda k, at: whole[k, at, :], rows)
    contract = (((1,), (1,)), ((), ()))
    sg = lax.dot_general(norm[...], sgate_ref[...], contract, preferred_element_type=F32)
    su = lax.dot_general(norm[...], sup_ref[...], contract, preferred_element_type=F32)
    shidden[...] = (jax.nn.silu(sg) * su).astype(BF16)


    def pair_copy(i):
        return remote(pair_out.at[i], pair_in.at[i], p_send, p_recv.at[i], g, mate)

    def produce(i):
        others = pl.ds(0, ep - 1)
        remote(res.at[i, others], ret.at[i, others], r_send, r_recv.at[i], g, mate).wait_recv()
        total = jnp.dot(
            spread[...], ret[i].reshape(ep * slots, cols), preferred_element_type=F32
        ) + jnp.dot(shidden[...], sdown_ref[:, lanes_of(i)], preferred_element_type=F32)
        part[i % 2] = total.reshape(part.shape[1:])
        for zz in range(chips):
            pair_out[i, zz] = part[i % 2, zz * 2 + 1 - c].astype(BF16)
        pair_copy(i).start()

    def finish(i):
        pair_copy(i).wait_recv()
        for d in range(1, chips):
            zz = partner(z, d, chips)
            far_out[i, zz] = (part[i % 2, zz * 2 + c] + pair_in[i, zz].astype(F32)).astype(BF16)
            remote(
                far_out.at[i, zz],
                far_in.at[i, z],
                q_send,
                q_recv,
                g,
                zz * 2 + c,
            ).start()
        own[i] = part[i % 2, t] + pair_in[i, z].astype(F32)

    def sum_step(i, carry):
        @pl.when(i < chunks)
        def _():
            produce(i)

        @pl.when(i > 0)
        def _():
            finish(i - 1)

        return carry

    lax.fori_loop(0, chunks + 1, sum_step, 0)

    rest = pl.ds(0, chips - 1)
    remote(far_out.at[:, rest], far_in.at[:, rest], q_send, q_recv, g, mate).wait()

    def out_step(i, carry):
        total = own[i]
        for d in range(1, chips):
            total = total + far_in[i, partner(z, d, chips)].astype(F32)
        out_ref[:, lanes_of(i)] = total.astype(BF16)
        return carry

    lax.fori_loop(0, chunks, out_step, 0)

    others = pl.ds(0, ep - 1)
    over = pl.ds(0, crossed)
    remote(
        sent.at[:, others, over], inc.at[:, others, over], b_send, b_recv.at[g], g, mate
    ).wait_send()
    remote(res.at[:, others], ret.at[:, others], r_send, r_recv.at[0], g, mate).wait_send()
    remote(pair_out, pair_in, p_send, p_recv.at[0], g, mate).wait_send()

    def sent_step(chip, carry):
        k = chip * 2 + c
        forward(k).wait_send()

        @pl.when((chip <= z) & (z < chips - 1))
        def _():
            upward(k).wait_send()

        @pl.when((chip >= z) & (z > 0))
        def _():
            downward(k).wait_send()

        if not shift:
            return carry
        extra_forward(k).wait_send()

        @pl.when((chip <= z) & (z < chips - 1))
        def _():
            extra_upward(k).wait_send()

        @pl.when((chip >= z) & (z > 0))
        def _():
            extra_downward(k).wait_send()

        return carry

    lax.fori_loop(0, chips, sent_step, 0)
    if shift:
        remote(ids_other, ids_other, i_send, i_recv, g, mate).wait_send()
        remote(extra.at[t], extra.at[t], x_send, x_recv, g, mate).wait_send()


def on_device(
    tokens,
    norm_gain,
    norm_shift,
    expert_ids,
    affinity,
    expert_gate,
    expert_up,
    expert_down,
    shared_gate,
    shared_up,
    shared_down,
):
    ep = lax.axis_size("ep")
    tp = lax.axis_size("tp")
    rows, feat = tokens.shape
    width = feat * tp
    top_count = expert_ids.shape[1]
    block = rows // tp
    expert_count = ep * tp
    slot_cap = max(1, 2 * block * top_count // expert_count)
    slots = tp * slot_cap
    hid = expert_gate.shape[2]
    shared_rows = shared_gate.shape[0]
    cols = 256
    chunks = width // cols
    chips = tp // 2
    shift = max(1, tp // 8)
    fits = (ep & (ep - 1)) == 0 and ep > 1 and slot_cap % 8 == 0 and block % 8 == 0
    if not fits or shift * block > 128 or rows < 128 or feat != cols:
        shift = 0
    lanes = min(rows, 128)

    vmem = pl.BlockSpec(memory_space=pltpu.VMEM)
    anywhere = pl.BlockSpec(memory_space=pl.ANY)
    dma = pltpu.SemaphoreType.DMA
    return pl.pallas_call(
        functools.partial(layer_kernel, (ep, tp, rows, slots, slot_cap, feat, chunks, cols, shift)),
        out_shape=jax.ShapeDtypeStruct((block, width), BF16),
        in_specs=[anywhere] * 11,
        out_specs=vmem,
        scratch_shapes=[
            pltpu.VMEM((top_count, rows), jnp.int32),
            pltpu.VMEM((top_count, rows), F32),
            pltpu.VMEM((1, width), F32),
            pltpu.VMEM((1, width), F32),
            pltpu.VMEM((shared_rows, width), BF16),
            pltpu.VMEM((shared_rows, width), BF16),
            pltpu.VMEM((width, hid), BF16),
            pltpu.VMEM((width, hid), BF16),
            pltpu.VMEM((hid, width), BF16),
            pltpu.VMEM((shared_rows, width), BF16),
            pltpu.VMEM((tp, rows, feat), BF16),
            pltpu.VMEM((ep, slots, rows), BF16),
            pltpu.VMEM((ep * slots, rows), F32),
            pltpu.VMEM((rows, ep * slots), BF16),
            pltpu.VMEM((tp, ep, slots, feat), BF16),
            pltpu.VMEM((tp, ep, slots, feat), BF16),
            pltpu.VMEM((max(rows, slots), width), BF16),
            pltpu.VMEM((ep, slots, hid), BF16),
            pltpu.VMEM((rows, shared_rows), BF16),
            pltpu.VMEM((chunks, ep, slots, cols), BF16),
            pltpu.VMEM((chunks, ep, slots, cols), BF16),
            pltpu.VMEM((ep - 1, top_count, lanes), jnp.int32),
            pltpu.VMEM((tp, ep - 1, max(8, shift * block), feat), BF16),
            pltpu.VMEM((ep - 1, max(8, shift * slot_cap), lanes), BF16),
            pltpu.VMEM((2, tp, block, cols), F32),
            pltpu.VMEM((chunks, block, cols), F32),
            pltpu.VMEM((chunks, chips, block, cols), BF16),
            pltpu.VMEM((chunks, chips, block, cols), BF16),
            pltpu.VMEM((chunks, chips, block, cols), BF16),
            pltpu.VMEM((chunks, chips, block, cols), BF16),
            dma((8,)),
            dma((3,)),
            dma((chips,)),
            dma((chips,)),
            dma((chips,)),
            dma((tp,)),
            dma,
            dma((ep,)),
            dma,
            dma((chunks,)),
            dma,
            dma((chunks,)),
            dma,
            dma,
            dma,
            dma,
            dma,
            dma,
            dma((chips,)),
            dma((chips,)),
            dma((chips,)),
            dma((tp,)),
        ],
        compiler_params=pltpu.CompilerParams(
            collective_id=0, has_side_effects=True, vmem_limit_bytes=56 * 1024 * 1024
        ),
        name="moe_layer",
    )(
        tokens,
        expert_ids.T,
        affinity.T,
        norm_gain.reshape(1, width),
        norm_shift.reshape(1, width),
        shared_gate,
        shared_up,
        expert_gate[0],
        expert_up[0],
        expert_down[0],
        shared_down,
    )


def solution(mesh):
    placed = (
        P("ep", "tp"),
        P(),
        P(),
        P("ep", None),
        P("ep", None),
        P(("ep", "tp"), None, None),
        P(("ep", "tp"), None, None),
        P(("ep", "tp"), None, None),
        P("tp", None),
        P("tp", None),
        P(),
    )
    return jax.shard_map(
        on_device, mesh=mesh, in_specs=placed, out_specs=P(("ep", "tp"), None), check_vma=False
    )
```

```python
import functools
import math

import jax
import jax.numpy as jnp
from jax import lax
from jax.experimental import pallas as pl
from jax.experimental.pallas import tpu as pltpu
from jax.sharding import PartitionSpec as P

ROUTED_SCALE = 2.5
EPSILON = 1e-05
MESH = pl.DeviceIdType.MESH
F32 = jnp.float32
BF16 = jnp.bfloat16


def partner(index, step, count):
    if count & (count - 1):
        return lax.rem(index + step, count)
    result, bit = 0, 1
    while bit < count:
        result = result + ((index // bit) % 2 + (step // bit) % 2) % 2 * bit
        bit *= 2
    return result


def layer_kernel(
    sizes,
    tokens_hbm,
    ids_hbm,
    affinity_hbm,
    gain_hbm,
    shift_hbm,
    sgate_hbm,
    sup_hbm,
    gate_hbm,
    up_hbm,
    down_hbm,
    sdown_hbm,
    out_ref,
    ids_ref,
    affinity_ref,
    gain_ref,
    shift_ref,
    sgate_ref,
    sup_ref,
    gate_ref,
    up_ref,
    down_ref,
    sdown_ref,
    whole,
    pick,
    spread_t,
    spread,
    sent,
    inc,
    norm,
    hidden,
    shidden,
    res,
    ret,
    ids_other,
    extra,
    pick_other,
    part,
    own,
    pair_out,
    pair_in,
    far_out,
    far_in,
    load_sem,
    first_sem,
    u_send,
    d_send,
    f_send,
    a_recv,
    b_send,
    b_recv,
    r_send,
    r_recv,
    p_send,
    p_recv,
    q_send,
    q_recv,
    i_send,
    i_recv,
    x_send,
    x_recv,
    eu_send,
    ed_send,
    ef_send,
    e_recv,
):
    ep, tp, rows, slots, slot_cap, feat, chunks, cols, shift = sizes
    chips = tp // 2
    g = lax.axis_index("ep")
    t = lax.axis_index("tp")
    z = t // 2
    c = t % 2
    mate = z * 2 + 1 - c
    width = tp * feat
    shared_rows = sdown_ref.shape[0]

    firsts = [
        pltpu.make_async_copy(ids_hbm, ids_ref, first_sem.at[0]),
        pltpu.make_async_copy(affinity_hbm, affinity_ref, first_sem.at[1]),
        pltpu.make_async_copy(tokens_hbm, whole.at[t], first_sem.at[2]),
    ]
    loads = [
        pltpu.make_async_copy(gain_hbm, gain_ref, load_sem.at[0]),
        pltpu.make_async_copy(shift_hbm, shift_ref, load_sem.at[1]),
        pltpu.make_async_copy(sgate_hbm, sgate_ref, load_sem.at[2]),
        pltpu.make_async_copy(sup_hbm, sup_ref, load_sem.at[3]),
        pltpu.make_async_copy(
            sdown_hbm.at[pl.ds(pl.multiple_of(t * shared_rows, 8), shared_rows)],
            sdown_ref,
            load_sem.at[4],
        ),
        pltpu.make_async_copy(gate_hbm, gate_ref, load_sem.at[5]),
        pltpu.make_async_copy(up_hbm, up_ref, load_sem.at[6]),
        pltpu.make_async_copy(down_hbm, down_ref, load_sem.at[7]),
    ]
    for load in firsts:
        load.start()

    def remote(src, dst, send, recv, e, k):
        return pltpu.make_async_remote_copy(
            src_ref=src,
            dst_ref=dst,
            send_sem=send,
            recv_sem=recv,
            device_id=(e, k),
            device_id_type=MESH,
        )

    barrier = pltpu.get_barrier_semaphore()
    partners = [(partner(g, p, ep), t) for p in range(1, ep)]
    partners += [(g, partner(z, d, chips) * 2 + c) for d in range(1, chips)]
    partners += [(g, mate)]
    for e, k in partners:
        pl.semaphore_signal(barrier, inc=1, device_id=(e, k), device_id_type=MESH)
    for load in loads:
        load.start()
    for load in firsts[:2]:
        load.wait()
    ids = ids_ref[...]
    affinity = affinity_ref[...]
    weights = affinity / jnp.sum(affinity, axis=0, keepdims=True) * ROUTED_SCALE
    block = rows // tp
    early = lax.broadcasted_iota(jnp.int32, (rows, rows), 0)
    late = lax.broadcasted_iota(jnp.int32, (rows, rows), 1)
    before = jnp.where((early < late) & (early // block == late // block), 1.0, 0.0).astype(BF16)
    hits = [ids == e * tp + t for e in range(ep)]
    chosen = [jnp.sum(jnp.where(hit, 1.0, 0.0), axis=0, keepdims=True) for hit in hits]
    pad = [jnp.zeros((-ep % 16, rows), F32)] if ep % 16 else []
    ranks = jnp.dot(
        jnp.concatenate(chosen + pad, axis=0).astype(BF16), before, preferred_element_type=F32
    ).astype(jnp.int32)
    base = (tp - 1 - lax.broadcasted_iota(jnp.int32, (1, rows), 1) // block) * slot_cap
    line = lax.broadcasted_iota(jnp.int32, (slots, rows), 0)
    for e in range(ep):
        place = jnp.where(chosen[e] > 0.5, base + ranks[e : e + 1, :], -1)
        weight = jnp.sum(jnp.where(hits[e], weights, 0.0), axis=0, keepdims=True)
        pick[e] = jnp.where(line == place, 1.0, 0.0).astype(BF16)
        spread_t[pl.ds(e * slots, slots), :] = jnp.where(line == place, weight, 0.0)
    pl.semaphore_wait(barrier, len(partners))

    def forward(k):
        return remote(whole.at[k], whole.at[k], f_send.at[k // 2], a_recv.at[k], g, mate)

    def upward(k):
        there = lax.rem(z + 1, chips) * 2 + c
        return remote(whole.at[k], whole.at[k], u_send.at[k // 2], a_recv.at[k], g, there)

    def downward(k):
        there = lax.rem(z + chips - 1, chips) * 2 + c
        return remote(whole.at[k], whole.at[k], d_send.at[k // 2], a_recv.at[k], g, there)

    firsts[2].wait()

    @pl.when(z < chips - 1)
    def _():
        upward(t).start()

    @pl.when(z > 0)
    def _():
        downward(t).start()

    forward(t).start()

    crossed = slots - shift * slot_cap
    extra_rows = shift * block

    def ids_copy(p):
        lanes = pl.ds(0, ids_other.shape[2])
        e = partner(g, p, ep)
        return remote(ids_ref.at[:, lanes], ids_other.at[p - 1], i_send, i_recv, e, t)

    def extra_copy(p):
        e = partner(g, p, ep)
        rows_out = whole.at[t, pl.ds(0, extra_rows)]
        return remote(rows_out, extra.at[t, p - 1], x_send, x_recv, e, t)

    def extra_forward(k):
        return remote(extra.at[k], extra.at[k], ef_send.at[k // 2], e_recv.at[k], g, mate)

    def extra_upward(k):
        there = lax.rem(z + 1, chips) * 2 + c
        return remote(extra.at[k], extra.at[k], eu_send.at[k // 2], e_recv.at[k], g, there)

    def extra_downward(k):
        there = lax.rem(z + chips - 1, chips) * 2 + c
        return remote(extra.at[k], extra.at[k], ed_send.at[k // 2], e_recv.at[k], g, there)

    if shift:
        for p in range(1, ep):
            ids_copy(p).start()
            extra_copy(p).start()

    def extra_onward(chip):
        k = chip * 2 + c

        @pl.when((chip <= z) & (z < chips - 1))
        def _():
            extra_upward(k).start()

        @pl.when((chip >= z) & (z > 0))
        def _():
            extra_downward(k).start()

        extra_forward(k).start()

    def pick_others():
        remote(ids_other, ids_other, i_send, i_recv, g, mate).wait_recv()
        lanes = ids_other.shape[2]
        early = lax.broadcasted_iota(jnp.int32, (lanes, lanes), 0)
        late = lax.broadcasted_iota(jnp.int32, (lanes, lanes), 1)
        before = jnp.where((early < late) & (early // block == late // block), 1.0, 0.0)
        chosen = [
            jnp.sum(jnp.where(ids_other[p] == g * tp + t, 1.0, 0.0), axis=0, keepdims=True)
            for p in range(ep - 1)
        ]
        pad = [jnp.zeros((-(ep - 1) % 16, lanes), F32)]
        ranks = jnp.dot(
            jnp.concatenate(chosen + pad, axis=0).astype(BF16),
            before.astype(BF16),
            preferred_element_type=F32,
        ).astype(jnp.int32)
        blocks = lax.broadcasted_iota(jnp.int32, (1, lanes), 1) // block
        base = (shift - 1 - blocks) * slot_cap
        line = lax.broadcasted_iota(jnp.int32, (shift * slot_cap, lanes), 0)
        for p in range(ep - 1):
            named = (chosen[p] > 0.5) & (blocks < shift)
            place = jnp.where(named, base + ranks[p : p + 1, :], -1)
            pick_other[p] = jnp.where(line == place, 1.0, 0.0).astype(BF16)

    near = [p for p in range(1, ep) if not p & (p - 1)]
    far = [p for p in range(1, ep) if p & (p - 1)]
    half = chunks * 1 // 8

    def send_rows(k, p):
        e = partner(g, p, ep)
        over = pl.ds(0, crossed)
        remote(sent.at[k, e, over], inc.at[k, g, over], b_send, b_recv.at[g], e, t).start()

    def arrive(chip):
        k = chip * 2 + c
        forward(k).wait_recv()

        @pl.when((chip < z) & (z < chips - 1))
        def _():
            upward(k).start()

        @pl.when((chip > z) & (z > 0))
        def _():
            downward(k).start()

        forward(k).start()

    def distance_step(d, carry):
        def at_side(side):
            chip = z + d * (side * 2 - 1)
            return chip, (chip >= 0) & (chip < chips) & ((d > 0) | (side == 0))

        for side in range(2):
            chip, there = at_side(side)

            @pl.when(there & (d > 0))
            def _():
                arrive(chip)

        def chunk_step(q, carry):
            chip, there = at_side(q % 2)
            lane = q // 2
            k = chip * 2 + lax.rem(c + lane, 2)

            @pl.when(there)
            def _():
                @pl.when(lane > 0)
                def _():
                    forward(k).wait_recv()

                picked = jnp.dot(
                    pick[...].reshape(ep * slots, rows), whole[k], preferred_element_type=F32
                ).astype(BF16)
                sent[k] = picked.reshape(ep, slots, feat)
                inc[k, g] = sent[k, g]
                for p in near:
                    send_rows(k, p)

            return carry

        lax.fori_loop(0, 4, chunk_step, 0)

        def far_step(q, carry):
            chip, there = at_side(q % 2)

            @pl.when(there)
            def _():
                for p in far:
                    send_rows(chip * 2 + lax.rem(c + q // 2, 2), p)

            return carry

        lax.fori_loop(0, 4, far_step, 0)
        if not shift:
            return carry

        @pl.when(d == 0)
        def _():
            remote(extra.at[t], extra.at[t], x_send, x_recv, g, mate).wait_recv()
            extra_onward(z)
            pick_others()

        for side in range(2):
            chip, there = at_side(side)

            @pl.when(there & (d > 0))
            def _():
                extra_forward(chip * 2 + c).wait_recv()
                extra_onward(chip)

        def extra_step(q, carry):
            chip, there = at_side(q % 2)
            lane = q // 2
            k = chip * 2 + lax.rem(c + lane, 2)

            @pl.when(there)
            def _():
                @pl.when(lane > 0)
                def _():
                    extra_forward(k).wait_recv()

                for p in range(1, ep):
                    inc[k, partner(g, p, ep), crossed:slots, :] = jnp.dot(
                        pick_other[p - 1][:, :extra_rows], extra[k, p - 1], preferred_element_type=F32
                    ).astype(BF16)

            return carry

        lax.fori_loop(0, 4, extra_step, 0)
        return carry

    lax.fori_loop(0, chips, distance_step, 0)
    def normalise(read, count):
        tile = math.gcd(64, count)

        def body(i, carry):
            at = pl.ds(pl.multiple_of(i * tile, tile), tile)
            total = jnp.zeros((tile, feat), F32)
            for k in range(tp):
                total = total + read(k, at).astype(F32)
            mean = jnp.sum(total, axis=1, keepdims=True) / width
            total = jnp.zeros((tile, feat), F32)
            for k in range(tp):
                center = read(k, at).astype(F32) - mean
                total = total + center * center
            scale = lax.rsqrt(jnp.sum(total, axis=1, keepdims=True) / width + EPSILON)
            for k in range(tp):
                lanes = slice(k * feat, (k + 1) * feat)
                value = (read(k, at).astype(F32) - mean) * scale
                value = value * gain_ref[:, lanes] + shift_ref[:, lanes]
                norm[at, lanes] = value.astype(BF16)
            return carry

        lax.fori_loop(0, count // tile, body, 0)

    for load in loads:
        load.wait()

    def activate(s):
        normalise(lambda k, at: inc[k, s, at, :], slots)
        got = norm[0:slots, :]
        gate_act = jnp.dot(got, gate_ref[...], preferred_element_type=F32)
        up_act = jnp.dot(got, up_ref[...], preferred_element_type=F32)
        hidden[s] = (jax.nn.silu(gate_act) * up_act).astype(BF16)

    def expert_step(j, carry):
        p = expert_order(j)
        s = partner(g, p, ep)
        over = pl.ds(0, crossed)
        remote(sent.at[:, s, over], inc.at[:, s, over], b_send, b_recv.at[s], s, t).wait_recv()

        activate(s)
        is_near = functools.reduce(jnp.logical_or, [p == n for n in near])

        @pl.when(is_near)
        def _():
            def near_step(i, carry):
                send_result(i, s)
                return carry

            lax.fori_loop(0, half, near_step, 0)

        return carry

    def lanes_of(i):
        return pl.ds(pl.multiple_of(i * cols, cols), cols)

    def down_rows(i, s):
        return jnp.dot(
            hidden[s], down_ref[:, lanes_of(i)], preferred_element_type=F32
        ).astype(BF16)

    def send_result(i, s):
        res[i, s] = down_rows(i, s)
        remote(res.at[i, s], ret.at[i, g], r_send, r_recv.at[i], s, t).start()

    normalise(lambda k, at: whole[k, at, :], rows)
    contract = (((1,), (1,)), ((), ()))
    sg = lax.dot_general(norm[...], sgate_ref[...], contract, preferred_element_type=F32)
    su = lax.dot_general(norm[...], sup_ref[...], contract, preferred_element_type=F32)
    shidden[...] = (jax.nn.silu(sg) * su).astype(BF16)

    spread[...] = spread_t[...].T.astype(BF16)
    order = near + far

    def expert_order(j):
        return sum(jnp.where(j == n, p, 0) for n, p in enumerate(order))

    lax.fori_loop(0, ep - 1, expert_step, 0)

    def down_step(i, carry):
        for p in far:
            send_result(i, partner(g, p, ep))

        @pl.when(i < chunks - half)
        def _():
            for p in near:
                send_result(i + half, partner(g, p, ep))

        return carry

    lax.fori_loop(0, chunks, down_step, 0)
    activate(g)

    def own_step(i, carry):
        ret[i, g] = down_rows(i, g)
        return carry

    lax.fori_loop(0, chunks, own_step, 0)
    def pair_copy(i):
        return remote(pair_out.at[i], pair_in.at[i], p_send, p_recv.at[i], g, mate)

    def produce(i):
        others = pl.ds(0, ep - 1)
        remote(res.at[i, others], ret.at[i, others], r_send, r_recv.at[i], g, mate).wait_recv()
        total = jnp.dot(
            spread[...], ret[i].reshape(ep * slots, cols), preferred_element_type=F32
        ) + jnp.dot(shidden[...], sdown_ref[:, lanes_of(i)], preferred_element_type=F32)
        part[i % 2] = total.reshape(part.shape[1:])
        for zz in range(chips):
            pair_out[i, zz] = part[i % 2, zz * 2 + 1 - c].astype(BF16)
        pair_copy(i).start()

    def finish(i):
        pair_copy(i).wait_recv()
        for d in range(1, chips):
            zz = partner(z, d, chips)
            far_out[i, zz] = (part[i % 2, zz * 2 + c] + pair_in[i, zz].astype(F32)).astype(BF16)
            remote(
                far_out.at[i, zz],
                far_in.at[i, z],
                q_send,
                q_recv,
                g,
                zz * 2 + c,
            ).start()
        own[i] = part[i % 2, t] + pair_in[i, z].astype(F32)

    def sum_step(i, carry):
        produce(i)
        finish(i)
        return carry

    lax.fori_loop(0, chunks, sum_step, 0)

    rest = pl.ds(0, chips - 1)
    remote(far_out.at[:, rest], far_in.at[:, rest], q_send, q_recv, g, mate).wait()

    def out_step(i, carry):
        total = own[i]
        for d in range(1, chips):
            total = total + far_in[i, partner(z, d, chips)].astype(F32)
        out_ref[:, lanes_of(i)] = total.astype(BF16)
        return carry

    lax.fori_loop(0, chunks, out_step, 0)

    others = pl.ds(0, ep - 1)
    over = pl.ds(0, crossed)
    remote(
        sent.at[:, others, over], inc.at[:, others, over], b_send, b_recv.at[g], g, mate
    ).wait_send()
    remote(res.at[:, others], ret.at[:, others], r_send, r_recv.at[0], g, mate).wait_send()
    remote(pair_out, pair_in, p_send, p_recv.at[0], g, mate).wait_send()

    def sent_step(chip, carry):
        k = chip * 2 + c
        forward(k).wait_send()

        @pl.when((chip <= z) & (z < chips - 1))
        def _():
            upward(k).wait_send()

        @pl.when((chip >= z) & (z > 0))
        def _():
            downward(k).wait_send()

        if not shift:
            return carry
        extra_forward(k).wait_send()

        @pl.when((chip <= z) & (z < chips - 1))
        def _():
            extra_upward(k).wait_send()

        @pl.when((chip >= z) & (z > 0))
        def _():
            extra_downward(k).wait_send()

        return carry

    lax.fori_loop(0, chips, sent_step, 0)
    if shift:
        remote(ids_other, ids_other, i_send, i_recv, g, mate).wait_send()
        remote(extra.at[t], extra.at[t], x_send, x_recv, g, mate).wait_send()


def on_device(
    tokens,
    norm_gain,
    norm_shift,
    expert_ids,
    affinity,
    expert_gate,
    expert_up,
    expert_down,
    shared_gate,
    shared_up,
    shared_down,
):
    ep = lax.axis_size("ep")
    tp = lax.axis_size("tp")
    rows, feat = tokens.shape
    width = feat * tp
    top_count = expert_ids.shape[1]
    block = rows // tp
    expert_count = ep * tp
    slot_cap = max(1, 2 * block * top_count // expert_count)
    slots = tp * slot_cap
    hid = expert_gate.shape[2]
    shared_rows = shared_gate.shape[0]
    cols = 256
    chunks = width // cols
    chips = tp // 2
    shift = max(1, tp // 8)
    fits = (ep & (ep - 1)) == 0 and ep > 1 and slot_cap % 8 == 0 and block % 8 == 0
    if not fits or shift * block > 128 or rows < 128 or feat != cols:
        shift = 0
    lanes = min(rows, 128)

    vmem = pl.BlockSpec(memory_space=pltpu.VMEM)
    anywhere = pl.BlockSpec(memory_space=pl.ANY)
    dma = pltpu.SemaphoreType.DMA
    return pl.pallas_call(
        functools.partial(layer_kernel, (ep, tp, rows, slots, slot_cap, feat, chunks, cols, shift)),
        out_shape=pltpu.VMEM((block, width), BF16),
        in_specs=[anywhere] * 11,
        out_specs=vmem,
        scratch_shapes=[
            pltpu.VMEM((top_count, rows), jnp.int32),
            pltpu.VMEM((top_count, rows), F32),
            pltpu.VMEM((1, width), F32),
            pltpu.VMEM((1, width), F32),
            pltpu.VMEM((shared_rows, width), BF16),
            pltpu.VMEM((shared_rows, width), BF16),
            pltpu.VMEM((width, hid), BF16),
            pltpu.VMEM((width, hid), BF16),
            pltpu.VMEM((hid, width), BF16),
            pltpu.VMEM((shared_rows, width), BF16),
            pltpu.VMEM((tp, rows, feat), BF16),
            pltpu.VMEM((ep, slots, rows), BF16),
            pltpu.VMEM((ep * slots, rows), F32),
            pltpu.VMEM((rows, ep * slots), BF16),
            pltpu.VMEM((tp, ep, slots, feat), BF16),
            pltpu.VMEM((tp, ep, slots, feat), BF16),
            pltpu.VMEM((max(rows, slots), width), BF16),
            pltpu.VMEM((ep, slots, hid), BF16),
            pltpu.VMEM((rows, shared_rows), BF16),
            pltpu.VMEM((chunks, ep, slots, cols), BF16),
            pltpu.VMEM((chunks, ep, slots, cols), BF16),
            pltpu.VMEM((ep - 1, top_count, lanes), jnp.int32),
            pltpu.VMEM((tp, ep - 1, max(8, shift * block), feat), BF16),
            pltpu.VMEM((ep - 1, max(8, shift * slot_cap), lanes), BF16),
            pltpu.VMEM((2, tp, block, cols), F32),
            pltpu.VMEM((chunks, block, cols), F32),
            pltpu.VMEM((chunks, chips, block, cols), BF16),
            pltpu.VMEM((chunks, chips, block, cols), BF16),
            pltpu.VMEM((chunks, chips, block, cols), BF16),
            pltpu.VMEM((chunks, chips, block, cols), BF16),
            dma((8,)),
            dma((3,)),
            dma((chips,)),
            dma((chips,)),
            dma((chips,)),
            dma((tp,)),
            dma,
            dma((ep,)),
            dma,
            dma((chunks,)),
            dma,
            dma((chunks,)),
            dma,
            dma,
            dma,
            dma,
            dma,
            dma,
            dma((chips,)),
            dma((chips,)),
            dma((chips,)),
            dma((tp,)),
        ],
        compiler_params=pltpu.CompilerParams(
            collective_id=0, has_side_effects=True, vmem_limit_bytes=56 * 1024 * 1024
        ),
        name="moe_layer",
    )(
        tokens,
        expert_ids.T,
        affinity.T,
        norm_gain.reshape(1, width),
        norm_shift.reshape(1, width),
        shared_gate,
        shared_up,
        expert_gate[0],
        expert_up[0],
        expert_down[0],
        shared_down,
    )


def solution(mesh):
    placed = (
        P("ep", "tp"),
        P(),
        P(),
        P("ep", None),
        P("ep", None),
        P(("ep", "tp"), None, None),
        P(("ep", "tp"), None, None),
        P(("ep", "tp"), None, None),
        P("tp", None),
        P("tp", None),
        P(),
    )
    return jax.shard_map(
        on_device, mesh=mesh, in_specs=placed, out_specs=P(("ep", "tp"), None), check_vma=False
    )
```

```python
import functools
import math

import jax
import jax.numpy as jnp
from jax import lax
from jax.experimental import pallas as pl
from jax.experimental.pallas import tpu as pltpu
from jax.sharding import PartitionSpec as P

ROUTED_SCALE = 2.5
EPSILON = 1e-05
MESH = pl.DeviceIdType.MESH
F32 = jnp.float32
BF16 = jnp.bfloat16


def partner(index, step, count):
    if count & (count - 1):
        return lax.rem(index + step, count)
    result, bit = 0, 1
    while bit < count:
        result = result + ((index // bit) % 2 + (step // bit) % 2) % 2 * bit
        bit *= 2
    return result


def layer_kernel(
    sizes,
    tokens_hbm,
    ids_hbm,
    affinity_hbm,
    gain_hbm,
    shift_hbm,
    sgate_hbm,
    sup_hbm,
    gate_hbm,
    up_hbm,
    down_hbm,
    sdown_hbm,
    out_ref,
    ids_ref,
    affinity_ref,
    gain_ref,
    shift_ref,
    sgate_ref,
    sup_ref,
    gate_ref,
    up_ref,
    down_ref,
    sdown_ref,
    whole,
    pick,
    spread_t,
    spread,
    sent,
    inc,
    norm,
    hidden,
    shidden,
    res,
    ret,
    ids_other,
    extra,
    pick_other,
    affinity_other,
    turn_weight,
    turn_hidden,
    mine,
    t_out,
    t_in,
    line_out,
    line_in,
    y_out,
    y_in,
    part,
    own,
    pair_out,
    pair_in,
    far_out,
    far_in,
    relay,
    load_sem,
    first_sem,
    u_send,
    d_send,
    f_send,
    a_recv,
    b_send,
    b_recv,
    r_send,
    r_recv,
    p_send,
    p_recv,
    q_send,
    q_recv,
    o_send,
    o_recv,
    i_send,
    i_recv,
    x_send,
    x_recv,
    eu_send,
    ed_send,
    ef_send,
    e_recv,
    w_send,
    w_recv,
    t_send,
    t_recv,
    l_send,
    l_recv,
    y_send,
    y_recv,
):
    ep, tp, rows, slots, slot_cap, feat, chunks, cols, shift, turn = sizes
    paired = tp == 8 and turn > 0
    chips = tp // 2
    g = lax.axis_index("ep")
    t = lax.axis_index("tp")
    z = t // 2
    c = t % 2
    mate = z * 2 + 1 - c
    width = tp * feat
    shared_rows = sdown_ref.shape[0]

    firsts = [
        pltpu.make_async_copy(ids_hbm, ids_ref, first_sem.at[0]),
        pltpu.make_async_copy(affinity_hbm, affinity_ref, first_sem.at[1]),
        pltpu.make_async_copy(tokens_hbm, whole.at[t], first_sem.at[2]),
    ]
    loads = [
        pltpu.make_async_copy(gain_hbm, gain_ref, load_sem.at[0]),
        pltpu.make_async_copy(shift_hbm, shift_ref, load_sem.at[1]),
        pltpu.make_async_copy(sgate_hbm, sgate_ref, load_sem.at[2]),
        pltpu.make_async_copy(sup_hbm, sup_ref, load_sem.at[3]),
        pltpu.make_async_copy(
            sdown_hbm.at[pl.ds(pl.multiple_of(t * shared_rows, 8), shared_rows)],
            sdown_ref,
            load_sem.at[4],
        ),
        pltpu.make_async_copy(gate_hbm, gate_ref, load_sem.at[5]),
        pltpu.make_async_copy(up_hbm, up_ref, load_sem.at[6]),
        pltpu.make_async_copy(down_hbm, down_ref, load_sem.at[7]),
    ]
    for load in firsts:
        load.start()

    def remote(src, dst, send, recv, e, k):
        return pltpu.make_async_remote_copy(
            src_ref=src,
            dst_ref=dst,
            send_sem=send,
            recv_sem=recv,
            device_id=(e, k),
            device_id_type=MESH,
        )

    barrier = pltpu.get_barrier_semaphore()
    partners = [(partner(g, p, ep), t) for p in range(1, ep)]
    partners += [(g, partner(z, d, chips) * 2 + c) for d in range(1, chips)]
    partners += [(g, mate)]
    for e, k in partners:
        pl.semaphore_signal(barrier, inc=1, device_id=(e, k), device_id_type=MESH)
    for load in loads:
        load.start()
    for load in firsts[:2]:
        load.wait()
    ids = ids_ref[...]
    affinity = affinity_ref[...]
    weights = affinity / jnp.sum(affinity, axis=0, keepdims=True) * ROUTED_SCALE
    block = rows // tp
    early = lax.broadcasted_iota(jnp.int32, (rows, rows), 0)
    late = lax.broadcasted_iota(jnp.int32, (rows, rows), 1)
    before = jnp.where((early < late) & (early // block == late // block), 1.0, 0.0).astype(BF16)
    hits = [ids == e * tp + t for e in range(ep)]
    chosen = [jnp.sum(jnp.where(hit, 1.0, 0.0), axis=0, keepdims=True) for hit in hits]
    pad = [jnp.zeros((-ep % 16, rows), F32)] if ep % 16 else []
    ranks = jnp.dot(
        jnp.concatenate(chosen + pad, axis=0).astype(BF16), before, preferred_element_type=F32
    ).astype(jnp.int32)
    base = (tp - 1 - lax.broadcasted_iota(jnp.int32, (1, rows), 1) // block) * slot_cap
    line = lax.broadcasted_iota(jnp.int32, (slots, rows), 0)
    for e in range(ep):
        place = jnp.where(chosen[e] > 0.5, base + ranks[e : e + 1, :], -1)
        weight = jnp.sum(jnp.where(hits[e], weights, 0.0), axis=0, keepdims=True)
        pick[e] = jnp.where(line == place, 1.0, 0.0).astype(BF16)
        spread_t[pl.ds(e * slots, slots), :] = jnp.where(line == place, weight, 0.0)
    returned = slots - turn * slot_cap
    turn_rows = turn * block
    turn_slots = turn * slot_cap
    if turn:
        turn_weight[...] = jnp.zeros(turn_weight.shape, BF16)

        def clear_step(i, carry):
            for e in range(ep):
                ret[i, e, returned:slots, :] = jnp.zeros((turn_slots, cols), BF16)
            return carry

        lax.fori_loop(0, chunks, clear_step, 0)
    pl.semaphore_wait(barrier, len(partners))

    def forward(k):
        return remote(whole.at[k], whole.at[k], f_send.at[k // 2], a_recv.at[k], g, mate)

    def upward(k):
        there = lax.rem(z + 1, chips) * 2 + c
        return remote(whole.at[k], whole.at[k], u_send.at[k // 2], a_recv.at[k], g, there)

    def downward(k):
        there = lax.rem(z + chips - 1, chips) * 2 + c
        return remote(whole.at[k], whole.at[k], d_send.at[k // 2], a_recv.at[k], g, there)

    firsts[2].wait()

    @pl.when(z < chips - 1)
    def _():
        upward(t).start()

    @pl.when(z > 0)
    def _():
        downward(t).start()

    forward(t).start()

    crossed = slots - shift * slot_cap
    extra_rows = shift * block

    def ids_copy(p):
        lanes = pl.ds(0, ids_other.shape[2])
        e = partner(g, p, ep)
        return remote(ids_ref.at[:, lanes], ids_other.at[p - 1], i_send, i_recv, e, t)

    def affinity_copy(p):
        lanes = pl.ds(0, ids_other.shape[2])
        e = partner(g, p, ep)
        return remote(affinity_ref.at[:, lanes], affinity_other.at[p - 1], w_send, w_recv, e, t)

    def extra_copy(p):
        e = partner(g, p, ep)
        rows_out = whole.at[t, pl.ds(0, extra_rows)]
        return remote(rows_out, extra.at[t, p - 1], x_send, x_recv, e, t)

    def extra_forward(k):
        return remote(extra.at[k], extra.at[k], ef_send.at[k // 2], e_recv.at[k], g, mate)

    def extra_upward(k):
        there = lax.rem(z + 1, chips) * 2 + c
        return remote(extra.at[k], extra.at[k], eu_send.at[k // 2], e_recv.at[k], g, there)

    def extra_downward(k):
        there = lax.rem(z + chips - 1, chips) * 2 + c
        return remote(extra.at[k], extra.at[k], ed_send.at[k // 2], e_recv.at[k], g, there)

    if shift:
        for p in range(1, ep):
            ids_copy(p).start()
            extra_copy(p).start()
            if turn:
                affinity_copy(p).start()

    def extra_onward(chip):
        k = chip * 2 + c

        @pl.when((chip <= z) & (z < chips - 1))
        def _():
            extra_upward(k).start()

        @pl.when((chip >= z) & (z > 0))
        def _():
            extra_downward(k).start()

        extra_forward(k).start()

    def pick_others():
        remote(ids_other, ids_other, i_send, i_recv, g, mate).wait_recv()
        lanes = ids_other.shape[2]
        early = lax.broadcasted_iota(jnp.int32, (lanes, lanes), 0)
        late = lax.broadcasted_iota(jnp.int32, (lanes, lanes), 1)
        before = jnp.where((early < late) & (early // block == late // block), 1.0, 0.0)
        chosen = [
            jnp.sum(jnp.where(ids_other[p] == g * tp + t, 1.0, 0.0), axis=0, keepdims=True)
            for p in range(ep - 1)
        ]
        pad = [jnp.zeros((-(ep - 1) % 16, lanes), F32)]
        ranks = jnp.dot(
            jnp.concatenate(chosen + pad, axis=0).astype(BF16),
            before.astype(BF16),
            preferred_element_type=F32,
        ).astype(jnp.int32)
        blocks = lax.broadcasted_iota(jnp.int32, (1, lanes), 1) // block
        base = (shift - 1 - blocks) * slot_cap
        line = lax.broadcasted_iota(jnp.int32, (shift * slot_cap, lanes), 0)
        for p in range(ep - 1):
            named = (chosen[p] > 0.5) & (blocks < shift)
            place = jnp.where(named, base + ranks[p : p + 1, :], -1)
            pick_other[p] = jnp.where(line == place, 1.0, 0.0).astype(BF16)
        if not turn:
            return
        remote(affinity_other, affinity_other, w_send, w_recv, g, mate).wait_recv()
        base = (turn - 1 - blocks) * slot_cap
        line = lax.broadcasted_iota(jnp.int32, ((ep - 1) * turn_slots, lanes), 0)
        for p in range(ep - 1):
            share = affinity_other[p] / jnp.sum(affinity_other[p], axis=0, keepdims=True)
            hit = ids_other[p] == g * tp + t
            weight = jnp.sum(jnp.where(hit, share * ROUTED_SCALE, 0.0), axis=0, keepdims=True)
            named = (chosen[p] > 0.5) & (blocks < turn)
            place = jnp.where(named, p * turn_slots + base + ranks[p : p + 1, :], -1)
            spread_p = jnp.where(line == place, weight, 0.0).T.astype(BF16)
            turn_weight[p * turn_rows : (p + 1) * turn_rows, :] = spread_p[:turn_rows, :]

    near = [p for p in range(1, ep) if not p & (p - 1)]
    far = [p for p in range(1, ep) if p & (p - 1)]
    half = chunks // 8

    def send_rows(k, p):
        e = partner(g, p, ep)
        over = pl.ds(0, crossed)
        remote(sent.at[k, e, over], inc.at[k, g, over], b_send, b_recv.at[g], e, t).start()

    def arrive(chip):
        k = chip * 2 + c
        forward(k).wait_recv()

        @pl.when((chip < z) & (z < chips - 1))
        def _():
            upward(k).start()

        @pl.when((chip > z) & (z > 0))
        def _():
            downward(k).start()

        forward(k).start()

    def distance_step(d, carry):
        def at_side(side):
            chip = z + d * (side * 2 - 1)
            return chip, (chip >= 0) & (chip < chips) & ((d > 0) | (side == 0))

        for side in range(2):
            chip, there = at_side(side)

            @pl.when(there & (d > 0))
            def _():
                arrive(chip)

        def chunk_step(q, carry):
            chip, there = at_side(q % 2)
            lane = q // 2
            k = chip * 2 + lax.rem(c + lane, 2)

            @pl.when(there)
            def _():
                @pl.when(lane > 0)
                def _():
                    forward(k).wait_recv()

                picked = jnp.dot(
                    pick[...].reshape(ep * slots, rows), whole[k], preferred_element_type=F32
                ).astype(BF16)
                sent[k] = picked.reshape(ep, slots, feat)
                inc[k, g] = sent[k, g]
                for p in near:
                    send_rows(k, p)

            return carry

        lax.fori_loop(0, 4, chunk_step, 0)

        def far_step(q, carry):
            chip, there = at_side(q % 2)

            @pl.when(there)
            def _():
                for p in far:
                    send_rows(chip * 2 + lax.rem(c + q // 2, 2), p)

            return carry

        lax.fori_loop(0, 4, far_step, 0)
        if not shift:
            return carry

        @pl.when(d == 0)
        def _():
            remote(extra.at[t], extra.at[t], x_send, x_recv, g, mate).wait_recv()
            extra_onward(z)
            pick_others()

        for side in range(2):
            chip, there = at_side(side)

            @pl.when(there & (d > 0))
            def _():
                extra_forward(chip * 2 + c).wait_recv()
                extra_onward(chip)

        def extra_step(q, carry):
            chip, there = at_side(q % 2)
            lane = q // 2
            k = chip * 2 + lax.rem(c + lane, 2)

            @pl.when(there)
            def _():
                @pl.when(lane > 0)
                def _():
                    extra_forward(k).wait_recv()

                for p in range(1, ep):
                    inc[k, partner(g, p, ep), crossed:slots, :] = jnp.dot(
                        pick_other[p - 1][:, :extra_rows], extra[k, p - 1], preferred_element_type=F32
                    ).astype(BF16)

            return carry

        lax.fori_loop(0, 4, extra_step, 0)
        return carry

    lax.fori_loop(0, chips, distance_step, 0)
    def normalise(read, count):
        tile = math.gcd(64, count)

        def body(i, carry):
            at = pl.ds(pl.multiple_of(i * tile, tile), tile)
            total = jnp.zeros((tile, feat), F32)
            for k in range(tp):
                total = total + read(k, at).astype(F32)
            mean = jnp.sum(total, axis=1, keepdims=True) / width
            total = jnp.zeros((tile, feat), F32)
            for k in range(tp):
                center = read(k, at).astype(F32) - mean
                total = total + center * center
            scale = lax.rsqrt(jnp.sum(total, axis=1, keepdims=True) / width + EPSILON)
            for k in range(tp):
                lanes = slice(k * feat, (k + 1) * feat)
                value = (read(k, at).astype(F32) - mean) * scale
                value = value * gain_ref[:, lanes] + shift_ref[:, lanes]
                norm[at, lanes] = value.astype(BF16)
            return carry

        lax.fori_loop(0, count // tile, body, 0)

    for load in loads:
        load.wait()

    def activate(s):
        normalise(lambda k, at: inc[k, s, at, :], slots)
        got = norm[0:slots, :]
        gate_act = jnp.dot(got, gate_ref[...], preferred_element_type=F32)
        up_act = jnp.dot(got, up_ref[...], preferred_element_type=F32)
        hidden[s] = (jax.nn.silu(gate_act) * up_act).astype(BF16)

    def expert_step(j, carry):
        p = expert_order(j)
        s = partner(g, p, ep)
        over = pl.ds(0, crossed)
        remote(sent.at[:, s, over], inc.at[:, s, over], b_send, b_recv.at[s], s, t).wait_recv()

        activate(s)
        is_near = functools.reduce(jnp.logical_or, [p == n for n in near])

        @pl.when(is_near)
        def _():
            def near_step(i, carry):
                send_result(i, s)
                return carry

            lax.fori_loop(0, half, near_step, 0)

        return carry

    def chunk_of(i):
        return lax.rem(i + (2 - 2 * (z // 2)) * 2, chunks) if turn else i

    def lanes_of(i):
        return pl.ds(pl.multiple_of(i * cols, cols), cols)

    def down_rows(i, s):
        return jnp.dot(
            hidden[s], down_ref[:, lanes_of(i)], preferred_element_type=F32
        ).astype(BF16)

    def send_result(i, s):
        n = chunk_of(i)
        res[n, s] = down_rows(n, s)

        @pl.when(i < held)
        def _():
            result_copy(n, s).start()

    def result_copy(n, s):
        back = pl.ds(0, returned)
        return remote(res.at[n, s, back], ret.at[n, g, back], r_send, r_recv.at[n], s, t)

    held = chunks * 6 // 8 if turn else chunks

    def held_step(i, carry):
        for p in far + near:
            result_copy(chunk_of(i), partner(g, p, ep)).start()
        return carry

    normalise(lambda k, at: whole[k, at, :], rows)
    contract = (((1,), (1,)), ((), ()))
    sg = lax.dot_general(norm[...], sgate_ref[...], contract, preferred_element_type=F32)
    su = lax.dot_general(norm[...], sup_ref[...], contract, preferred_element_type=F32)
    shidden[...] = (jax.nn.silu(sg) * su).astype(BF16)

    spread[...] = spread_t[...].T.astype(BF16)
    order = near + far

    def expert_order(j):
        return sum(jnp.where(j == n, p, 0) for n, p in enumerate(order))

    lax.fori_loop(0, ep - 1, expert_step, 0)

    def turned_copy(i):
        return remote(t_out.at[i], t_in.at[i], t_send, t_recv, g, mate)

    def turned_back(p):
        return remote(y_out.at[p - 1], y_in.at[p - 1], y_send, y_recv, partner(g, p, ep), t)

    def turned_rows(i):
        result = jnp.dot(
            turn_hidden[...], down_ref[:, lanes_of(i)], preferred_element_type=F32
        ).astype(BF16)
        return jnp.dot(turn_weight[...], result, preferred_element_type=F32)

    def turn_start():
        for p in range(1, ep):
            at = slice((p - 1) * turn_slots, p * turn_slots)
            turn_hidden[at, :] = hidden[partner(g, p, ep), returned:slots, :]

    def turn_step(i):
        t_out[i] = turned_rows(i * 2 + 1 - c).astype(BF16)
        turned_copy(i).start()
        mine[i] = turned_rows(i * 2 + c)

    def line_start():
        remote(t_out, t_in, t_send, t_recv, g, mate).wait_recv()

        def add_step(j, carry):
            mine[j] = mine[j] + t_in[j].astype(F32)
            return carry

        lax.fori_loop(0, chips, add_step, 0)

        for d in range(1, chips):
            zz = partner(z, d, chips)
            line_out[zz] = mine[zz].astype(BF16)
            remote(line_out.at[zz], line_in.at[z], l_send, l_recv, g, zz * 2 + c).start()

    def line_finish():
        some = pl.ds(0, chips - 1)
        remote(line_out.at[some], line_in.at[some], l_send, l_recv, g, mate).wait_recv()
        total = mine[z]
        for d in range(1, chips):
            total = total + line_in[partner(z, d, chips)].astype(F32)
        for p in range(1, ep):
            y_out[p - 1] = total[(p - 1) * turn_rows : p * turn_rows, :].astype(BF16)
            turned_back(p).start()

    def down_step(i, carry):
        for p in far:
            send_result(i, partner(g, p, ep))

        @pl.when(i < chunks - half)
        def _():
            for p in near:
                send_result(i + half, partner(g, p, ep))

        if turn:

            @pl.when(i < chips)
            def _():
                turn_step(i)

            @pl.when(i == chips + 1)
            def _():
                line_start()

        return carry

    if turn:
        turn_start()
    lax.fori_loop(0, chunks, down_step, 0)
    activate(g)

    def own_step(i, carry):
        ret[i, g] = down_rows(i, g)
        return carry

    lax.fori_loop(0, chunks, own_step, 0)
    def pair_copy(n):
        return remote(pair_out.at[n], pair_in.at[n], p_send, p_recv.at[n], g, mate)

    def produce(i, n):
        others = pl.ds(0, ep - 1)
        back = pl.ds(0, returned)
        came = remote(res.at[n, others, back], ret.at[n, others, back], r_send, r_recv.at[n], g, mate)
        came.wait_recv()
        total = jnp.dot(
            spread[...], ret[n].reshape(ep * slots, cols), preferred_element_type=F32
        ) + jnp.dot(shidden[...], sdown_ref[:, lanes_of(n)], preferred_element_type=F32)
        part[i % 2] = total.reshape(part.shape[1:])
        if turn:

            @pl.when(n == t)
            def _():
                remote(y_out, y_in, y_send, y_recv, g, mate).wait_recv()
                more = y_in[0].astype(F32)
                for p in range(1, ep - 1):
                    more = more + y_in[p].astype(F32)
                more = more.reshape((turn,) + part.shape[2:])
                part[i % 2, 0:turn] = part[i % 2, 0:turn] + more

        for zz in range(chips):
            pair_out[n, zz] = part[i % 2, zz * 2 + 1 - c].astype(BF16)
        pair_copy(n).start()

    inner = (z == 1) | (z == 2)
    beside = partner(z, 1, chips)
    across = (2 - 2 * (z // 2)) if paired else 0
    relayed = chunks - 4

    def mixed(i, n, zz):
        return part[i % 2, zz * 2 + c] + pair_in[n, zz].astype(F32)

    def far_copy(n, zz, send):
        return remote(far_out.at[n, zz], far_in.at[n, z], send, q_recv.at[n], g, zz * 2 + c)

    def relay_copy(n):
        two = pl.ds(across, 2)
        return remote(far_out.at[n, two], relay.at[n], o_send, o_recv.at[n], g, beside * 2 + c)

    def finish(i, n):
        pair_copy(n).wait_recv()
        direct = (i >= relayed) if paired else True
        for d in range(1, chips):
            zz = partner(z, d, chips)
            far_out[n, zz] = mixed(i, n, zz).astype(BF16)
            if d == 1 or not paired:
                far_copy(n, zz, q_send).start()
        if paired:

            for send, which in ((q_send, inner), (o_send, jnp.logical_not(inner))):

                @pl.when(direct & which)
                def _():
                    for k in range(2):
                        far_copy(n, across + k, send).start()

            @pl.when(jnp.logical_not(direct | inner))
            def _():
                relay_copy(n).start()

        own[n] = part[i % 2, t] + pair_in[n, z].astype(F32)

    def pass_on(i, n):
        relay_copy(n).wait_recv()
        for k in range(2):
            zz = across + k
            far_out[n, zz] = (mixed(i, n, zz) + relay[n, k].astype(F32)).astype(BF16)
            far_copy(n, zz, q_send).start()

    def sum_step(i, carry):
        n = chunk_of(i)
        produce(i, n)
        if paired:

            @pl.when(inner & (i > 0) & (i <= relayed))
            def _():
                pass_on(i - 1, chunk_of(i - 1))

        finish(i, n)
        if turn:

            @pl.when(i == 1)
            def _():
                line_finish()
                lax.fori_loop(held, chunks, held_step, 0)

        return carry

    lax.fori_loop(0, chunks, sum_step, 0)

    def gathered(n, count):
        some = pl.ds(0, count)
        return remote(far_out.at[n, some], far_in.at[n, some], q_send, q_recv.at[n], g, mate)

    def put(n, sources):
        gathered(n, len(sources)).wait_recv()
        total = own[n]
        for source in sources:
            total = total + far_in[n, source].astype(F32)
        out_ref[:, lanes_of(n)] = total.astype(BF16)

    def out_step(i, carry):
        n = chunk_of(i)
        if not paired:
            put(n, [partner(z, d, chips) for d in range(1, chips)])
            return carry
        straight = lax.rem(n + chunks - z // 2 * 4, chunks) >= relayed

        @pl.when(straight)
        def _():
            put(n, [beside, across, across + 1])

        @pl.when(jnp.logical_not(straight))
        def _():
            put(n, [beside, 2 - z // 2])

        return carry

    lax.fori_loop(0, chunks, out_step, 0)

    rest = pl.ds(0, chips - 1)
    if paired:

        @pl.when(inner)
        def _():
            remote(far_out.at[:, rest], far_in.at[:, rest], q_send, q_recv.at[0], g, mate).wait_send()

        @pl.when(jnp.logical_not(inner))
        def _():
            one = pl.ds(0, 1)
            remote(far_out.at[:, one], far_in.at[:, one], q_send, q_recv.at[0], g, mate).wait_send()
            remote(relay, relay, o_send, o_recv.at[0], g, mate).wait_send()

    else:
        remote(far_out.at[:, rest], far_in.at[:, rest], q_send, q_recv.at[0], g, mate).wait_send()

    others = pl.ds(0, ep - 1)
    over = pl.ds(0, crossed)
    remote(
        sent.at[:, others, over], inc.at[:, others, over], b_send, b_recv.at[g], g, mate
    ).wait_send()
    back = pl.ds(0, returned)
    remote(
        res.at[:, others, back], ret.at[:, others, back], r_send, r_recv.at[0], g, mate
    ).wait_send()
    remote(pair_out, pair_in, p_send, p_recv.at[0], g, mate).wait_send()

    def sent_step(chip, carry):
        k = chip * 2 + c
        forward(k).wait_send()

        @pl.when((chip <= z) & (z < chips - 1))
        def _():
            upward(k).wait_send()

        @pl.when((chip >= z) & (z > 0))
        def _():
            downward(k).wait_send()

        if not shift:
            return carry
        extra_forward(k).wait_send()

        @pl.when((chip <= z) & (z < chips - 1))
        def _():
            extra_upward(k).wait_send()

        @pl.when((chip >= z) & (z > 0))
        def _():
            extra_downward(k).wait_send()

        return carry

    lax.fori_loop(0, chips, sent_step, 0)
    if shift:
        remote(ids_other, ids_other, i_send, i_recv, g, mate).wait_send()
        remote(extra.at[t], extra.at[t], x_send, x_recv, g, mate).wait_send()
    if not turn:
        return
    remote(affinity_other, affinity_other, w_send, w_recv, g, mate).wait_send()
    remote(t_out, t_in, t_send, t_recv, g, mate).wait_send()
    remote(y_out, y_in, y_send, y_recv, g, mate).wait_send()

    some = pl.ds(0, chips - 1)
    remote(line_out.at[some], line_in.at[some], l_send, l_recv, g, mate).wait_send()


def on_device(
    tokens,
    norm_gain,
    norm_shift,
    expert_ids,
    affinity,
    expert_gate,
    expert_up,
    expert_down,
    shared_gate,
    shared_up,
    shared_down,
):
    ep = lax.axis_size("ep")
    tp = lax.axis_size("tp")
    rows, feat = tokens.shape
    width = feat * tp
    top_count = expert_ids.shape[1]
    block = rows // tp
    expert_count = ep * tp
    slot_cap = max(1, 2 * block * top_count // expert_count)
    slots = tp * slot_cap
    hid = expert_gate.shape[2]
    shared_rows = shared_gate.shape[0]
    cols = 256
    chunks = width // cols
    chips = tp // 2
    shift = max(1, tp // 8)
    fits = (ep & (ep - 1)) == 0 and ep > 1 and slot_cap % 8 == 0 and block % 8 == 0
    if not fits or shift * block > 128 or rows < 128 or feat != cols:
        shift = 0
    lanes = min(rows, 128)
    turn = 1 * shift if 1 * shift * block <= 128 and chunks == tp and chips > 2 else 0
    turn_rows = max(8, (ep - 1) * turn * block)
    turn_slots = max(8, (ep - 1) * turn * slot_cap)
    line = (chips if turn else 1, turn_rows, cols)

    vmem = pl.BlockSpec(memory_space=pltpu.VMEM)
    anywhere = pl.BlockSpec(memory_space=pl.ANY)
    dma = pltpu.SemaphoreType.DMA
    return pl.pallas_call(
        functools.partial(layer_kernel, (ep, tp, rows, slots, slot_cap, feat, chunks, cols, shift, turn)),
        out_shape=pltpu.VMEM((block, width), BF16),
        in_specs=[anywhere] * 11,
        out_specs=vmem,
        scratch_shapes=[
            pltpu.VMEM((top_count, rows), jnp.int32),
            pltpu.VMEM((top_count, rows), F32),
            pltpu.VMEM((1, width), F32),
            pltpu.VMEM((1, width), F32),
            pltpu.VMEM((shared_rows, width), BF16),
            pltpu.VMEM((shared_rows, width), BF16),
            pltpu.VMEM((width, hid), BF16),
            pltpu.VMEM((width, hid), BF16),
            pltpu.VMEM((hid, width), BF16),
            pltpu.VMEM((shared_rows, width), BF16),
            pltpu.VMEM((tp, rows, feat), BF16),
            pltpu.VMEM((ep, slots, rows), BF16),
            pltpu.VMEM((ep * slots, rows), F32),
            pltpu.VMEM((rows, ep * slots), BF16),
            pltpu.VMEM((tp, ep, slots, feat), BF16),
            pltpu.VMEM((tp, ep, slots, feat), BF16),
            pltpu.VMEM((max(rows, slots), width), BF16),
            pltpu.VMEM((ep, slots, hid), BF16),
            pltpu.VMEM((rows, shared_rows), BF16),
            pltpu.VMEM((chunks, ep, slots, cols), BF16),
            pltpu.VMEM((chunks, ep, slots, cols), BF16),
            pltpu.VMEM((ep - 1, top_count, lanes), jnp.int32),
            pltpu.VMEM((tp, ep - 1, max(8, shift * block), feat), BF16),
            pltpu.VMEM((ep - 1, max(8, shift * slot_cap), lanes), BF16),
            pltpu.VMEM((ep - 1, top_count, lanes), F32),
            pltpu.VMEM((turn_rows, turn_slots), BF16),
            pltpu.VMEM((turn_slots, hid), BF16),
            pltpu.VMEM(line, F32),
            pltpu.VMEM(line, BF16),
            pltpu.VMEM(line, BF16),
            pltpu.VMEM(line, BF16),
            pltpu.VMEM(line, BF16),
            pltpu.VMEM((ep - 1, max(8, turn * block), cols), BF16),
            pltpu.VMEM((ep - 1, max(8, turn * block), cols), BF16),
            pltpu.VMEM((2, tp, block, cols), F32),
            pltpu.VMEM((chunks, block, cols), F32),
            pltpu.VMEM((chunks, chips, block, cols), BF16),
            pltpu.VMEM((chunks, chips, block, cols), BF16),
            pltpu.VMEM((chunks, chips, block, cols), BF16),
            pltpu.VMEM((chunks, chips, block, cols), BF16),
            pltpu.VMEM((chunks, 2, block, cols), BF16),
            dma((8,)),
            dma((3,)),
            dma((chips,)),
            dma((chips,)),
            dma((chips,)),
            dma((tp,)),
            dma,
            dma((ep,)),
            dma,
            dma((chunks,)),
            dma,
            dma((chunks,)),
            dma,
            dma((chunks,)),
            dma,
            dma((chunks,)),
            dma,
            dma,
            dma,
            dma,
            dma((chips,)),
            dma((chips,)),
            dma((chips,)),
            dma((tp,)),
            dma,
            dma,
            dma,
            dma,
            dma,
            dma,
            dma,
            dma,
        ],
        compiler_params=pltpu.CompilerParams(
            collective_id=0, has_side_effects=True, vmem_limit_bytes=56 * 1024 * 1024
        ),
        name="moe_layer",
    )(
        tokens,
        expert_ids.T,
        affinity.T,
        norm_gain.reshape(1, width),
        norm_shift.reshape(1, width),
        shared_gate,
        shared_up,
        expert_gate[0],
        expert_up[0],
        expert_down[0],
        shared_down,
    )


def solution(mesh):
    placed = (
        P("ep", "tp"),
        P(),
        P(),
        P("ep", None),
        P("ep", None),
        P(("ep", "tp"), None, None),
        P(("ep", "tp"), None, None),
        P(("ep", "tp"), None, None),
        P("tp", None),
        P("tp", None),
        P(),
    )
    return jax.shard_map(
        on_device, mesh=mesh, in_specs=placed, out_specs=P(("ep", "tp"), None), check_vma=False
    )
```

```python
import functools
import math

import jax
import jax.numpy as jnp
from jax import lax
from jax.experimental import pallas as pl
from jax.experimental.pallas import tpu as pltpu
from jax.sharding import PartitionSpec as P

ROUTED_SCALE = 2.5
EPSILON = 1e-05
MESH = pl.DeviceIdType.MESH
F32 = jnp.float32
BF16 = jnp.bfloat16


def partner(index, step, count):
    if count & (count - 1):
        return lax.rem(index + step, count)
    result, bit = 0, 1
    while bit < count:
        result = result + ((index // bit) % 2 + (step // bit) % 2) % 2 * bit
        bit *= 2
    return result


def layer_kernel(
    sizes,
    tokens_hbm,
    ids_hbm,
    affinity_hbm,
    gain_hbm,
    shift_hbm,
    sgate_hbm,
    sup_hbm,
    gate_hbm,
    up_hbm,
    down_hbm,
    sdown_hbm,
    out_ref,
    ids_ref,
    affinity_ref,
    gain_ref,
    shift_ref,
    sgate_ref,
    sup_ref,
    gate_ref,
    up_ref,
    down_ref,
    sdown_ref,
    whole,
    pick,
    spread_t,
    spread,
    sent,
    inc,
    norm,
    hidden,
    shidden,
    res,
    ret,
    ids_other,
    extra,
    pick_other,
    affinity_other,
    spread_other,
    mine,
    t_out,
    t_in,
    line_out,
    line_in,
    hop_in,
    y_out,
    y_in,
    part,
    own,
    pair_out,
    pair_in,
    far_out,
    far_in,
    relay,
    load_sem,
    first_sem,
    u_send,
    d_send,
    f_send,
    a_recv,
    b_send,
    b_recv,
    r_send,
    r_recv,
    p_send,
    p_recv,
    q_send,
    q_recv,
    o_send,
    o_recv,
    i_send,
    i_recv,
    x_send,
    x_recv,
    eu_send,
    ed_send,
    ef_send,
    e_recv,
    w_send,
    w_recv,
    t_send,
    t_recv,
    l_send,
    l_recv,
    y_send,
    y_recv,
    m_send,
    m_recv,
    h_send,
    h_recv,
):
    ep, tp, rows, slots, slot_cap, feat, chunks, cols, shift = sizes
    chips = tp // 2
    g = lax.axis_index("ep")
    t = lax.axis_index("tp")
    z = t // 2
    c = t % 2
    mate = z * 2 + 1 - c
    width = tp * feat
    shared_rows = sdown_ref.shape[0]

    firsts = [
        pltpu.make_async_copy(ids_hbm, ids_ref, first_sem.at[0]),
        pltpu.make_async_copy(affinity_hbm, affinity_ref, first_sem.at[1]),
        pltpu.make_async_copy(tokens_hbm, whole.at[t], first_sem.at[2]),
    ]
    loads = [
        pltpu.make_async_copy(gain_hbm, gain_ref, load_sem.at[0]),
        pltpu.make_async_copy(shift_hbm, shift_ref, load_sem.at[1]),
        pltpu.make_async_copy(sgate_hbm, sgate_ref, load_sem.at[2]),
        pltpu.make_async_copy(sup_hbm, sup_ref, load_sem.at[3]),
        pltpu.make_async_copy(
            sdown_hbm.at[pl.ds(pl.multiple_of(t * shared_rows, 8), shared_rows)],
            sdown_ref,
            load_sem.at[4],
        ),
        pltpu.make_async_copy(gate_hbm, gate_ref, load_sem.at[5]),
        pltpu.make_async_copy(up_hbm, up_ref, load_sem.at[6]),
        pltpu.make_async_copy(down_hbm, down_ref, load_sem.at[7]),
    ]
    for load in firsts:
        load.start()

    def remote(src, dst, send, recv, e, k):
        return pltpu.make_async_remote_copy(
            src_ref=src,
            dst_ref=dst,
            send_sem=send,
            recv_sem=recv,
            device_id=(e, k),
            device_id_type=MESH,
        )

    barrier = pltpu.get_barrier_semaphore()
    partners = [(partner(g, p, ep), t) for p in range(1, ep)]
    partners += [(g, partner(z, d, chips) * 2 + c) for d in range(1, chips)]
    partners += [(g, mate)]
    for e, k in partners:
        pl.semaphore_signal(barrier, inc=1, device_id=(e, k), device_id_type=MESH)
    for load in loads:
        load.start()
    for load in firsts[:2]:
        load.wait()
    ids = ids_ref[...]
    affinity = affinity_ref[...]
    weights = affinity / jnp.sum(affinity, axis=0, keepdims=True) * ROUTED_SCALE
    block = rows // tp
    early = lax.broadcasted_iota(jnp.int32, (rows, rows), 0)
    late = lax.broadcasted_iota(jnp.int32, (rows, rows), 1)
    before = jnp.where((early < late) & (early // block == late // block), 1.0, 0.0).astype(BF16)
    hits = [ids == e * tp + t for e in range(ep)]
    chosen = [jnp.sum(jnp.where(hit, 1.0, 0.0), axis=0, keepdims=True) for hit in hits]
    pad = [jnp.zeros((-ep % 16, rows), F32)] if ep % 16 else []
    ranks = jnp.dot(
        jnp.concatenate(chosen + pad, axis=0).astype(BF16), before, preferred_element_type=F32
    ).astype(jnp.int32)
    base = (tp - 1 - lax.broadcasted_iota(jnp.int32, (1, rows), 1) // block) * slot_cap
    line = lax.broadcasted_iota(jnp.int32, (slots, rows), 0)
    for e in range(ep):
        place = jnp.where(chosen[e] > 0.5, base + ranks[e : e + 1, :], -1)
        weight = jnp.sum(jnp.where(hits[e], weights, 0.0), axis=0, keepdims=True)
        pick[e] = jnp.where(line == place, 1.0, 0.0).astype(BF16)
        spread_t[pl.ds(e * slots, slots), :] = jnp.where(line == place, weight, 0.0)
    sent_chunks = chunks - 1 if shift else chunks
    if shift:
        ret[chunks - 1] = jnp.zeros(ret.shape[1:], BF16)
    pl.semaphore_wait(barrier, len(partners))

    def forward(k):
        return remote(whole.at[k], whole.at[k], f_send.at[k // 2], a_recv.at[k], g, mate)

    def upward(k):
        there = lax.rem(z + 1, chips) * 2 + c
        return remote(whole.at[k], whole.at[k], u_send.at[k // 2], a_recv.at[k], g, there)

    def downward(k):
        there = lax.rem(z + chips - 1, chips) * 2 + c
        return remote(whole.at[k], whole.at[k], d_send.at[k // 2], a_recv.at[k], g, there)

    firsts[2].wait()

    @pl.when(z < chips - 1)
    def _():
        upward(t).start()

    @pl.when(z > 0)
    def _():
        downward(t).start()

    forward(t).start()

    crossed = slots - shift * slot_cap
    extra_rows = shift * block

    def ids_copy(p):
        e = partner(g, p, ep)
        return remote(ids_ref, ids_other.at[p - 1], i_send, i_recv, e, t)

    def affinity_copy(p):
        e = partner(g, p, ep)
        return remote(affinity_ref, affinity_other.at[p - 1], w_send, w_recv, e, t)

    def extra_copy(p):
        e = partner(g, p, ep)
        rows_out = whole.at[t, pl.ds(0, extra_rows)]
        return remote(rows_out, extra.at[t, p - 1], x_send, x_recv, e, t)

    def extra_forward(k):
        return remote(extra.at[k], extra.at[k], ef_send.at[k // 2], e_recv.at[k], g, mate)

    def extra_upward(k):
        there = lax.rem(z + 1, chips) * 2 + c
        return remote(extra.at[k], extra.at[k], eu_send.at[k // 2], e_recv.at[k], g, there)

    def extra_downward(k):
        there = lax.rem(z + chips - 1, chips) * 2 + c
        return remote(extra.at[k], extra.at[k], ed_send.at[k // 2], e_recv.at[k], g, there)

    if shift:
        for p in range(1, ep):
            extra_copy(p).start()

        @pl.when(c == 0)
        def _():
            for p in range(1, ep):
                ids_copy(p).start()

        @pl.when(c == 1)
        def _():
            for p in range(1, ep):
                affinity_copy(p).start()

    def extra_onward(chip):
        k = chip * 2 + c

        @pl.when((chip <= z) & (z < chips - 1))
        def _():
            extra_upward(k).start()

        @pl.when((chip >= z) & (z > 0))
        def _():
            extra_downward(k).start()

        extra_forward(k).start()

    def ids_share():
        return remote(ids_other, ids_other, m_send, m_recv, g, mate)

    def affinity_share():
        return remote(affinity_other, affinity_other, m_send, m_recv, g, mate)

    def pick_others():
        @pl.when(c == 0)
        def _():
            remote(ids_other, ids_other, i_send, i_recv, g, mate).wait_recv()
            ids_share().start()
            affinity_share().wait_recv()

        @pl.when(c == 1)
        def _():
            remote(affinity_other, affinity_other, w_send, w_recv, g, mate).wait_recv()
            affinity_share().start()
            ids_share().wait_recv()

        early = lax.broadcasted_iota(jnp.int32, (rows, rows), 0)
        late = lax.broadcasted_iota(jnp.int32, (rows, rows), 1)
        before = jnp.where((early < late) & (early // block == late // block), 1.0, 0.0)
        hits = [ids_other[p] == g * tp + t for p in range(ep - 1)]
        chosen = [jnp.sum(jnp.where(hit, 1.0, 0.0), axis=0, keepdims=True) for hit in hits]
        pad = [jnp.zeros((-(ep - 1) % 16, rows), F32)]
        ranks = jnp.dot(
            jnp.concatenate(chosen + pad, axis=0).astype(BF16),
            before.astype(BF16),
            preferred_element_type=F32,
        ).astype(jnp.int32)
        base = (tp - 1 - lax.broadcasted_iota(jnp.int32, (1, rows), 1) // block) * slot_cap
        line = lax.broadcasted_iota(jnp.int32, (slots, rows), 0)
        lanes = pick_other.shape[2]
        late_line = lax.broadcasted_iota(jnp.int32, (shift * slot_cap, lanes), 0) + crossed
        for p in range(ep - 1):
            place = jnp.where(chosen[p] > 0.5, base + ranks[p : p + 1, :], -1)
            pick_other[p] = jnp.where(late_line == place[:, :lanes], 1.0, 0.0).astype(BF16)
            share = affinity_other[p] / jnp.sum(affinity_other[p], axis=0, keepdims=True)
            weight = jnp.sum(jnp.where(hits[p], share * ROUTED_SCALE, 0.0), axis=0, keepdims=True)
            spread_other[p] = jnp.where(line == place, weight, 0.0).T.astype(BF16)

    near = [p for p in range(1, ep) if not p & (p - 1)]
    far = [p for p in range(1, ep) if p & (p - 1)]
    half = chunks // 8

    def send_rows(k, p):
        e = partner(g, p, ep)
        over = pl.ds(0, crossed)
        remote(sent.at[k, e, over], inc.at[k, g, over], b_send, b_recv.at[g], e, t).start()

    def arrive(chip):
        k = chip * 2 + c
        forward(k).wait_recv()

        @pl.when((chip < z) & (z < chips - 1))
        def _():
            upward(k).start()

        @pl.when((chip > z) & (z > 0))
        def _():
            downward(k).start()

        forward(k).start()

    def distance_step(d, carry):
        def at_side(side):
            chip = z + d * (side * 2 - 1)
            return chip, (chip >= 0) & (chip < chips) & ((d > 0) | (side == 0))

        for side in range(2):
            chip, there = at_side(side)

            @pl.when(there & (d > 0))
            def _():
                arrive(chip)

        def chunk_step(q, carry):
            chip, there = at_side(q % 2)
            lane = q // 2
            k = chip * 2 + lax.rem(c + lane, 2)

            @pl.when(there)
            def _():
                @pl.when(lane > 0)
                def _():
                    forward(k).wait_recv()

                picked = jnp.dot(
                    pick[...].reshape(ep * slots, rows), whole[k], preferred_element_type=F32
                ).astype(BF16)
                sent[k] = picked.reshape(ep, slots, feat)
                inc[k, g] = sent[k, g]
                for p in near:
                    send_rows(k, p)

            return carry

        lax.fori_loop(0, 4, chunk_step, 0)

        def far_step(q, carry):
            chip, there = at_side(q % 2)

            @pl.when(there)
            def _():
                for p in far:
                    send_rows(chip * 2 + lax.rem(c + q // 2, 2), p)

            return carry

        lax.fori_loop(0, 4, far_step, 0)
        if not shift:
            return carry

        @pl.when(d == 0)
        def _():
            remote(extra.at[t], extra.at[t], x_send, x_recv, g, mate).wait_recv()
            extra_onward(z)
            pick_others()

        for side in range(2):
            chip, there = at_side(side)

            @pl.when(there & (d > 0))
            def _():
                extra_forward(chip * 2 + c).wait_recv()
                extra_onward(chip)

        def extra_step(q, carry):
            chip, there = at_side(q % 2)
            lane = q // 2
            k = chip * 2 + lax.rem(c + lane, 2)

            @pl.when(there)
            def _():
                @pl.when(lane > 0)
                def _():
                    extra_forward(k).wait_recv()

                for p in range(1, ep):
                    inc[k, partner(g, p, ep), crossed:slots, :] = jnp.dot(
                        pick_other[p - 1][:, :extra_rows], extra[k, p - 1], preferred_element_type=F32
                    ).astype(BF16)

            return carry

        lax.fori_loop(0, 4, extra_step, 0)
        return carry

    lax.fori_loop(0, chips, distance_step, 0)
    def normalise(read, count):
        tile = math.gcd(64, count)

        def body(i, carry):
            at = pl.ds(pl.multiple_of(i * tile, tile), tile)
            total = jnp.zeros((tile, feat), F32)
            for k in range(tp):
                total = total + read(k, at).astype(F32)
            mean = jnp.sum(total, axis=1, keepdims=True) / width
            total = jnp.zeros((tile, feat), F32)
            for k in range(tp):
                center = read(k, at).astype(F32) - mean
                total = total + center * center
            scale = lax.rsqrt(jnp.sum(total, axis=1, keepdims=True) / width + EPSILON)
            for k in range(tp):
                lanes = slice(k * feat, (k + 1) * feat)
                value = (read(k, at).astype(F32) - mean) * scale
                value = value * gain_ref[:, lanes] + shift_ref[:, lanes]
                norm[at, lanes] = value.astype(BF16)
            return carry

        lax.fori_loop(0, count // tile, body, 0)

    for load in loads:
        load.wait()

    def activate(s):
        normalise(lambda k, at: inc[k, s, at, :], slots)
        got = norm[0:slots, :]
        gate_act = jnp.dot(got, gate_ref[...], preferred_element_type=F32)
        up_act = jnp.dot(got, up_ref[...], preferred_element_type=F32)
        hidden[s] = (jax.nn.silu(gate_act) * up_act).astype(BF16)

    def expert_step(j, carry):
        p = expert_order(j)
        s = partner(g, p, ep)
        over = pl.ds(0, crossed)
        remote(sent.at[:, s, over], inc.at[:, s, over], b_send, b_recv.at[s], s, t).wait_recv()

        activate(s)
        is_near = functools.reduce(jnp.logical_or, [p == n for n in near])

        @pl.when(is_near)
        def _():
            def near_step(i, carry):
                send_result(i, s)
                return carry

            lax.fori_loop(0, half, near_step, 0)

        return carry

    def lanes_of(i):
        return pl.ds(pl.multiple_of(i * cols, cols), cols)

    def down_rows(i, s):
        return jnp.dot(
            hidden[s], down_ref[:, lanes_of(i)], preferred_element_type=F32
        ).astype(BF16)

    def send_result(i, s):
        res[i, s] = down_rows(i, s)
        remote(res.at[i, s], ret.at[i, g], r_send, r_recv.at[i], s, t).start()

    normalise(lambda k, at: whole[k, at, :], rows)
    contract = (((1,), (1,)), ((), ()))
    sg = lax.dot_general(norm[...], sgate_ref[...], contract, preferred_element_type=F32)
    su = lax.dot_general(norm[...], sup_ref[...], contract, preferred_element_type=F32)
    shidden[...] = (jax.nn.silu(sg) * su).astype(BF16)

    spread[...] = spread_t[...].T.astype(BF16)
    order = near + far

    def expert_order(j):
        return sum(jnp.where(j == n, p, 0) for n, p in enumerate(order))

    lax.fori_loop(0, ep - 1, expert_step, 0)

    def turn_step(p):
        result = down_rows(chunks - 1, partner(g, p, ep))
        total = jnp.dot(spread_other[p - 1], result, preferred_element_type=F32)
        part[0] = total.reshape(part.shape[1:])
        for zz in range(chips):
            t_out[zz, p - 1] = part[0, zz * 2 + 1 - c].astype(BF16)
            mine[zz, p - 1] = part[0, zz * 2 + c]

        @pl.when(p == ep - 1)
        def _():
            remote(t_out, t_in, t_send, t_recv, g, mate).start()

    paired = chips == 4 and shift > 0
    inner = (z == 1) | (z == 2)
    beside = partner(z, 1, chips)
    across = 2 - 2 * (z // 2) if paired else 0

    def line_copy(zz):
        return remote(line_out.at[zz], line_in.at[z], l_send, l_recv, g, zz * 2 + c)

    def hop_copy():
        two = pl.ds(across, 2)
        return remote(line_out.at[two], hop_in, h_send, h_recv, g, beside * 2 + c)

    def line_start():
        remote(t_out, t_in, t_send, t_recv, g, mate).wait_recv()
        for d in range(1, chips):
            zz = partner(z, d, chips)
            line_out[zz] = (mine[zz] + t_in[zz].astype(F32)).astype(BF16)
            if d == 1 or not paired:
                line_copy(zz).start()
        if paired:

            @pl.when(jnp.logical_not(inner))
            def _():
                hop_copy().start()

    def line_pass():
        hop_copy().wait_recv()
        for k in range(2):
            zz = across + k
            total = mine[zz] + t_in[zz].astype(F32) + hop_in[k].astype(F32)
            line_out[zz] = total.astype(BF16)
            line_copy(zz).start()

    def line_finish():
        sources = [partner(z, d, chips) for d in range(1, chips)]
        if paired:
            sources = [beside, 2 - z // 2]
        some = pl.ds(0, len(sources))
        remote(line_out.at[some], line_in.at[some], l_send, l_recv, g, mate).wait_recv()
        total = mine[z] + t_in[z].astype(F32)
        for source in sources:
            total = total + line_in[source].astype(F32)
        y_out[...] = total.astype(BF16)
        for p in range(1, ep):
            there = partner(g, p, ep)
            remote(y_out.at[p - 1], y_in.at[p - 1], y_send, y_recv, there, t).start()

    def down_step(i, carry):
        for p in far:
            send_result(i, partner(g, p, ep))

        @pl.when(i < sent_chunks - half)
        def _():
            for p in near:
                send_result(i + half, partner(g, p, ep))

        if shift:

            @pl.when(i < ep - 1)
            def _():
                turn_step(i + 1)

            @pl.when(i == ep + 1)
            def _():
                line_start()

        return carry

    lax.fori_loop(0, sent_chunks, down_step, 0)
    activate(g)

    def own_step(i, carry):
        ret[i, g] = down_rows(i, g)
        return carry

    lax.fori_loop(0, chunks, own_step, 0)
    def pair_copy(n):
        return remote(pair_out.at[n], pair_in.at[n], p_send, p_recv.at[n], g, mate)

    def produce(i, n):
        @pl.when(n < sent_chunks)
        def _():
            others = pl.ds(0, ep - 1)
            came = remote(res.at[n, others], ret.at[n, others], r_send, r_recv.at[n], g, mate)
            came.wait_recv()

        total = jnp.dot(
            spread[...], ret[n].reshape(ep * slots, cols), preferred_element_type=F32
        ) + jnp.dot(shidden[...], sdown_ref[:, lanes_of(n)], preferred_element_type=F32)
        part[i % 2] = total.reshape(part.shape[1:])
        for zz in range(chips):
            pair_out[n, zz] = part[i % 2, zz * 2 + 1 - c].astype(BF16)
        pair_copy(n).start()

    relayed = chunks - 3 if paired else 0

    def mixed(i, n, zz):
        return part[i % 2, zz * 2 + c] + pair_in[n, zz].astype(F32)

    def far_copy(n, zz, send):
        return remote(far_out.at[n, zz], far_in.at[n, z], send, q_recv.at[n], g, zz * 2 + c)

    def relay_copy(n):
        two = pl.ds(across, 2)
        return remote(far_out.at[n, two], relay.at[n], o_send, o_recv.at[n], g, beside * 2 + c)

    def finish(i, n):
        pair_copy(n).wait_recv()
        for d in range(1, chips):
            zz = partner(z, d, chips)
            far_out[n, zz] = mixed(i, n, zz).astype(BF16)
            if d == 1 or not paired:
                far_copy(n, zz, q_send).start()
        if paired:
            for send, which in ((q_send, inner), (o_send, jnp.logical_not(inner))):

                @pl.when((i >= relayed) & which)
                def _():
                    for k in range(2):
                        far_copy(n, across + k, send).start()

            @pl.when((i < relayed) & jnp.logical_not(inner))
            def _():
                relay_copy(n).start()

        own[n] = part[i % 2, t] + pair_in[n, z].astype(F32)

    def pass_on(i, n):
        relay_copy(n).wait_recv()
        for k in range(2):
            zz = across + k
            far_out[n, zz] = (mixed(i, n, zz) + relay[n, k].astype(F32)).astype(BF16)
            far_copy(n, zz, q_send).start()

    def chunk_of(i):
        return lax.rem(i + sent_chunks, chunks)

    def sum_step(i, carry):
        n = chunk_of(i)
        produce(i, n)
        if paired:

            @pl.when(inner & (i > 0) & (i <= relayed))
            def _():
                pass_on(i - 1, chunk_of(i - 1))

        finish(i, n)
        if shift:

            if paired:

                @pl.when(inner & (i == 0))
                def _():
                    line_pass()

            @pl.when(i == 4)
            def _():
                line_finish()

        return carry

    lax.fori_loop(0, chunks, sum_step, 0)

    def gathered(n, count):
        some = pl.ds(0, count)
        return remote(far_out.at[n, some], far_in.at[n, some], q_send, q_recv.at[n], g, mate)

    def put(n, sources):
        gathered(n, len(sources)).wait_recv()
        total = own[n]
        for source in sources:
            total = total + far_in[n, source].astype(F32)
        if shift:

            @pl.when(n == sent_chunks)
            def _():
                remote(y_out, y_in, y_send, y_recv, g, mate).wait_recv()
                more = y_in[0].astype(F32)
                for p in range(1, ep - 1):
                    more = more + y_in[p].astype(F32)
                own[n] = total + more

            @pl.when(n < sent_chunks)
            def _():
                own[n] = total

            total = own[n]
        out_ref[:, lanes_of(n)] = total.astype(BF16)

    def out_step(i, carry):
        n = lax.rem(i, chunks)
        later = lax.rem(n + chunks - sent_chunks, chunks) >= relayed

        @pl.when(later)
        def _():
            put(n, [partner(z, d, chips) for d in range(1, chips)])

        if paired:

            @pl.when(jnp.logical_not(later))
            def _():
                put(n, [beside, 2 - z // 2])

        return carry

    lax.fori_loop(0, chunks, out_step, 0)

    rest = pl.ds(0, chips - 1)
    if paired:

        @pl.when(inner)
        def _():
            remote(far_out.at[:, rest], far_in.at[:, rest], q_send, q_recv.at[0], g, mate).wait_send()

        @pl.when(jnp.logical_not(inner))
        def _():
            one = pl.ds(0, 1)
            remote(far_out.at[:, one], far_in.at[:, one], q_send, q_recv.at[0], g, mate).wait_send()
            remote(relay, relay, o_send, o_recv.at[0], g, mate).wait_send()

    else:
        remote(far_out.at[:, rest], far_in.at[:, rest], q_send, q_recv.at[0], g, mate).wait_send()

    others = pl.ds(0, ep - 1)
    over = pl.ds(0, crossed)
    remote(
        sent.at[:, others, over], inc.at[:, others, over], b_send, b_recv.at[g], g, mate
    ).wait_send()
    some = pl.ds(0, sent_chunks)
    remote(
        res.at[some, others], ret.at[some, others], r_send, r_recv.at[0], g, mate
    ).wait_send()
    remote(pair_out, pair_in, p_send, p_recv.at[0], g, mate).wait_send()

    def sent_step(chip, carry):
        k = chip * 2 + c
        forward(k).wait_send()

        @pl.when((chip <= z) & (z < chips - 1))
        def _():
            upward(k).wait_send()

        @pl.when((chip >= z) & (z > 0))
        def _():
            downward(k).wait_send()

        if not shift:
            return carry
        extra_forward(k).wait_send()

        @pl.when((chip <= z) & (z < chips - 1))
        def _():
            extra_upward(k).wait_send()

        @pl.when((chip >= z) & (z > 0))
        def _():
            extra_downward(k).wait_send()

        return carry

    lax.fori_loop(0, chips, sent_step, 0)
    if shift:

        @pl.when(c == 0)
        def _():
            remote(ids_other, ids_other, i_send, i_recv, g, mate).wait_send()
            ids_share().wait_send()

        @pl.when(c == 1)
        def _():
            remote(affinity_other, affinity_other, w_send, w_recv, g, mate).wait_send()
            affinity_share().wait_send()

        remote(extra.at[t], extra.at[t], x_send, x_recv, g, mate).wait_send()
        remote(t_out, t_in, t_send, t_recv, g, mate).wait_send()
        remote(y_out, y_in, y_send, y_recv, g, mate).wait_send()
        some = pl.ds(0, chips - 1)
        if paired:

            @pl.when(inner)
            def _():
                remote(line_out.at[some], line_in.at[some], l_send, l_recv, g, mate).wait_send()

            @pl.when(jnp.logical_not(inner))
            def _():
                line_copy(beside).wait_send()
                hop_copy().wait_send()

        else:
            remote(line_out.at[some], line_in.at[some], l_send, l_recv, g, mate).wait_send()


def on_device(
    tokens,
    norm_gain,
    norm_shift,
    expert_ids,
    affinity,
    expert_gate,
    expert_up,
    expert_down,
    shared_gate,
    shared_up,
    shared_down,
):
    ep = lax.axis_size("ep")
    tp = lax.axis_size("tp")
    rows, feat = tokens.shape
    width = feat * tp
    top_count = expert_ids.shape[1]
    block = rows // tp
    expert_count = ep * tp
    slot_cap = max(1, 2 * block * top_count // expert_count)
    slots = tp * slot_cap
    hid = expert_gate.shape[2]
    shared_rows = shared_gate.shape[0]
    cols = 256
    chunks = width // cols
    chips = tp // 2
    shift = max(1, tp // 8)
    fits = (ep & (ep - 1)) == 0 and ep > 1 and slot_cap % 8 == 0 and block % 8 == 0
    if not fits or shift * block > 128 or rows < 128:
        shift = 0
    lanes = min(rows, 128)
    line = (chips, ep - 1, block, cols) if shift else (1, 1, 8, 128)
    back = line[1:]
    other = (ep - 1, rows, slots) if shift else (1, 8, 128)

    vmem = pl.BlockSpec(memory_space=pltpu.VMEM)
    anywhere = pl.BlockSpec(memory_space=pl.ANY)
    dma = pltpu.SemaphoreType.DMA
    return pl.pallas_call(
        functools.partial(layer_kernel, (ep, tp, rows, slots, slot_cap, feat, chunks, cols, shift)),
        out_shape=pltpu.VMEM((block, width), BF16),
        in_specs=[anywhere] * 11,
        out_specs=vmem,
        scratch_shapes=[
            pltpu.VMEM((top_count, rows), jnp.int32),
            pltpu.VMEM((top_count, rows), F32),
            pltpu.VMEM((1, width), F32),
            pltpu.VMEM((1, width), F32),
            pltpu.VMEM((shared_rows, width), BF16),
            pltpu.VMEM((shared_rows, width), BF16),
            pltpu.VMEM((width, hid), BF16),
            pltpu.VMEM((width, hid), BF16),
            pltpu.VMEM((hid, width), BF16),
            pltpu.VMEM((shared_rows, width), BF16),
            pltpu.VMEM((tp, rows, feat), BF16),
            pltpu.VMEM((ep, slots, rows), BF16),
            pltpu.VMEM((ep * slots, rows), F32),
            pltpu.VMEM((rows, ep * slots), BF16),
            pltpu.VMEM((tp, ep, slots, feat), BF16),
            pltpu.VMEM((tp, ep, slots, feat), BF16),
            pltpu.VMEM((max(rows, slots), width), BF16),
            pltpu.VMEM((ep, slots, hid), BF16),
            pltpu.VMEM((rows, shared_rows), BF16),
            pltpu.VMEM((chunks, ep, slots, cols), BF16),
            pltpu.VMEM((chunks, ep, slots, cols), BF16),
            pltpu.VMEM((ep - 1, top_count, rows), jnp.int32),
            pltpu.VMEM((tp, ep - 1, max(8, shift * block), feat), BF16),
            pltpu.VMEM((ep - 1, max(8, shift * slot_cap), lanes), BF16),
            pltpu.VMEM((ep - 1, top_count, rows), F32),
            pltpu.VMEM(other, BF16),
            pltpu.VMEM(line, F32),
            pltpu.VMEM(line, BF16),
            pltpu.VMEM(line, BF16),
            pltpu.VMEM(line, BF16),
            pltpu.VMEM(line, BF16),
            pltpu.VMEM((2,) + back, BF16),
            pltpu.VMEM(back, BF16),
            pltpu.VMEM(back, BF16),
            pltpu.VMEM((2, tp, block, cols), F32),
            pltpu.VMEM((chunks, block, cols), F32),
            pltpu.VMEM((chunks, chips, block, cols), BF16),
            pltpu.VMEM((chunks, chips, block, cols), BF16),
            pltpu.VMEM((chunks, chips, block, cols), BF16),
            pltpu.VMEM((chunks, chips, block, cols), BF16),
            pltpu.VMEM((chunks, 2, block, cols), BF16),
            dma((8,)),
            dma((3,)),
            dma((chips,)),
            dma((chips,)),
            dma((chips,)),
            dma((tp,)),
            dma,
            dma((ep,)),
            dma,
            dma((chunks,)),
            dma,
            dma((chunks,)),
            dma,
            dma((chunks,)),
            dma,
            dma((chunks,)),
            dma,
            dma,
            dma,
            dma,
            dma((chips,)),
            dma((chips,)),
            dma((chips,)),
            dma((tp,)),
            dma,
            dma,
            dma,
            dma,
            dma,
            dma,
            dma,
            dma,
            dma,
            dma,
            dma,
            dma,
        ],
        compiler_params=pltpu.CompilerParams(
            collective_id=0, has_side_effects=True, vmem_limit_bytes=56 * 1024 * 1024
        ),
        name="moe_layer",
    )(
        tokens,
        expert_ids.T,
        affinity.T,
        norm_gain.reshape(1, width),
        norm_shift.reshape(1, width),
        shared_gate,
        shared_up,
        expert_gate[0],
        expert_up[0],
        expert_down[0],
        shared_down,
    )


def solution(mesh):
    placed = (
        P("ep", "tp"),
        P(),
        P(),
        P("ep", None),
        P("ep", None),
        P(("ep", "tp"), None, None),
        P(("ep", "tp"), None, None),
        P(("ep", "tp"), None, None),
        P("tp", None),
        P("tp", None),
        P(),
    )
    return jax.shard_map(
        on_device, mesh=mesh, in_specs=placed, out_specs=P(("ep", "tp"), None), check_vma=False
    )
```

```python
import functools
import math

import jax
import jax.numpy as jnp
from jax import lax
from jax.experimental import pallas as pl
from jax.experimental.pallas import tpu as pltpu
from jax.sharding import PartitionSpec as P

ROUTED_SCALE = 2.5
EPSILON = 1e-05
MESH = pl.DeviceIdType.MESH
F32 = jnp.float32
BF16 = jnp.bfloat16


def partner(index, step, count):
    if count & (count - 1):
        return lax.rem(index + step, count)
    result, bit = 0, 1
    while bit < count:
        result = result + ((index // bit) % 2 + (step // bit) % 2) % 2 * bit
        bit *= 2
    return result


def layer_kernel(
    sizes,
    tokens_hbm,
    ids_hbm,
    affinity_hbm,
    gain_hbm,
    shift_hbm,
    sgate_hbm,
    sup_hbm,
    gate_hbm,
    up_hbm,
    down_hbm,
    sdown_hbm,
    out_ref,
    ids_ref,
    affinity_ref,
    gain_ref,
    shift_ref,
    sgate_ref,
    sup_ref,
    gate_ref,
    up_ref,
    down_ref,
    sdown_ref,
    whole,
    pick,
    spread_t,
    spread,
    sent,
    inc,
    norm,
    hidden,
    shidden,
    res,
    ret,
    ids_other,
    extra,
    pick_other,
    affinity_other,
    spread_other,
    mine,
    t_out,
    t_in,
    line_out,
    line_in,
    hop_in,
    y_out,
    y_in,
    part,
    own,
    pair_out,
    pair_in,
    far_out,
    far_in,
    relay,
    load_sem,
    first_sem,
    u_send,
    d_send,
    f_send,
    a_recv,
    b_send,
    b_recv,
    r_send,
    r_recv,
    p_send,
    p_recv,
    q_send,
    q_recv,
    o_send,
    o_recv,
    i_send,
    i_recv,
    x_send,
    x_recv,
    eu_send,
    ed_send,
    ef_send,
    e_recv,
    w_send,
    w_recv,
    t_send,
    t_recv,
    l_send,
    l_recv,
    y_send,
    y_recv,
    m_send,
    m_recv,
    h_send,
    h_recv,
):
    ep, tp, rows, slots, slot_cap, feat, chunks, cols, shift = sizes
    chips = tp // 2
    g = lax.axis_index("ep")
    t = lax.axis_index("tp")
    z = t // 2
    c = t % 2
    mate = z * 2 + 1 - c
    width = tp * feat
    shared_rows = sdown_ref.shape[0]

    firsts = [
        pltpu.make_async_copy(ids_hbm, ids_ref, first_sem.at[0]),
        pltpu.make_async_copy(affinity_hbm, affinity_ref, first_sem.at[1]),
        pltpu.make_async_copy(tokens_hbm, whole.at[t], first_sem.at[2]),
    ]
    loads = [
        pltpu.make_async_copy(gain_hbm, gain_ref, load_sem.at[0]),
        pltpu.make_async_copy(shift_hbm, shift_ref, load_sem.at[1]),
        pltpu.make_async_copy(sgate_hbm, sgate_ref, load_sem.at[2]),
        pltpu.make_async_copy(sup_hbm, sup_ref, load_sem.at[3]),
        pltpu.make_async_copy(
            sdown_hbm.at[pl.ds(pl.multiple_of(t * shared_rows, 8), shared_rows)],
            sdown_ref,
            load_sem.at[4],
        ),
        pltpu.make_async_copy(gate_hbm, gate_ref, load_sem.at[5]),
        pltpu.make_async_copy(up_hbm, up_ref, load_sem.at[6]),
        pltpu.make_async_copy(down_hbm, down_ref, load_sem.at[7]),
    ]
    for load in firsts:
        load.start()

    def remote(src, dst, send, recv, e, k):
        return pltpu.make_async_remote_copy(
            src_ref=src,
            dst_ref=dst,
            send_sem=send,
            recv_sem=recv,
            device_id=(e, k),
            device_id_type=MESH,
        )

    barrier = pltpu.get_barrier_semaphore()
    partners = [(partner(g, p, ep), t) for p in range(1, ep)]
    partners += [(g, partner(z, d, chips) * 2 + c) for d in range(1, chips)]
    partners += [(g, mate)]
    for e, k in partners:
        pl.semaphore_signal(barrier, inc=1, device_id=(e, k), device_id_type=MESH)
    for load in loads:
        load.start()
    for load in firsts[:2]:
        load.wait()
    ids = ids_ref[...]
    affinity = affinity_ref[...]
    weights = affinity / jnp.sum(affinity, axis=0, keepdims=True) * ROUTED_SCALE
    block = rows // tp
    early = lax.broadcasted_iota(jnp.int32, (rows, rows), 0)
    late = lax.broadcasted_iota(jnp.int32, (rows, rows), 1)
    before = jnp.where((early < late) & (early // block == late // block), 1.0, 0.0).astype(BF16)
    hits = [ids == e * tp + t for e in range(ep)]
    chosen = [jnp.sum(jnp.where(hit, 1.0, 0.0), axis=0, keepdims=True) for hit in hits]
    pad = [jnp.zeros((-ep % 16, rows), F32)] if ep % 16 else []
    ranks = jnp.dot(
        jnp.concatenate(chosen + pad, axis=0).astype(BF16), before, preferred_element_type=F32
    ).astype(jnp.int32)
    base = (tp - 1 - lax.broadcasted_iota(jnp.int32, (1, rows), 1) // block) * slot_cap
    line = lax.broadcasted_iota(jnp.int32, (slots, rows), 0)
    for e in range(ep):
        place = jnp.where(chosen[e] > 0.5, base + ranks[e : e + 1, :], -1)
        weight = jnp.sum(jnp.where(hits[e], weights, 0.0), axis=0, keepdims=True)
        pick[e] = jnp.where(line == place, 1.0, 0.0).astype(BF16)
        spread_t[pl.ds(e * slots, slots), :] = jnp.where(line == place, weight, 0.0)
    sent_chunks = chunks - 1 if shift else chunks
    if shift:
        ret[chunks - 1] = jnp.zeros(ret.shape[1:], BF16)
    pl.semaphore_wait(barrier, len(partners))

    def forward(k):
        return remote(whole.at[k], whole.at[k], f_send.at[k // 2], a_recv.at[k], g, mate)

    def upward(k):
        there = lax.rem(z + 1, chips) * 2 + c
        return remote(whole.at[k], whole.at[k], u_send.at[k // 2], a_recv.at[k], g, there)

    def downward(k):
        there = lax.rem(z + chips - 1, chips) * 2 + c
        return remote(whole.at[k], whole.at[k], d_send.at[k // 2], a_recv.at[k], g, there)

    firsts[2].wait()

    @pl.when(z < chips - 1)
    def _():
        upward(t).start()

    @pl.when(z > 0)
    def _():
        downward(t).start()

    forward(t).start()

    crossed = slots - shift * slot_cap
    extra_rows = shift * block

    def ids_copy(p):
        e = partner(g, p, ep)
        return remote(ids_ref, ids_other.at[p - 1], i_send, i_recv, e, t)

    def affinity_copy(p):
        e = partner(g, p, ep)
        return remote(affinity_ref, affinity_other.at[p - 1], w_send, w_recv, e, t)

    def extra_copy(p):
        e = partner(g, p, ep)
        rows_out = whole.at[t, pl.ds(0, extra_rows)]
        return remote(rows_out, extra.at[t, p - 1], x_send, x_recv, e, t)

    def extra_forward(k):
        return remote(extra.at[k], extra.at[k], ef_send.at[k // 2], e_recv.at[k], g, mate)

    def extra_upward(k):
        there = lax.rem(z + 1, chips) * 2 + c
        return remote(extra.at[k], extra.at[k], eu_send.at[k // 2], e_recv.at[k], g, there)

    def extra_downward(k):
        there = lax.rem(z + chips - 1, chips) * 2 + c
        return remote(extra.at[k], extra.at[k], ed_send.at[k // 2], e_recv.at[k], g, there)

    if shift:
        for p in range(1, ep):
            extra_copy(p).start()

        @pl.when(c == 0)
        def _():
            for p in range(1, ep):
                ids_copy(p).start()

        @pl.when(c == 1)
        def _():
            for p in range(1, ep):
                affinity_copy(p).start()

    def extra_onward(chip):
        k = chip * 2 + c

        @pl.when((chip <= z) & (z < chips - 1))
        def _():
            extra_upward(k).start()

        @pl.when((chip >= z) & (z > 0))
        def _():
            extra_downward(k).start()

        extra_forward(k).start()

    def ids_share():
        return remote(ids_other, ids_other, m_send, m_recv, g, mate)

    def affinity_share():
        return remote(affinity_other, affinity_other, m_send, m_recv, g, mate)

    def pick_others():
        @pl.when(c == 0)
        def _():
            remote(ids_other, ids_other, i_send, i_recv, g, mate).wait_recv()
            ids_share().start()
            affinity_share().wait_recv()

        @pl.when(c == 1)
        def _():
            remote(affinity_other, affinity_other, w_send, w_recv, g, mate).wait_recv()
            affinity_share().start()
            ids_share().wait_recv()

        early = lax.broadcasted_iota(jnp.int32, (rows, rows), 0)
        late = lax.broadcasted_iota(jnp.int32, (rows, rows), 1)
        before = jnp.where((early < late) & (early // block == late // block), 1.0, 0.0)
        hits = [ids_other[p] == g * tp + t for p in range(ep - 1)]
        chosen = [jnp.sum(jnp.where(hit, 1.0, 0.0), axis=0, keepdims=True) for hit in hits]
        pad = [jnp.zeros((-(ep - 1) % 16, rows), F32)]
        ranks = jnp.dot(
            jnp.concatenate(chosen + pad, axis=0).astype(BF16),
            before.astype(BF16),
            preferred_element_type=F32,
        ).astype(jnp.int32)
        base = (tp - 1 - lax.broadcasted_iota(jnp.int32, (1, rows), 1) // block) * slot_cap
        line = lax.broadcasted_iota(jnp.int32, (slots, rows), 0)
        lanes = pick_other.shape[2]
        late_line = lax.broadcasted_iota(jnp.int32, (shift * slot_cap, lanes), 0) + crossed
        for p in range(ep - 1):
            place = jnp.where(chosen[p] > 0.5, base + ranks[p : p + 1, :], -1)
            pick_other[p] = jnp.where(late_line == place[:, :lanes], 1.0, 0.0).astype(BF16)
            share = affinity_other[p] / jnp.sum(affinity_other[p], axis=0, keepdims=True)
            weight = jnp.sum(jnp.where(hits[p], share * ROUTED_SCALE, 0.0), axis=0, keepdims=True)
            spread_other[p] = jnp.where(line == place, weight, 0.0).T.astype(BF16)

    near = [p for p in range(1, ep) if not p & (p - 1)]
    far = [p for p in range(1, ep) if p & (p - 1)]
    half = chunks // 8

    def send_rows(k, p):
        e = partner(g, p, ep)
        over = pl.ds(0, crossed)
        remote(sent.at[k, e, over], inc.at[k, g, over], b_send, b_recv.at[g], e, t).start()

    def arrive(chip):
        k = chip * 2 + c
        forward(k).wait_recv()

        @pl.when((chip < z) & (z < chips - 1))
        def _():
            upward(k).start()

        @pl.when((chip > z) & (z > 0))
        def _():
            downward(k).start()

        forward(k).start()

    def distance_step(d, carry):
        def at_side(side):
            chip = z + d * (side * 2 - 1)
            return chip, (chip >= 0) & (chip < chips) & ((d > 0) | (side == 0))

        for side in range(2):
            chip, there = at_side(side)

            @pl.when(there & (d > 0))
            def _():
                arrive(chip)

        def chunk_step(q, carry):
            chip, there = at_side(q % 2)
            lane = q // 2
            k = chip * 2 + lax.rem(c + lane, 2)

            @pl.when(there)
            def _():
                @pl.when(lane > 0)
                def _():
                    forward(k).wait_recv()

                picked = jnp.dot(
                    pick[...].reshape(ep * slots, rows), whole[k], preferred_element_type=F32
                ).astype(BF16)
                sent[k] = picked.reshape(ep, slots, feat)
                inc[k, g] = sent[k, g]
                for p in near:
                    send_rows(k, p)

            return carry

        lax.fori_loop(0, 4, chunk_step, 0)

        def far_step(q, carry):
            chip, there = at_side(q % 2)

            @pl.when(there)
            def _():
                for p in far:
                    send_rows(chip * 2 + lax.rem(c + q // 2, 2), p)

            return carry

        lax.fori_loop(0, 4, far_step, 0)
        if not shift:

            @pl.when(d == 0)
            def _():
                spread[...] = spread_t[...].T.astype(BF16)

            return carry

        @pl.when(d == 0)
        def _():
            remote(extra.at[t], extra.at[t], x_send, x_recv, g, mate).wait_recv()
            extra_onward(z)
            pick_others()
            spread[...] = spread_t[...].T.astype(BF16)

        for side in range(2):
            chip, there = at_side(side)

            @pl.when(there & (d > 0))
            def _():
                extra_forward(chip * 2 + c).wait_recv()
                extra_onward(chip)

        def extra_step(q, carry):
            chip, there = at_side(q % 2)
            lane = q // 2
            k = chip * 2 + lax.rem(c + lane, 2)

            @pl.when(there)
            def _():
                @pl.when(lane > 0)
                def _():
                    extra_forward(k).wait_recv()

                for p in range(1, ep):
                    inc[k, partner(g, p, ep), crossed:slots, :] = jnp.dot(
                        pick_other[p - 1][:, :extra_rows], extra[k, p - 1], preferred_element_type=F32
                    ).astype(BF16)

            return carry

        lax.fori_loop(0, 4, extra_step, 0)
        return carry

    lax.fori_loop(0, chips, distance_step, 0)
    def normalise(read, count):
        tile = math.gcd(64, count)

        def body(i, carry):
            at = pl.ds(pl.multiple_of(i * tile, tile), tile)
            total = jnp.zeros((tile, feat), F32)
            for k in range(tp):
                total = total + read(k, at).astype(F32)
            mean = jnp.sum(total, axis=1, keepdims=True) / width
            total = jnp.zeros((tile, feat), F32)
            for k in range(tp):
                center = read(k, at).astype(F32) - mean
                total = total + center * center
            scale = lax.rsqrt(jnp.sum(total, axis=1, keepdims=True) / width + EPSILON)
            for k in range(tp):
                lanes = slice(k * feat, (k + 1) * feat)
                value = (read(k, at).astype(F32) - mean) * scale
                value = value * gain_ref[:, lanes] + shift_ref[:, lanes]
                norm[at, lanes] = value.astype(BF16)
            return carry

        lax.fori_loop(0, count // tile, body, 0)

    for load in loads:
        load.wait()

    def activate(s):
        normalise(lambda k, at: inc[k, s, at, :], slots)
        got = norm[0:slots, :]
        gate_act = jnp.dot(got, gate_ref[...], preferred_element_type=F32)
        up_act = jnp.dot(got, up_ref[...], preferred_element_type=F32)
        hidden[s] = (jax.nn.silu(gate_act) * up_act).astype(BF16)

    def expert_step(j, carry):
        p = expert_order(j)
        s = partner(g, p, ep)
        over = pl.ds(0, crossed)
        remote(sent.at[:, s, over], inc.at[:, s, over], b_send, b_recv.at[s], s, t).wait_recv()

        activate(s)
        is_near = functools.reduce(jnp.logical_or, [p == n for n in near])

        @pl.when(is_near)
        def _():
            def near_step(i, carry):
                send_result(i, s)
                return carry

            lax.fori_loop(0, half, near_step, 0)

        return carry

    def lanes_of(i):
        return pl.ds(pl.multiple_of(i * cols, cols), cols)

    def down_rows(i, s):
        return jnp.dot(
            hidden[s], down_ref[:, lanes_of(i)], preferred_element_type=F32
        ).astype(BF16)

    def send_result(i, s):
        res[i, s] = down_rows(i, s)
        remote(res.at[i, s], ret.at[i, g], r_send, r_recv.at[i], s, t).start()

    normalise(lambda k, at: whole[k, at, :], rows)
    contract = (((1,), (1,)), ((), ()))
    sg = lax.dot_general(norm[...], sgate_ref[...], contract, preferred_element_type=F32)
    su = lax.dot_general(norm[...], sup_ref[...], contract, preferred_element_type=F32)
    shidden[...] = (jax.nn.silu(sg) * su).astype(BF16)

    order = near + far

    def expert_order(j):
        return sum(jnp.where(j == n, p, 0) for n, p in enumerate(order))

    lax.fori_loop(0, ep - 1, expert_step, 0)

    def turn_step(p):
        result = down_rows(chunks - 1, partner(g, p, ep))
        total = jnp.dot(spread_other[p - 1], result, preferred_element_type=F32)
        part[0] = total.reshape(part.shape[1:])
        for zz in range(chips):
            t_out[zz, p - 1] = part[0, zz * 2 + 1 - c].astype(BF16)
            mine[zz, p - 1] = part[0, zz * 2 + c]

        @pl.when(p == ep - 1)
        def _():
            remote(t_out, t_in, t_send, t_recv, g, mate).start()

    paired = chips == 4 and shift > 0
    inner = (z == 1) | (z == 2)
    beside = partner(z, 1, chips)
    across = 2 - 2 * (z // 2) if paired else 0

    def line_copy(zz):
        return remote(line_out.at[zz], line_in.at[z], l_send, l_recv, g, zz * 2 + c)

    def hop_copy():
        two = pl.ds(across, 2)
        return remote(line_out.at[two], hop_in, h_send, h_recv, g, beside * 2 + c)

    def line_start():
        remote(t_out, t_in, t_send, t_recv, g, mate).wait_recv()
        for d in range(1, chips):
            zz = partner(z, d, chips)
            line_out[zz] = (mine[zz] + t_in[zz].astype(F32)).astype(BF16)
            if d == 1 or not paired:
                line_copy(zz).start()
        if paired:

            @pl.when(jnp.logical_not(inner))
            def _():
                hop_copy().start()

    def line_pass():
        hop_copy().wait_recv()
        for k in range(2):
            zz = across + k
            total = mine[zz] + t_in[zz].astype(F32) + hop_in[k].astype(F32)
            line_out[zz] = total.astype(BF16)
            line_copy(zz).start()

    def line_finish():
        sources = [partner(z, d, chips) for d in range(1, chips)]
        if paired:
            sources = [beside, 2 - z // 2]
        some = pl.ds(0, len(sources))
        remote(line_out.at[some], line_in.at[some], l_send, l_recv, g, mate).wait_recv()
        total = mine[z] + t_in[z].astype(F32)
        for source in sources:
            total = total + line_in[source].astype(F32)
        y_out[...] = total.astype(BF16)
        for p in range(1, ep):
            there = partner(g, p, ep)
            remote(y_out.at[p - 1], y_in.at[p - 1], y_send, y_recv, there, t).start()

    def down_step(i, carry):
        for p in far:
            send_result(i, partner(g, p, ep))

        @pl.when(i < sent_chunks - half)
        def _():
            for p in near:
                send_result(i + half, partner(g, p, ep))

        if shift:

            @pl.when(i < ep - 1)
            def _():
                turn_step(i + 1)

            @pl.when(i == ep + 1)
            def _():
                line_start()

        return carry

    lax.fori_loop(0, sent_chunks, down_step, 0)
    activate(g)

    def own_step(i, carry):
        ret[i, g] = down_rows(i, g)
        return carry

    lax.fori_loop(0, chunks, own_step, 0)
    def pair_copy(n):
        return remote(pair_out.at[n], pair_in.at[n], p_send, p_recv.at[n], g, mate)

    def produce(i, n):
        @pl.when(n < sent_chunks)
        def _():
            others = pl.ds(0, ep - 1)
            came = remote(res.at[n, others], ret.at[n, others], r_send, r_recv.at[n], g, mate)
            came.wait_recv()

        total = jnp.dot(
            spread[...], ret[n].reshape(ep * slots, cols), preferred_element_type=F32
        ) + jnp.dot(shidden[...], sdown_ref[:, lanes_of(n)], preferred_element_type=F32)
        part[i % 2] = total.reshape(part.shape[1:])
        for zz in range(chips):
            pair_out[n, zz] = part[i % 2, zz * 2 + 1 - c].astype(BF16)
        pair_copy(n).start()

    relayed = chunks - 3 if paired else 0

    def mixed(i, n, zz):
        return part[i % 2, zz * 2 + c] + pair_in[n, zz].astype(F32)

    def far_copy(n, zz, send):
        return remote(far_out.at[n, zz], far_in.at[n, z], send, q_recv.at[n], g, zz * 2 + c)

    def relay_copy(n):
        two = pl.ds(across, 2)
        return remote(far_out.at[n, two], relay.at[n], o_send, o_recv.at[n], g, beside * 2 + c)

    def finish(i, n):
        pair_copy(n).wait_recv()
        for d in range(1, chips):
            zz = partner(z, d, chips)
            far_out[n, zz] = mixed(i, n, zz).astype(BF16)
            if d == 1 or not paired:
                far_copy(n, zz, q_send).start()
        if paired:
            for send, which in ((q_send, inner), (o_send, jnp.logical_not(inner))):

                @pl.when((i >= relayed) & which)
                def _():
                    for k in range(2):
                        far_copy(n, across + k, send).start()

            @pl.when((i < relayed) & jnp.logical_not(inner))
            def _():
                relay_copy(n).start()

        own[n] = part[i % 2, t] + pair_in[n, z].astype(F32)

    def pass_on(i, n):
        relay_copy(n).wait_recv()
        for k in range(2):
            zz = across + k
            far_out[n, zz] = (mixed(i, n, zz) + relay[n, k].astype(F32)).astype(BF16)
            far_copy(n, zz, q_send).start()

    def chunk_of(i):
        return lax.rem(i + sent_chunks, chunks)

    def sum_step(i, carry):
        n = chunk_of(i)
        produce(i, n)
        if paired:

            @pl.when(inner & (i > 0) & (i <= relayed))
            def _():
                pass_on(i - 1, chunk_of(i - 1))

        finish(i, n)
        if shift:

            if paired:

                @pl.when(inner & (i == 0))
                def _():
                    line_pass()

            @pl.when(i == 4)
            def _():
                line_finish()

        return carry

    lax.fori_loop(0, chunks, sum_step, 0)

    def gathered(n, count):
        some = pl.ds(0, count)
        return remote(far_out.at[n, some], far_in.at[n, some], q_send, q_recv.at[n], g, mate)

    def put(n, sources):
        gathered(n, len(sources)).wait_recv()
        total = own[n]
        for source in sources:
            total = total + far_in[n, source].astype(F32)
        if shift:

            @pl.when(n == sent_chunks)
            def _():
                remote(y_out, y_in, y_send, y_recv, g, mate).wait_recv()
                more = y_in[0].astype(F32)
                for p in range(1, ep - 1):
                    more = more + y_in[p].astype(F32)
                own[n] = total + more

            @pl.when(n < sent_chunks)
            def _():
                own[n] = total

            total = own[n]
        out_ref[:, lanes_of(n)] = total.astype(BF16)

    def out_step(i, carry):
        n = lax.rem(i, chunks)
        later = lax.rem(n + chunks - sent_chunks, chunks) >= relayed

        @pl.when(later)
        def _():
            put(n, [partner(z, d, chips) for d in range(1, chips)])

        if paired:

            @pl.when(jnp.logical_not(later))
            def _():
                put(n, [beside, 2 - z // 2])

        return carry

    lax.fori_loop(0, chunks, out_step, 0)

    rest = pl.ds(0, chips - 1)
    if paired:

        @pl.when(inner)
        def _():
            remote(far_out.at[:, rest], far_in.at[:, rest], q_send, q_recv.at[0], g, mate).wait_send()

        @pl.when(jnp.logical_not(inner))
        def _():
            one = pl.ds(0, 1)
            remote(far_out.at[:, one], far_in.at[:, one], q_send, q_recv.at[0], g, mate).wait_send()
            remote(relay, relay, o_send, o_recv.at[0], g, mate).wait_send()

    else:
        remote(far_out.at[:, rest], far_in.at[:, rest], q_send, q_recv.at[0], g, mate).wait_send()

    others = pl.ds(0, ep - 1)
    over = pl.ds(0, crossed)
    remote(
        sent.at[:, others, over], inc.at[:, others, over], b_send, b_recv.at[g], g, mate
    ).wait_send()
    some = pl.ds(0, sent_chunks)
    remote(
        res.at[some, others], ret.at[some, others], r_send, r_recv.at[0], g, mate
    ).wait_send()
    remote(pair_out, pair_in, p_send, p_recv.at[0], g, mate).wait_send()

    def sent_step(chip, carry):
        k = chip * 2 + c
        forward(k).wait_send()

        @pl.when((chip <= z) & (z < chips - 1))
        def _():
            upward(k).wait_send()

        @pl.when((chip >= z) & (z > 0))
        def _():
            downward(k).wait_send()

        if not shift:
            return carry
        extra_forward(k).wait_send()

        @pl.when((chip <= z) & (z < chips - 1))
        def _():
            extra_upward(k).wait_send()

        @pl.when((chip >= z) & (z > 0))
        def _():
            extra_downward(k).wait_send()

        return carry

    lax.fori_loop(0, chips, sent_step, 0)
    if shift:

        @pl.when(c == 0)
        def _():
            remote(ids_other, ids_other, i_send, i_recv, g, mate).wait_send()
            ids_share().wait_send()

        @pl.when(c == 1)
        def _():
            remote(affinity_other, affinity_other, w_send, w_recv, g, mate).wait_send()
            affinity_share().wait_send()

        remote(extra.at[t], extra.at[t], x_send, x_recv, g, mate).wait_send()
        remote(t_out, t_in, t_send, t_recv, g, mate).wait_send()
        remote(y_out, y_in, y_send, y_recv, g, mate).wait_send()
        some = pl.ds(0, chips - 1)
        if paired:

            @pl.when(inner)
            def _():
                remote(line_out.at[some], line_in.at[some], l_send, l_recv, g, mate).wait_send()

            @pl.when(jnp.logical_not(inner))
            def _():
                line_copy(beside).wait_send()
                hop_copy().wait_send()

        else:
            remote(line_out.at[some], line_in.at[some], l_send, l_recv, g, mate).wait_send()


def on_device(
    tokens,
    norm_gain,
    norm_shift,
    expert_ids,
    affinity,
    expert_gate,
    expert_up,
    expert_down,
    shared_gate,
    shared_up,
    shared_down,
):
    ep = lax.axis_size("ep")
    tp = lax.axis_size("tp")
    rows, feat = tokens.shape
    width = feat * tp
    top_count = expert_ids.shape[1]
    block = rows // tp
    expert_count = ep * tp
    slot_cap = max(1, 2 * block * top_count // expert_count)
    slots = tp * slot_cap
    hid = expert_gate.shape[2]
    shared_rows = shared_gate.shape[0]
    cols = 256
    chunks = width // cols
    chips = tp // 2
    shift = max(1, tp // 8)
    fits = (ep & (ep - 1)) == 0 and ep > 1 and slot_cap % 8 == 0 and block % 8 == 0
    if not fits or shift * block > 128 or rows < 128:
        shift = 0
    lanes = min(rows, 128)
    line = (chips, ep - 1, block, cols) if shift else (1, 1, 8, 128)
    back = line[1:]
    other = (ep - 1, rows, slots) if shift else (1, 8, 128)

    vmem = pl.BlockSpec(memory_space=pltpu.VMEM)
    anywhere = pl.BlockSpec(memory_space=pl.ANY)
    dma = pltpu.SemaphoreType.DMA
    return pl.pallas_call(
        functools.partial(layer_kernel, (ep, tp, rows, slots, slot_cap, feat, chunks, cols, shift)),
        out_shape=pltpu.VMEM((block, width), BF16),
        in_specs=[anywhere] * 11,
        out_specs=vmem,
        scratch_shapes=[
            pltpu.VMEM((top_count, rows), jnp.int32),
            pltpu.VMEM((top_count, rows), F32),
            pltpu.VMEM((1, width), F32),
            pltpu.VMEM((1, width), F32),
            pltpu.VMEM((shared_rows, width), BF16),
            pltpu.VMEM((shared_rows, width), BF16),
            pltpu.VMEM((width, hid), BF16),
            pltpu.VMEM((width, hid), BF16),
            pltpu.VMEM((hid, width), BF16),
            pltpu.VMEM((shared_rows, width), BF16),
            pltpu.VMEM((tp, rows, feat), BF16),
            pltpu.VMEM((ep, slots, rows), BF16),
            pltpu.VMEM((ep * slots, rows), F32),
            pltpu.VMEM((rows, ep * slots), BF16),
            pltpu.VMEM((tp, ep, slots, feat), BF16),
            pltpu.VMEM((tp, ep, slots, feat), BF16),
            pltpu.VMEM((max(rows, slots), width), BF16),
            pltpu.VMEM((ep, slots, hid), BF16),
            pltpu.VMEM((rows, shared_rows), BF16),
            pltpu.VMEM((chunks, ep, slots, cols), BF16),
            pltpu.VMEM((chunks, ep, slots, cols), BF16),
            pltpu.VMEM((ep - 1, top_count, rows), jnp.int32),
            pltpu.VMEM((tp, ep - 1, max(8, shift * block), feat), BF16),
            pltpu.VMEM((ep - 1, max(8, shift * slot_cap), lanes), BF16),
            pltpu.VMEM((ep - 1, top_count, rows), F32),
            pltpu.VMEM(other, BF16),
            pltpu.VMEM(line, F32),
            pltpu.VMEM(line, BF16),
            pltpu.VMEM(line, BF16),
            pltpu.VMEM(line, BF16),
            pltpu.VMEM(line, BF16),
            pltpu.VMEM((2,) + back, BF16),
            pltpu.VMEM(back, BF16),
            pltpu.VMEM(back, BF16),
            pltpu.VMEM((2, tp, block, cols), F32),
            pltpu.VMEM((chunks, block, cols), F32),
            pltpu.VMEM((chunks, chips, block, cols), BF16),
            pltpu.VMEM((chunks, chips, block, cols), BF16),
            pltpu.VMEM((chunks, chips, block, cols), BF16),
            pltpu.VMEM((chunks, chips, block, cols), BF16),
            pltpu.VMEM((chunks, 2, block, cols), BF16),
            dma((8,)),
            dma((3,)),
            dma((chips,)),
            dma((chips,)),
            dma((chips,)),
            dma((tp,)),
            dma,
            dma((ep,)),
            dma,
            dma((chunks,)),
            dma,
            dma((chunks,)),
            dma,
            dma((chunks,)),
            dma,
            dma((chunks,)),
            dma,
            dma,
            dma,
            dma,
            dma((chips,)),
            dma((chips,)),
            dma((chips,)),
            dma((tp,)),
            dma,
            dma,
            dma,
            dma,
            dma,
            dma,
            dma,
            dma,
            dma,
            dma,
            dma,
            dma,
        ],
        compiler_params=pltpu.CompilerParams(
            collective_id=0, has_side_effects=True, vmem_limit_bytes=56 * 1024 * 1024
        ),
        name="moe_layer",
    )(
        tokens,
        expert_ids.T,
        affinity.T,
        norm_gain.reshape(1, width),
        norm_shift.reshape(1, width),
        shared_gate,
        shared_up,
        expert_gate[0],
        expert_up[0],
        expert_down[0],
        shared_down,
    )


def solution(mesh):
    placed = (
        P("ep", "tp"),
        P(),
        P(),
        P("ep", None),
        P("ep", None),
        P(("ep", "tp"), None, None),
        P(("ep", "tp"), None, None),
        P(("ep", "tp"), None, None),
        P("tp", None),
        P("tp", None),
        P(),
    )
    return jax.shard_map(
        on_device, mesh=mesh, in_specs=placed, out_specs=P(("ep", "tp"), None), check_vma=False
    )
```

```python
import functools
import math

import jax
import jax.numpy as jnp
from jax import lax
from jax.experimental import pallas as pl
from jax.experimental.pallas import tpu as pltpu
from jax.sharding import PartitionSpec as P

ROUTED_SCALE = 2.5
EPSILON = 1e-05
MESH = pl.DeviceIdType.MESH
F32 = jnp.float32
BF16 = jnp.bfloat16


def partner(index, step, count):
    if count & (count - 1):
        return lax.rem(index + step, count)
    result, bit = 0, 1
    while bit < count:
        result = result + ((index // bit) % 2 + (step // bit) % 2) % 2 * bit
        bit *= 2
    return result


def layer_kernel(
    sizes,
    tokens_hbm,
    ids_hbm,
    affinity_hbm,
    gain_hbm,
    shift_hbm,
    sgate_hbm,
    sup_hbm,
    gate_hbm,
    up_hbm,
    down_hbm,
    sdown_hbm,
    out_ref,
    ids_ref,
    affinity_ref,
    gain_ref,
    shift_ref,
    sgate_ref,
    sup_ref,
    gate_ref,
    up_ref,
    down_ref,
    sdown_ref,
    whole,
    pick,
    spread_t,
    spread,
    sent,
    inc,
    norm,
    hidden,
    shidden,
    res,
    ret,
    ids_other,
    extra,
    pick_other,
    affinity_other,
    spread_other,
    mine,
    t_out,
    t_in,
    line_out,
    line_in,
    hop_in,
    y_out,
    y_in,
    part,
    own,
    pair_out,
    pair_in,
    far_out,
    far_in,
    relay,
    load_sem,
    first_sem,
    u_send,
    d_send,
    f_send,
    a_recv,
    b_send,
    b_recv,
    r_send,
    r_recv,
    p_send,
    p_recv,
    q_send,
    q_recv,
    o_send,
    o_recv,
    i_send,
    i_recv,
    x_send,
    x_recv,
    eu_send,
    ed_send,
    ef_send,
    e_recv,
    w_send,
    w_recv,
    t_send,
    t_recv,
    l_send,
    l_recv,
    y_send,
    y_recv,
    m_send,
    m_recv,
    h_send,
    h_recv,
):
    ep, tp, rows, slots, slot_cap, feat, chunks, cols, shift = sizes
    chips = tp // 2
    g = lax.axis_index("ep")
    t = lax.axis_index("tp")
    z = t // 2
    c = t % 2
    mate = z * 2 + 1 - c
    width = tp * feat
    shared_rows = sdown_ref.shape[0]

    firsts = [
        pltpu.make_async_copy(ids_hbm, ids_ref, first_sem.at[0]),
        pltpu.make_async_copy(affinity_hbm, affinity_ref, first_sem.at[1]),
        pltpu.make_async_copy(tokens_hbm, whole.at[t], first_sem.at[2]),
    ]
    loads = [
        pltpu.make_async_copy(gain_hbm, gain_ref, load_sem.at[0]),
        pltpu.make_async_copy(shift_hbm, shift_ref, load_sem.at[1]),
        pltpu.make_async_copy(sgate_hbm, sgate_ref, load_sem.at[2]),
        pltpu.make_async_copy(sup_hbm, sup_ref, load_sem.at[3]),
        pltpu.make_async_copy(
            sdown_hbm.at[pl.ds(pl.multiple_of(t * shared_rows, 8), shared_rows)],
            sdown_ref,
            load_sem.at[4],
        ),
        pltpu.make_async_copy(gate_hbm, gate_ref, load_sem.at[5]),
        pltpu.make_async_copy(up_hbm, up_ref, load_sem.at[6]),
        pltpu.make_async_copy(down_hbm, down_ref, load_sem.at[7]),
    ]
    for load in firsts:
        load.start()

    def remote(src, dst, send, recv, e, k):
        return pltpu.make_async_remote_copy(
            src_ref=src,
            dst_ref=dst,
            send_sem=send,
            recv_sem=recv,
            device_id=(e, k),
            device_id_type=MESH,
        )

    barrier = pltpu.get_barrier_semaphore()
    partners = [(partner(g, p, ep), t) for p in range(1, ep)]
    partners += [(g, partner(z, d, chips) * 2 + c) for d in range(1, chips)]
    partners += [(g, mate)]
    for e, k in partners:
        pl.semaphore_signal(barrier, inc=1, device_id=(e, k), device_id_type=MESH)
    for load in loads:
        load.start()
    for load in firsts[:2]:
        load.wait()
    ids = ids_ref[...]
    affinity = affinity_ref[...]
    weights = affinity / jnp.sum(affinity, axis=0, keepdims=True) * ROUTED_SCALE
    block = rows // tp
    early = lax.broadcasted_iota(jnp.int32, (rows, rows), 0)
    late = lax.broadcasted_iota(jnp.int32, (rows, rows), 1)
    before = jnp.where((early < late) & (early // block == late // block), 1.0, 0.0).astype(BF16)
    hits = [ids == e * tp + t for e in range(ep)]
    chosen = [jnp.sum(jnp.where(hit, 1.0, 0.0), axis=0, keepdims=True) for hit in hits]
    pad = [jnp.zeros((-ep % 16, rows), F32)] if ep % 16 else []
    ranks = jnp.dot(
        jnp.concatenate(chosen + pad, axis=0).astype(BF16), before, preferred_element_type=F32
    ).astype(jnp.int32)
    base = (tp - 1 - lax.broadcasted_iota(jnp.int32, (1, rows), 1) // block) * slot_cap
    line = lax.broadcasted_iota(jnp.int32, (slots, rows), 0)
    for e in range(ep):
        place = jnp.where(chosen[e] > 0.5, base + ranks[e : e + 1, :], -1)
        weight = jnp.sum(jnp.where(hits[e], weights, 0.0), axis=0, keepdims=True)
        pick[e] = jnp.where(line == place, 1.0, 0.0).astype(BF16)
        spread_t[pl.ds(e * slots, slots), :] = jnp.where(line == place, weight, 0.0)
    sent_chunks = chunks - 1 if shift else chunks
    if shift:
        ret[chunks - 1] = jnp.zeros(ret.shape[1:], BF16)
    pl.semaphore_wait(barrier, len(partners))

    def forward(k):
        return remote(whole.at[k], whole.at[k], f_send.at[k // 2], a_recv.at[k], g, mate)

    def upward(k):
        there = lax.rem(z + 1, chips) * 2 + c
        return remote(whole.at[k], whole.at[k], u_send.at[k // 2], a_recv.at[k], g, there)

    def downward(k):
        there = lax.rem(z + chips - 1, chips) * 2 + c
        return remote(whole.at[k], whole.at[k], d_send.at[k // 2], a_recv.at[k], g, there)

    firsts[2].wait()

    @pl.when(z < chips - 1)
    def _():
        upward(t).start()

    @pl.when(z > 0)
    def _():
        downward(t).start()

    forward(t).start()

    crossed = slots - shift * slot_cap
    extra_rows = shift * block

    def ids_copy(p):
        e = partner(g, p, ep)
        return remote(ids_ref, ids_other.at[p - 1], i_send, i_recv, e, t)

    def affinity_copy(p):
        e = partner(g, p, ep)
        return remote(affinity_ref, affinity_other.at[p - 1], w_send, w_recv, e, t)

    def extra_copy(p):
        e = partner(g, p, ep)
        rows_out = whole.at[t, pl.ds(0, extra_rows)]
        return remote(rows_out, extra.at[t, p - 1], x_send, x_recv, e, t)

    def extra_forward(k):
        return remote(extra.at[k], extra.at[k], ef_send.at[k // 2], e_recv.at[k], g, mate)

    def extra_upward(k):
        there = lax.rem(z + 1, chips) * 2 + c
        return remote(extra.at[k], extra.at[k], eu_send.at[k // 2], e_recv.at[k], g, there)

    def extra_downward(k):
        there = lax.rem(z + chips - 1, chips) * 2 + c
        return remote(extra.at[k], extra.at[k], ed_send.at[k // 2], e_recv.at[k], g, there)

    if shift:
        for p in range(1, ep):
            extra_copy(p).start()

        @pl.when(c == 0)
        def _():
            for p in range(1, ep):
                ids_copy(p).start()

        @pl.when(c == 1)
        def _():
            for p in range(1, ep):
                affinity_copy(p).start()

    def extra_onward(chip):
        k = chip * 2 + c

        @pl.when((chip <= z) & (z < chips - 1))
        def _():
            extra_upward(k).start()

        @pl.when((chip >= z) & (z > 0))
        def _():
            extra_downward(k).start()

        extra_forward(k).start()

    def ids_share():
        return remote(ids_other, ids_other, m_send, m_recv, g, mate)

    def affinity_share():
        return remote(affinity_other, affinity_other, m_send, m_recv, g, mate)

    def pick_others():
        @pl.when(c == 0)
        def _():
            remote(ids_other, ids_other, i_send, i_recv, g, mate).wait_recv()
            ids_share().start()
            affinity_share().wait_recv()

        @pl.when(c == 1)
        def _():
            remote(affinity_other, affinity_other, w_send, w_recv, g, mate).wait_recv()
            affinity_share().start()
            ids_share().wait_recv()

        early = lax.broadcasted_iota(jnp.int32, (rows, rows), 0)
        late = lax.broadcasted_iota(jnp.int32, (rows, rows), 1)
        before = jnp.where((early < late) & (early // block == late // block), 1.0, 0.0)
        hits = [ids_other[p] == g * tp + t for p in range(ep - 1)]
        chosen = [jnp.sum(jnp.where(hit, 1.0, 0.0), axis=0, keepdims=True) for hit in hits]
        pad = [jnp.zeros((-(ep - 1) % 16, rows), F32)]
        ranks = jnp.dot(
            jnp.concatenate(chosen + pad, axis=0).astype(BF16),
            before.astype(BF16),
            preferred_element_type=F32,
        ).astype(jnp.int32)
        base = (tp - 1 - lax.broadcasted_iota(jnp.int32, (1, rows), 1) // block) * slot_cap
        line = lax.broadcasted_iota(jnp.int32, (slots, rows), 0)
        lanes = pick_other.shape[2]
        late_line = lax.broadcasted_iota(jnp.int32, (shift * slot_cap, lanes), 0) + crossed
        for p in range(ep - 1):
            place = jnp.where(chosen[p] > 0.5, base + ranks[p : p + 1, :], -1)
            pick_other[p] = jnp.where(late_line == place[:, :lanes], 1.0, 0.0).astype(BF16)
            share = affinity_other[p] / jnp.sum(affinity_other[p], axis=0, keepdims=True)
            weight = jnp.sum(jnp.where(hits[p], share * ROUTED_SCALE, 0.0), axis=0, keepdims=True)
            spread_other[p] = jnp.where(line == place, weight, 0.0).T.astype(BF16)

    near = [p for p in range(1, ep) if not p & (p - 1)]
    far = [p for p in range(1, ep) if p & (p - 1)]
    half = chunks // 8

    def send_rows(k, p):
        e = partner(g, p, ep)
        over = pl.ds(0, crossed)
        remote(sent.at[k, e, over], inc.at[k, g, over], b_send, b_recv.at[g], e, t).start()

    def arrive(chip):
        k = chip * 2 + c
        forward(k).wait_recv()

        @pl.when((chip < z) & (z < chips - 1))
        def _():
            upward(k).start()

        @pl.when((chip > z) & (z > 0))
        def _():
            downward(k).start()

        forward(k).start()

    def distance_step(d, carry):
        def at_side(side):
            chip = z + d * (side * 2 - 1)
            return chip, (chip >= 0) & (chip < chips) & ((d > 0) | (side == 0))

        for side in range(2):
            chip, there = at_side(side)

            @pl.when(there & (d > 0))
            def _():
                arrive(chip)

        def chunk_step(q, carry):
            chip, there = at_side(q % 2)
            lane = q // 2
            k = chip * 2 + lax.rem(c + lane, 2)

            @pl.when(there)
            def _():
                @pl.when(lane > 0)
                def _():
                    forward(k).wait_recv()

                picked = jnp.dot(
                    pick[...].reshape(ep * slots, rows), whole[k], preferred_element_type=F32
                ).astype(BF16)
                sent[k] = picked.reshape(ep, slots, feat)
                inc[k, g] = sent[k, g]
                for p in near:
                    send_rows(k, p)

            return carry

        lax.fori_loop(0, 4, chunk_step, 0)

        def far_step(q, carry):
            chip, there = at_side(q % 2)

            @pl.when(there)
            def _():
                for p in far:
                    send_rows(chip * 2 + lax.rem(c + q // 2, 2), p)

            return carry

        lax.fori_loop(0, 4, far_step, 0)
        if not shift:

            @pl.when(d == 0)
            def _():
                spread[...] = spread_t[...].T.astype(BF16)

            return carry

        @pl.when(d == 0)
        def _():
            remote(extra.at[t], extra.at[t], x_send, x_recv, g, mate).wait_recv()
            extra_onward(z)
            pick_others()
            spread[...] = spread_t[...].T.astype(BF16)

        for side in range(2):
            chip, there = at_side(side)

            @pl.when(there & (d > 0))
            def _():
                extra_forward(chip * 2 + c).wait_recv()
                extra_onward(chip)

        def extra_step(q, carry):
            chip, there = at_side(q % 2)
            lane = q // 2
            k = chip * 2 + lax.rem(c + lane, 2)

            @pl.when(there)
            def _():
                @pl.when(lane > 0)
                def _():
                    extra_forward(k).wait_recv()

                for p in range(1, ep):
                    inc[k, partner(g, p, ep), crossed:slots, :] = jnp.dot(
                        pick_other[p - 1][:, :extra_rows], extra[k, p - 1], preferred_element_type=F32
                    ).astype(BF16)

            return carry

        lax.fori_loop(0, 4, extra_step, 0)
        return carry

    lax.fori_loop(0, chips, distance_step, 0)
    def normalise(read, count):
        tile = math.gcd(64, count)

        def body(i, carry):
            at = pl.ds(pl.multiple_of(i * tile, tile), tile)
            total = jnp.zeros((tile, feat), F32)
            for k in range(tp):
                total = total + read(k, at).astype(F32)
            mean = jnp.sum(total, axis=1, keepdims=True) / width
            total = jnp.zeros((tile, feat), F32)
            for k in range(tp):
                center = read(k, at).astype(F32) - mean
                total = total + center * center
            scale = lax.rsqrt(jnp.sum(total, axis=1, keepdims=True) / width + EPSILON)
            for k in range(tp):
                lanes = slice(k * feat, (k + 1) * feat)
                value = (read(k, at).astype(F32) - mean) * scale
                value = value * gain_ref[:, lanes] + shift_ref[:, lanes]
                norm[at, lanes] = value.astype(BF16)
            return carry

        lax.fori_loop(0, count // tile, body, 0)

    for load in loads:
        load.wait()

    def activate(s):
        normalise(lambda k, at: inc[k, s, at, :], slots)
        got = norm[0:slots, :]
        gate_act = jnp.dot(got, gate_ref[...], preferred_element_type=F32)
        up_act = jnp.dot(got, up_ref[...], preferred_element_type=F32)
        hidden[s] = (jax.nn.silu(gate_act) * up_act).astype(BF16)

    def expert_step(j, carry):
        p = expert_order(j)
        s = partner(g, p, ep)
        over = pl.ds(0, crossed)
        remote(sent.at[:, s, over], inc.at[:, s, over], b_send, b_recv.at[s], s, t).wait_recv()

        activate(s)
        is_near = functools.reduce(jnp.logical_or, [p == n for n in near])

        @pl.when(is_near)
        def _():
            def near_step(i, carry):
                send_result(i, s)
                return carry

            lax.fori_loop(0, half, near_step, 0)

        return carry

    def lanes_of(i):
        return pl.ds(pl.multiple_of(i * cols, cols), cols)

    def down_rows(i, s):
        return jnp.dot(
            hidden[s], down_ref[:, lanes_of(i)], preferred_element_type=F32
        ).astype(BF16)

    def send_result(i, s):
        res[i, s] = down_rows(i, s)
        remote(res.at[i, s], ret.at[i, g], r_send, r_recv.at[i], s, t).start()

    normalise(lambda k, at: whole[k, at, :], rows)
    contract = (((1,), (1,)), ((), ()))
    sg = lax.dot_general(norm[...], sgate_ref[...], contract, preferred_element_type=F32)
    su = lax.dot_general(norm[...], sup_ref[...], contract, preferred_element_type=F32)
    shidden[...] = (jax.nn.silu(sg) * su).astype(BF16)

    order = near + far

    def expert_order(j):
        return sum(jnp.where(j == n, p, 0) for n, p in enumerate(order))

    lax.fori_loop(0, ep - 1, expert_step, 0)

    def turn_step(p):
        result = down_rows(chunks - 1, partner(g, p, ep))
        total = jnp.dot(spread_other[p - 1], result, preferred_element_type=F32)
        part[0] = total.reshape(part.shape[1:])
        for zz in range(chips):
            t_out[zz, p - 1] = part[0, zz * 2 + 1 - c].astype(BF16)
            mine[zz, p - 1] = part[0, zz * 2 + c]

        @pl.when(p == ep - 1)
        def _():
            remote(t_out, t_in, t_send, t_recv, g, mate).start()

    paired = chips == 4 and shift > 0
    inner = (z == 1) | (z == 2)
    beside = partner(z, 1, chips)
    across = 2 - 2 * (z // 2) if paired else 0

    def line_copy(zz):
        return remote(line_out.at[zz], line_in.at[z], l_send, l_recv, g, zz * 2 + c)

    def hop_copy():
        two = pl.ds(across, 2)
        return remote(line_out.at[two], hop_in, h_send, h_recv, g, beside * 2 + c)

    def line_start():
        remote(t_out, t_in, t_send, t_recv, g, mate).wait_recv()
        for d in range(1, chips):
            zz = partner(z, d, chips)
            line_out[zz] = (mine[zz] + t_in[zz].astype(F32)).astype(BF16)
            if d == 1 or not paired:
                line_copy(zz).start()
        if paired:

            @pl.when(jnp.logical_not(inner))
            def _():
                hop_copy().start()

    def line_pass():
        hop_copy().wait_recv()
        for k in range(2):
            zz = across + k
            total = mine[zz] + t_in[zz].astype(F32) + hop_in[k].astype(F32)
            line_out[zz] = total.astype(BF16)
            line_copy(zz).start()

    def line_finish():
        sources = [partner(z, d, chips) for d in range(1, chips)]
        if paired:
            sources = [beside, 2 - z // 2]
        some = pl.ds(0, len(sources))
        remote(line_out.at[some], line_in.at[some], l_send, l_recv, g, mate).wait_recv()
        total = mine[z] + t_in[z].astype(F32)
        for source in sources:
            total = total + line_in[source].astype(F32)
        y_out[...] = total.astype(BF16)
        for p in range(1, ep):
            there = partner(g, p, ep)
            remote(y_out.at[p - 1], y_in.at[p - 1], y_send, y_recv, there, t).start()

    def down_step(i, carry):
        for p in far:
            send_result(i, partner(g, p, ep))

        @pl.when(i < sent_chunks - half)
        def _():
            for p in near:
                send_result(i + half, partner(g, p, ep))

        if shift:

            @pl.when(i < ep - 1)
            def _():
                turn_step(i + 1)

            @pl.when(i == ep)
            def _():
                line_start()

        return carry

    lax.fori_loop(0, sent_chunks, down_step, 0)
    activate(g)

    def own_step(i, carry):
        ret[i, g] = down_rows(i, g)
        return carry

    lax.fori_loop(0, chunks, own_step, 0)
    def pair_copy(n):
        return remote(pair_out.at[n], pair_in.at[n], p_send, p_recv.at[n], g, mate)

    def produce(i, n):
        @pl.when(n < sent_chunks)
        def _():
            others = pl.ds(0, ep - 1)
            came = remote(res.at[n, others], ret.at[n, others], r_send, r_recv.at[n], g, mate)
            came.wait_recv()

        total = jnp.dot(
            spread[...], ret[n].reshape(ep * slots, cols), preferred_element_type=F32
        ) + jnp.dot(shidden[...], sdown_ref[:, lanes_of(n)], preferred_element_type=F32)
        part[i % 2] = total.reshape(part.shape[1:])
        for zz in range(chips):
            pair_out[n, zz] = part[i % 2, zz * 2 + 1 - c].astype(BF16)
        pair_copy(n).start()

    relayed = chunks - 3 if paired else 0

    def mixed(i, n, zz):
        return part[i % 2, zz * 2 + c] + pair_in[n, zz].astype(F32)

    def far_copy(n, zz, send):
        return remote(far_out.at[n, zz], far_in.at[n, z], send, q_recv.at[n], g, zz * 2 + c)

    def relay_copy(n):
        two = pl.ds(across, 2)
        return remote(far_out.at[n, two], relay.at[n], o_send, o_recv.at[n], g, beside * 2 + c)

    def finish(i, n):
        pair_copy(n).wait_recv()
        for d in range(1, chips):
            zz = partner(z, d, chips)
            far_out[n, zz] = mixed(i, n, zz).astype(BF16)
            if d == 1 or not paired:
                far_copy(n, zz, q_send).start()
        if paired:
            for send, which in ((q_send, inner), (o_send, jnp.logical_not(inner))):

                @pl.when((i >= relayed) & which)
                def _():
                    for k in range(2):
                        far_copy(n, across + k, send).start()

            @pl.when((i < relayed) & jnp.logical_not(inner))
            def _():
                relay_copy(n).start()

        own[n] = part[i % 2, t] + pair_in[n, z].astype(F32)

    def pass_on(i, n):
        relay_copy(n).wait_recv()
        for k in range(2):
            zz = across + k
            far_out[n, zz] = (mixed(i, n, zz) + relay[n, k].astype(F32)).astype(BF16)
            far_copy(n, zz, q_send).start()

    def chunk_of(i):
        return lax.rem(i + sent_chunks, chunks)

    def sum_step(i, carry):
        n = chunk_of(i)
        produce(i, n)
        if paired:

            @pl.when(inner & (i > 0) & (i <= relayed))
            def _():
                pass_on(i - 1, chunk_of(i - 1))

        finish(i, n)
        if shift:

            if paired:

                @pl.when(inner & (i == 0))
                def _():
                    line_pass()

            @pl.when(i == 4)
            def _():
                line_finish()

        return carry

    lax.fori_loop(0, chunks, sum_step, 0)

    def gathered(n, count):
        some = pl.ds(0, count)
        return remote(far_out.at[n, some], far_in.at[n, some], q_send, q_recv.at[n], g, mate)

    def put(n, sources):
        gathered(n, len(sources)).wait_recv()
        total = own[n]
        for source in sources:
            total = total + far_in[n, source].astype(F32)
        if shift:

            @pl.when(n == sent_chunks)
            def _():
                remote(y_out, y_in, y_send, y_recv, g, mate).wait_recv()
                more = y_in[0].astype(F32)
                for p in range(1, ep - 1):
                    more = more + y_in[p].astype(F32)
                own[n] = total + more

            @pl.when(n < sent_chunks)
            def _():
                own[n] = total

            total = own[n]
        out_ref[:, lanes_of(n)] = total.astype(BF16)

    def out_step(i, carry):
        n = lax.rem(i, chunks)
        later = lax.rem(n + chunks - sent_chunks, chunks) >= relayed

        @pl.when(later)
        def _():
            put(n, [partner(z, d, chips) for d in range(1, chips)])

        if paired:

            @pl.when(jnp.logical_not(later))
            def _():
                put(n, [beside, 2 - z // 2])

        return carry


    rest = pl.ds(0, chips - 1)
    if paired:

        @pl.when(inner)
        def _():
            remote(far_out.at[:, rest], far_in.at[:, rest], q_send, q_recv.at[0], g, mate).wait_send()

        @pl.when(jnp.logical_not(inner))
        def _():
            one = pl.ds(0, 1)
            remote(far_out.at[:, one], far_in.at[:, one], q_send, q_recv.at[0], g, mate).wait_send()
            remote(relay, relay, o_send, o_recv.at[0], g, mate).wait_send()

    else:
        remote(far_out.at[:, rest], far_in.at[:, rest], q_send, q_recv.at[0], g, mate).wait_send()

    others = pl.ds(0, ep - 1)
    over = pl.ds(0, crossed)
    remote(
        sent.at[:, others, over], inc.at[:, others, over], b_send, b_recv.at[g], g, mate
    ).wait_send()
    some = pl.ds(0, sent_chunks)
    remote(
        res.at[some, others], ret.at[some, others], r_send, r_recv.at[0], g, mate
    ).wait_send()
    remote(pair_out, pair_in, p_send, p_recv.at[0], g, mate).wait_send()

    def sent_step(chip, carry):
        k = chip * 2 + c
        forward(k).wait_send()

        @pl.when((chip <= z) & (z < chips - 1))
        def _():
            upward(k).wait_send()

        @pl.when((chip >= z) & (z > 0))
        def _():
            downward(k).wait_send()

        if not shift:
            return carry
        extra_forward(k).wait_send()

        @pl.when((chip <= z) & (z < chips - 1))
        def _():
            extra_upward(k).wait_send()

        @pl.when((chip >= z) & (z > 0))
        def _():
            extra_downward(k).wait_send()

        return carry

    lax.fori_loop(0, chips, sent_step, 0)
    if shift:

        @pl.when(c == 0)
        def _():
            remote(ids_other, ids_other, i_send, i_recv, g, mate).wait_send()
            ids_share().wait_send()

        @pl.when(c == 1)
        def _():
            remote(affinity_other, affinity_other, w_send, w_recv, g, mate).wait_send()
            affinity_share().wait_send()

        remote(extra.at[t], extra.at[t], x_send, x_recv, g, mate).wait_send()
        remote(t_out, t_in, t_send, t_recv, g, mate).wait_send()
        remote(y_out, y_in, y_send, y_recv, g, mate).wait_send()
        some = pl.ds(0, chips - 1)
        if paired:

            @pl.when(inner)
            def _():
                remote(line_out.at[some], line_in.at[some], l_send, l_recv, g, mate).wait_send()

            @pl.when(jnp.logical_not(inner))
            def _():
                line_copy(beside).wait_send()
                hop_copy().wait_send()

        else:
            remote(line_out.at[some], line_in.at[some], l_send, l_recv, g, mate).wait_send()

    lax.fori_loop(0, chunks, out_step, 0)


def on_device(
    tokens,
    norm_gain,
    norm_shift,
    expert_ids,
    affinity,
    expert_gate,
    expert_up,
    expert_down,
    shared_gate,
    shared_up,
    shared_down,
):
    ep = lax.axis_size("ep")
    tp = lax.axis_size("tp")
    rows, feat = tokens.shape
    width = feat * tp
    top_count = expert_ids.shape[1]
    block = rows // tp
    expert_count = ep * tp
    slot_cap = max(1, 2 * block * top_count // expert_count)
    slots = tp * slot_cap
    hid = expert_gate.shape[2]
    shared_rows = shared_gate.shape[0]
    cols = 256
    chunks = width // cols
    chips = tp // 2
    shift = max(1, tp // 8)
    fits = (ep & (ep - 1)) == 0 and ep > 1 and slot_cap % 8 == 0 and block % 8 == 0
    if not fits or shift * block > 128 or rows < 128:
        shift = 0
    lanes = min(rows, 128)
    line = (chips, ep - 1, block, cols) if shift else (1, 1, 8, 128)
    back = line[1:]
    other = (ep - 1, rows, slots) if shift else (1, 8, 128)

    vmem = pl.BlockSpec(memory_space=pltpu.VMEM)
    anywhere = pl.BlockSpec(memory_space=pl.ANY)
    dma = pltpu.SemaphoreType.DMA
    return pl.pallas_call(
        functools.partial(layer_kernel, (ep, tp, rows, slots, slot_cap, feat, chunks, cols, shift)),
        out_shape=pltpu.VMEM((block, width), BF16),
        in_specs=[anywhere] * 11,
        out_specs=vmem,
        scratch_shapes=[
            pltpu.VMEM((top_count, rows), jnp.int32),
            pltpu.VMEM((top_count, rows), F32),
            pltpu.VMEM((1, width), F32),
            pltpu.VMEM((1, width), F32),
            pltpu.VMEM((shared_rows, width), BF16),
            pltpu.VMEM((shared_rows, width), BF16),
            pltpu.VMEM((width, hid), BF16),
            pltpu.VMEM((width, hid), BF16),
            pltpu.VMEM((hid, width), BF16),
            pltpu.VMEM((shared_rows, width), BF16),
            pltpu.VMEM((tp, rows, feat), BF16),
            pltpu.VMEM((ep, slots, rows), BF16),
            pltpu.VMEM((ep * slots, rows), F32),
            pltpu.VMEM((rows, ep * slots), BF16),
            pltpu.VMEM((tp, ep, slots, feat), BF16),
            pltpu.VMEM((tp, ep, slots, feat), BF16),
            pltpu.VMEM((max(rows, slots), width), BF16),
            pltpu.VMEM((ep, slots, hid), BF16),
            pltpu.VMEM((rows, shared_rows), BF16),
            pltpu.VMEM((chunks, ep, slots, cols), BF16),
            pltpu.VMEM((chunks, ep, slots, cols), BF16),
            pltpu.VMEM((ep - 1, top_count, rows), jnp.int32),
            pltpu.VMEM((tp, ep - 1, max(8, shift * block), feat), BF16),
            pltpu.VMEM((ep - 1, max(8, shift * slot_cap), lanes), BF16),
            pltpu.VMEM((ep - 1, top_count, rows), F32),
            pltpu.VMEM(other, BF16),
            pltpu.VMEM(line, F32),
            pltpu.VMEM(line, BF16),
            pltpu.VMEM(line, BF16),
            pltpu.VMEM(line, BF16),
            pltpu.VMEM(line, BF16),
            pltpu.VMEM((2,) + back, BF16),
            pltpu.VMEM(back, BF16),
            pltpu.VMEM(back, BF16),
            pltpu.VMEM((2, tp, block, cols), F32),
            pltpu.VMEM((chunks, block, cols), F32),
            pltpu.VMEM((chunks, chips, block, cols), BF16),
            pltpu.VMEM((chunks, chips, block, cols), BF16),
            pltpu.VMEM((chunks, chips, block, cols), BF16),
            pltpu.VMEM((chunks, chips, block, cols), BF16),
            pltpu.VMEM((chunks, 2, block, cols), BF16),
            dma((8,)),
            dma((3,)),
            dma((chips,)),
            dma((chips,)),
            dma((chips,)),
            dma((tp,)),
            dma,
            dma((ep,)),
            dma,
            dma((chunks,)),
            dma,
            dma((chunks,)),
            dma,
            dma((chunks,)),
            dma,
            dma((chunks,)),
            dma,
            dma,
            dma,
            dma,
            dma((chips,)),
            dma((chips,)),
            dma((chips,)),
            dma((tp,)),
            dma,
            dma,
            dma,
            dma,
            dma,
            dma,
            dma,
            dma,
            dma,
            dma,
            dma,
            dma,
        ],
        compiler_params=pltpu.CompilerParams(
            collective_id=0, has_side_effects=True, vmem_limit_bytes=56 * 1024 * 1024
        ),
        name="moe_layer",
    )(
        tokens,
        expert_ids.T,
        affinity.T,
        norm_gain.reshape(1, width),
        norm_shift.reshape(1, width),
        shared_gate,
        shared_up,
        expert_gate[0],
        expert_up[0],
        expert_down[0],
        shared_down,
    )


def solution(mesh):
    placed = (
        P("ep", "tp"),
        P(),
        P(),
        P("ep", None),
        P("ep", None),
        P(("ep", "tp"), None, None),
        P(("ep", "tp"), None, None),
        P(("ep", "tp"), None, None),
        P("tp", None),
        P("tp", None),
        P(),
    )
    return jax.shard_map(
        on_device, mesh=mesh, in_specs=placed, out_specs=P(("ep", "tp"), None), check_vma=False
    )
```
